128 devices in a mesh: ep: 64 (over z, y, x), tp: 2 (over core).
Axes of the slice: x: 4, y: 4, z: 4, core: 2. Of those that a mesh axis runs over, the one named last changes fastest.
Arguments:
- tokens: bfloat16 [2048, 2048], P('ep'), may hold values from -6 to 6
- lengths: int32 [2048], P('ep'), may hold values from 128 to 1024
- key_cache: bfloat16 [2048, 1024, 256], P('ep', None, 'tp'), may hold values from -1000 to 1000
- value_cache: bfloat16 [2048, 1024, 256], P('ep', None, 'tp'), may hold values from -6 to 6
- gate_cache: float32 [2048, 16, 1024], P('ep', 'tp'), may hold values from -130 to 0, as said below
- mix_gain: float32 [2048], replicated, may hold values from 0.1 to 1.9
- query_weight: bfloat16 [2048, 1024], P(None, 'tp'), may hold values from -0.125 to 0.125
- key_weight: bfloat16 [2048, 256], P(None, 'tp'), may hold values from -0.125 to 0.125
- value_weight: bfloat16 [2048, 256], P(None, 'tp'), may hold values from -0.125 to 0.125
- forget_weight: bfloat16 [2048, 16], P(None, 'tp'), may hold values from -0.125 to 0.125
- out_weight: bfloat16 [1024, 2048], P('tp'), may hold values from -0.1875 to 0.1875
- expert_gain: float32 [2048], replicated, may hold values from 0.1 to 1.9
- routes: int32 [2048, 2], P('ep'), may hold values from 0 to 7, all different within a row; in each aligned block of 32 rows (0 to 31, 32 to 63, ...) at most 12 rows name the same one
- route_weights: float32 [2048, 2], P('ep'), may hold values from 0.2 to 1
- expert_gate: bfloat16 [2048, 65536], P(None, ('ep', 'tp')), may hold values from -0.125 to 0.125
- expert_up: bfloat16 [2048, 65536], P(None, ('ep', 'tp')), may hold values from -0.125 to 0.125
- expert_down: bfloat16 [65536, 2048], P(('ep', 'tp')), may hold values from -0.0625 to 0.0625
Outputs:
- layer_out: bfloat16 [2048, 2048], P('ep')
The draws below stay inside these ranges and needn't reach their ends.
Inputs may be any that keep to these rules, and one draw needn't show every extreme that they name: `routes`: within the rows of one index of ep, no expert is named more than 12 times, and in every draw some expert is named exactly 12 times in some such rows; the 2 experts of a row differ. `gate_cache`: for each sequence and head the values never rise along the cache positions.
All inputs are finite; a program needn't handle non-finite values.
Results may differ from the reference program's by a relative error of at most 0.013.
Values may be sent and summed in bfloat16 or wider, within the bound.
A program may use at most 128 MiB of HBM per device.

```python
import math
import jax
import jax.numpy as jnp
import numpy as np
from jax import lax

D = 2048
HEADS = 16
KV_HEADS = 4
HD = 64
FF = 8192
EXPERTS = 8
TOP = 2
SEQ_DEV = 32
CACHE_POSITIONS = 1024
CAP = 12
SEQUENCE_TOTAL = 2048
N_EP = 64
N_TP = 2


def draw_gate_cache(key, part):
    key_fragments = jax.random.split(jax.random.fold_in(key, 11), 7)
    order = jax.random.permutation(key_fragments[0], HEADS)
    slow = order < HEADS // 2
    slow_rate = jax.random.uniform(key_fragments[1], (SEQUENCE_TOTAL, HEADS), jnp.float32, 0.1, 0.5) / CACHE_POSITIONS
    fast_rate = jnp.exp(jax.random.uniform(key_fragments[2], (SEQUENCE_TOTAL, HEADS), jnp.float32, jnp.log(1.0 / 100.0), jnp.log(1.0 / 30.0)))
    rate = jnp.where(slow[None, :], slow_rate, fast_rate)
    seq_factor = jnp.exp(jax.random.uniform(key_fragments[3], (SEQUENCE_TOTAL, 1, 1), jnp.float32, -0.7, 0.7))
    rough = jax.random.uniform(key_fragments[4], (SEQUENCE_TOTAL, HEADS, CACHE_POSITIONS), jnp.float32, 0.4, 1.6)
    step_log_gates = -rate[:, :, None] * seq_factor * rough
    spike_position = jax.random.randint(key_fragments[5], (SEQUENCE_TOTAL, 3), 0, CACHE_POSITIONS)
    decay_amounts = jax.random.uniform(key_fragments[6], (SEQUENCE_TOTAL, 3), jnp.float32, 0.2, 0.4)
    cache_locations = jnp.arange(CACHE_POSITIONS, dtype=jnp.int32)
    spike_events = jnp.sum(jnp.where(cache_locations[None, None, :] == spike_position[:, :, None], jnp.log(1.0 - decay_amounts)[:, :, None], 0.0), axis=1)
    step_log_gates = step_log_gates + spike_events[:, None, :]
    return jnp.cumsum(step_log_gates, axis=-1).astype(jnp.float32)


def draw_key_cache(key, part):
    key_fragments = jax.random.split(jax.random.fold_in(key, 23), 1)
    base = jnp.clip(jax.random.normal(key_fragments[0], (SEQUENCE_TOTAL, CACHE_POSITIONS, KV_HEADS * HD), jnp.float32), -6.0, 6.0)
    return base.astype(jnp.bfloat16)


def with_ends(values, rng, smallest, largest):
    shape = values.shape
    place = [jax.random.randint(jax.random.fold_in(rng, axis), (), 0, shape[axis]) for axis in range(len(shape))]
    values = values.at[tuple(place)].set(smallest)
    longest = shape.index(max(shape))
    place[longest] = (place[longest] + 1) % shape[longest]
    return values.at[tuple(place)].set(largest)


def levels(rng, dims, cuts, smallest, top_value):
    level = 1.0
    for axis_at, shards_of in cuts:
        steps = jax.random.uniform(jax.random.fold_in(jax.random.fold_in(rng, 6), axis_at), (shards_of,), jnp.float32, smallest / len(cuts), top_value / len(cuts))
        level = level * jnp.repeat(jnp.exp(steps), dims[axis_at] // shards_of).reshape((-1,) + (1,) * (len(dims) - 1 - axis_at))
    return level


def deal_out(key, own, number, rows, count, top, bound, lean):
    sequence = jax.random.permutation(key, count)
    crowded, usual = shares(count, rows * top, bound, lean, True), shares(count, rows * top, bound, lean, False)
    places = jnp.arange(count)

    def named(sizes, rotation):
        used = int((sizes > 0).sum())
        fixed = max(1, used // 4)
        shifted = fixed + (places - fixed + rotation * (used - fixed)) % max(1, count - fixed)
        return jnp.zeros((count,), jnp.int32).at[sequence[jnp.where(places < fixed, places, shifted)]].set(jnp.asarray(sizes, jnp.int32))

    sizes = jnp.where(number % 4 == 0, named(crowded, number // 4), named(usual, number - number // 4 - 1))
    mixed = jax.random.permutation(jax.random.fold_in(own, 3), count)
    source_of, taker = mixed[0:count // 2 * 2:2], mixed[1:count // 2 * 2:2]
    room = jnp.minimum(sizes[source_of] - 1, bound - sizes[taker]) // 2
    room = jnp.where((source_of == sequence[0]) | (taker == sequence[0]) | (sizes[taker] == 0), 0, jnp.maximum(room, 0))
    shifted = jax.random.randint(jax.random.fold_in(own, 4), (count // 2,), 0, 1 << 20) % (room + 1)
    sizes = sizes.at[source_of].add(-shifted).at[taker].add(shifted)
    members = jnp.searchsorted(jnp.cumsum(sizes), jnp.arange(rows * top), side="right").astype(jnp.int32)
    listing = members.reshape(top, rows).T
    listing = listing[jax.random.permutation(jax.random.fold_in(own, 1), rows)]
    rotation = jax.random.randint(jax.random.fold_in(own, 2), (rows, 1), 0, top)
    return jnp.take_along_axis(listing, (jnp.arange(top)[None, :] + rotation) % top, axis=1)


def shares(count, total, reach, lean, full):
    loads = [(1 << 20) // math.isqrt(grade ** lean) + 1 for grade in range(1, count + 1)]
    largest = reach if full else min(reach, max(-(-total // count), total * loads[0] // sum(loads)))
    least = 1 if total - largest >= count - 1 else 0
    counts, rest = [largest] + [least] * (count - 1), total - largest - least * (count - 1)
    while rest > 0:
        candidates = [i for i in range(1, count) if counts[i] < largest] or [i for i in range(1, count) if counts[i] < reach]
        pool, budget = sum([loads[i] for i in candidates]), rest
        for i in candidates:
            addition = min(reach - counts[i], max(1, budget * loads[i] // pool), rest)
            counts[i] = counts[i] + addition
            rest = rest - addition
    return np.array(counts)


def scatter_about(own_key, extent, scale, reach, cuts=(), held_as=jnp.bfloat16):
    array = jax.random.normal(own_key, extent, jnp.float32) * scale
    if len(cuts) > 0:
        array = levels(own_key, extent, cuts, -0.22, 0.18) * array
    return jnp.clip(array, min=-reach, max=reach).astype(held_as)


def setup_inputs(seed: int = 0) -> dict:
    splits = jax.random.split(jax.random.key(seed), 18)
    tokens = scatter_about(splits[0], (SEQUENCE_TOTAL, D), 1.0, 6.0, ((0, 64),))
    lengths = with_ends(jax.random.randint(splits[1], (SEQUENCE_TOTAL,), CACHE_POSITIONS // 8, CACHE_POSITIONS + 1), jax.random.fold_in(splits[1], 1), CACHE_POSITIONS // 8, CACHE_POSITIONS).astype(jnp.int32)
    key_cache = draw_key_cache(jax.random.fold_in(splits[17], 71), 0)
    value_cache = scatter_about(splits[3], (SEQUENCE_TOTAL, CACHE_POSITIONS, KV_HEADS * HD), 1.0, 6.0, ((0, 64), (2, 2)))
    gate_cache = draw_gate_cache(jax.random.fold_in(splits[17], 71), 0)
    mix_gain = jnp.clip(1.0 + 0.18 * jax.random.normal(splits[5], (D,), jnp.float32), 0.1, 1.9)
    query_weight = scatter_about(splits[6], (D, HEADS * HD), D ** -0.5, 0.125, ((1, 2),))
    key_weight = scatter_about(splits[7], (D, KV_HEADS * HD), D ** -0.5, 0.125, ((1, 2),))
    value_weight = scatter_about(splits[8], (D, KV_HEADS * HD), D ** -0.5, 0.125, ((1, 2),))
    forget_weight = scatter_about(splits[9], (D, HEADS), D ** -0.5, 0.125, ((1, 2),))
    out_weight = scatter_about(splits[10], (HEADS * HD, D), (HEADS * HD) ** -0.5, 0.1875, ((0, 2),))
    expert_gain = jnp.clip(1.0 + 0.18 * jax.random.normal(splits[11], (D,), jnp.float32), 0.1, 1.9)
    routes_keys = jax.random.split(jax.random.fold_in(splits[12], 1), SEQUENCE_TOTAL // SEQ_DEV)
    routes_turns = jax.random.permutation(jax.random.fold_in(splits[12], 3), SEQUENCE_TOTAL // SEQ_DEV)
    routes = jax.vmap(lambda own, number: deal_out(jax.random.fold_in(splits[12], 2), own, number, SEQ_DEV, EXPERTS, TOP, CAP, 2))(routes_keys, routes_turns).reshape((SEQUENCE_TOTAL, TOP))
    route_weights = jnp.clip(0.2 + 0.8 * jax.random.uniform(splits[13], (SEQUENCE_TOTAL, TOP), jnp.float32) ** levels(splits[13], (SEQUENCE_TOTAL, TOP), ((0, 64),), -0.2, 0.2), 0.2, 1.0)
    expert_gate = scatter_about(splits[14], (D, EXPERTS * FF), D ** -0.5, 0.125, ((1, 128),))
    expert_up = scatter_about(splits[15], (D, EXPERTS * FF), D ** -0.5, 0.125, ((1, 128),))
    expert_down = scatter_about(splits[16], (EXPERTS * FF, D), FF ** -0.5, 0.0625, ((0, 128),))
    return dict(tokens=tokens, lengths=lengths, key_cache=key_cache, value_cache=value_cache, gate_cache=gate_cache, mix_gain=mix_gain, query_weight=query_weight, key_weight=key_weight, value_weight=value_weight, forget_weight=forget_weight, out_weight=out_weight, expert_gain=expert_gain, routes=routes, route_weights=route_weights, expert_gate=expert_gate, expert_up=expert_up, expert_down=expert_down)


eps = 1e-06

def normed(values, gain):
    floats = values.astype(jnp.float32)
    return floats * lax.rsqrt(lax.optimization_barrier(jnp.mean(floats * floats, axis=-1, keepdims=True)) + eps) * gain

def attend(pack):
    queries, key_new, value_new, log_gate, key_rows, value_rows, cumulative, length = pack
    seq_count, head_count, head_size = queries.shape
    kv_count = key_new.shape[1]
    group_size = head_count // kv_count
    cache_locations = key_rows.shape[1]
    factor = head_size ** (-0.5)
    grouped = queries.reshape(seq_count, kv_count, group_size, head_size).astype(jnp.float32)
    key_split = key_rows.reshape(seq_count, cache_locations, kv_count, head_size).astype(jnp.float32)
    value_split = value_rows.reshape(seq_count, cache_locations, kv_count, head_size).astype(jnp.float32)
    scores = jnp.einsum('skgd,spkd->skgp', grouped, key_split).reshape(seq_count, head_count, cache_locations) * factor
    positions = jnp.arange(cache_locations, dtype=jnp.int32)
    latest = lax.optimization_barrier(jnp.sum(jnp.where(positions[None, None, :] == (length - 1)[:, None, None], cumulative, 0.0), axis=-1))
    scores = scores + (latest + log_gate)[..., None] - cumulative
    valid = positions[None, None, :] < length[:, None, None]
    scores = jnp.where(valid, scores, -jnp.inf)
    own_score = jnp.einsum('skgd,skd->skg', grouped, key_new.astype(jnp.float32)).reshape(seq_count, head_count) * factor
    highest = jnp.maximum(lax.optimization_barrier(jnp.max(scores, axis=-1)), own_score)
    raised = jnp.exp(scores - highest[..., None])
    own_raised = jnp.exp(own_score - highest)
    denominator = lax.optimization_barrier(jnp.sum(raised, axis=-1)) + own_raised
    weights = (raised / denominator[..., None]).astype(jnp.bfloat16)
    own_weight = (own_raised / denominator).astype(jnp.bfloat16)
    mixed = jnp.einsum('skgp,spkd->skgd', weights.reshape(seq_count, kv_count, group_size, cache_locations).astype(jnp.float32), value_split)
    mixed = mixed + own_weight.reshape(seq_count, kv_count, group_size)[..., None].astype(jnp.float32) * value_new.astype(jnp.float32)[:, :, None, :]
    return mixed.reshape(seq_count, head_count * head_size).astype(jnp.bfloat16)

def reference(tokens, lengths, key_cache, value_cache, gate_cache, mix_gain, query_weight, key_weight, value_weight, forget_weight, out_weight, expert_gain, routes, route_weights, expert_gate, expert_up, expert_down):
    normal_in = normed(tokens, mix_gain).astype(jnp.bfloat16)
    queries = jnp.dot(normal_in, query_weight, preferred_element_type=jnp.float32).astype(jnp.bfloat16).reshape(N_EP, SEQ_DEV, HEADS, HD)
    key_new = jnp.dot(normal_in, key_weight, preferred_element_type=jnp.float32).astype(jnp.bfloat16).reshape(N_EP, SEQ_DEV, KV_HEADS, HD)
    value_new = jnp.dot(normal_in, value_weight, preferred_element_type=jnp.float32).astype(jnp.bfloat16).reshape(N_EP, SEQ_DEV, KV_HEADS, HD)
    log_gate = jax.nn.log_sigmoid(jnp.dot(normal_in, forget_weight, preferred_element_type=jnp.float32)).reshape(N_EP, SEQ_DEV, HEADS)
    mixed = lax.map(attend, (queries, key_new, value_new, log_gate, key_cache.reshape(N_EP, SEQ_DEV, CACHE_POSITIONS, KV_HEADS * HD), value_cache.reshape(N_EP, SEQ_DEV, CACHE_POSITIONS, KV_HEADS * HD), gate_cache.reshape(N_EP, SEQ_DEV, HEADS, CACHE_POSITIONS), lengths.reshape(N_EP, SEQ_DEV)))
    mixed = mixed.reshape(SEQUENCE_TOTAL, HEADS * HD)
    split = HEADS * HD // N_TP
    summed = tokens.astype(jnp.float32)
    for group_index in range(N_TP):
        product = jnp.dot(mixed[:, group_index * split:(group_index + 1) * split], out_weight[group_index * split:(group_index + 1) * split], preferred_element_type=jnp.float32)
        summed = summed + lax.optimization_barrier(product.astype(jnp.bfloat16)).astype(jnp.float32)
    residual = summed.astype(jnp.bfloat16)
    expert_in = normed(residual, expert_gain).astype(jnp.bfloat16)
    flat_routes = routes.reshape(N_EP, SEQ_DEV * TOP)
    one_hot = (flat_routes[..., None] == jnp.arange(EXPERTS, dtype=jnp.int32)).astype(jnp.int32)
    slot_index = lax.optimization_barrier(jnp.sum((jnp.cumsum(one_hot, axis=1) - 1) * one_hot, axis=-1))
    repeated = jnp.repeat(expert_in.reshape(N_EP, SEQ_DEV, D), TOP, axis=1).astype(jnp.float32)
    pieces = N_EP // EXPERTS
    quarter = FF // (pieces * N_TP)

    def one_expert(expert):
        chosen = (flat_routes == expert)[:, None, :] & (slot_index[:, None, :] == jnp.arange(CAP, dtype=jnp.int32)[None, :, None])
        rows_in = jnp.einsum('ncr,nrd->ncd', chosen.astype(jnp.float32), repeated).astype(jnp.bfloat16).reshape(N_EP * CAP, D)
        w_gate = lax.dynamic_slice_in_dim(expert_gate, expert * FF, FF, 1)
        w_up = lax.dynamic_slice_in_dim(expert_up, expert * FF, FF, 1)
        w_down = lax.dynamic_slice_in_dim(expert_down, expert * FF, FF, 0)
        gate_out = jnp.dot(rows_in, w_gate, preferred_element_type=jnp.float32)
        up_out = jnp.dot(rows_in, w_up, preferred_element_type=jnp.float32)
        hidden = (jax.nn.silu(gate_out) * up_out).astype(jnp.bfloat16)
        halves = jnp.einsum('rbtf,btfd->rbtd', hidden.reshape(N_EP * CAP, pieces, N_TP, quarter).astype(jnp.float32), w_down.reshape(pieces, N_TP, quarter, D).astype(jnp.float32))
        halves = lax.optimization_barrier(halves.astype(jnp.bfloat16)).astype(jnp.float32)
        blocks = lax.optimization_barrier(lax.optimization_barrier(jnp.sum(halves, axis=2)).astype(jnp.bfloat16)).astype(jnp.float32)
        return lax.optimization_barrier(jnp.sum(blocks, axis=1))
    results = lax.map(one_expert, jnp.arange(EXPERTS, dtype=jnp.int32))
    row_index = flat_routes * (N_EP * CAP) + jnp.arange(N_EP, dtype=jnp.int32)[:, None] * CAP + slot_index
    picked = jnp.take(results.reshape(EXPERTS * N_EP * CAP, D), row_index.reshape(-1).astype(jnp.int32), axis=0).reshape(SEQUENCE_TOTAL, TOP, D)
    mixture = lax.optimization_barrier(jnp.sum(picked * route_weights[..., None], axis=1))
    return (residual.astype(jnp.float32) + mixture).astype(jnp.bfloat16)
```

```python
import functools
import jax
import jax.numpy as jnp
from jax import lax
from jax.experimental import pallas as pl
from jax.experimental.pallas import tpu as pltpu
from jax.sharding import PartitionSpec as P

SEQS = 32
POS = 1024
LANES = 128
HEADS_HERE = 8


def rms(values, gain):
    return values * lax.rsqrt(jnp.mean(values * values, axis=-1, keepdims=True) + 1e-06) * gain


def attention_kernel(
    len_ref, tok_hbm, key_hbm, value_hbm, gate_hbm, gain_hbm, wq_hbm, wk_hbm, wv_hbm, wf_hbm, wo_hbm,
    out_ref,
    tok, gain, wq, wk, wv, wf, wo, keys, values, gates, qs, owns, lgs, vnew, mixed, sems, kv_sems,
):
    blocks, per = kv_sems.shape[1], SEQS // kv_sems.shape[1]
    small = [(tok_hbm, tok), (gain_hbm, gain), (wq_hbm, wq), (wk_hbm, wk), (wv_hbm, wv), (wf_hbm, wf), (wo_hbm, wo)]
    copies = [pltpu.make_async_copy(a, b, sems.at[i]) for i, (a, b) in enumerate(small)]

    def block_copies(b):
        rows = pl.ds(b * per, per)
        return [
            pltpu.make_async_copy(src.at[rows], dst.at[rows], kv_sems.at[i, b])
            for i, (src, dst) in enumerate(((key_hbm, keys), (gate_hbm, gates), (value_hbm, values)))
        ]

    for c in copies[:6]:
        c.start()
    for b in range(blocks):
        for c in block_copies(b):
            c.start()
    copies[6].start()

    copies[0].wait()
    copies[1].wait()
    ni = rms(tok[...].astype(jnp.float32), gain[...]).astype(jnp.bfloat16)
    lane = lax.broadcasted_iota(jnp.int32, (SEQS, LANES), 1)
    left = lane < 64
    for c in copies[2:6]:
        c.wait()
    dot = functools.partial(jnp.dot, preferred_element_type=jnp.float32)
    q = dot(ni, wq[...]).astype(jnp.bfloat16).astype(jnp.float32) * 0.125
    kn = dot(ni, wk[...]).astype(jnp.bfloat16).astype(jnp.float32)
    vnew[...] = dot(ni, wv[...]).astype(jnp.bfloat16).astype(jnp.float32)
    f = dot(ni, wf[...])
    lg = jnp.minimum(f, 0.0) - jnp.log1p(jnp.exp(-jnp.abs(f)))
    for h in range(HEADS_HERE):
        column = q[:, 128 * (h // 2) : 128 * (h // 2) + 128]
        if h % 2 != h // 4:
            column = pltpu.roll(column, 64, 1)
        column = jnp.where(left if h < 4 else ~left, column, 0.0)
        rows = pl.ds(h, SEQS, stride=HEADS_HERE)
        qs[rows, :] = column
        owns[rows, :] = jnp.broadcast_to(jnp.sum(column * kn, axis=1, keepdims=True), (SEQS, LANES))
        lgs[rows, :] = jnp.broadcast_to(lg[:, h : h + 1], (SEQS, LANES))

    position = lax.broadcasted_iota(jnp.int32, (HEADS_HERE, POS), 1)

    def block(b, carry):
        for c in block_copies(b):
            c.wait()
        for j in range(per):
            s = b * per + j
            rows = pl.ds(s * HEADS_HERE, HEADS_HERE)
            length = len_ref[s]
            g = gates[s]
            score = lax.dot_general(
                qs[rows, :].astype(jnp.bfloat16), keys[s], (((1,), (1,)), ((), ())),
                preferred_element_type=jnp.float32,
            )
            latest = jnp.sum(jnp.where(position == length - 1, g, 0.0), axis=1, keepdims=True)
            own = owns[rows, 0:1]
            score = jnp.where(position < length, score + (latest + lgs[rows, 0:1]) - g, -jnp.inf)
            top = jnp.maximum(jnp.max(score, axis=1, keepdims=True), own)
            raised = jnp.exp(score - top)
            own_raised = jnp.exp(own - top)
            total = jnp.sum(raised, axis=1, keepdims=True) + own_raised
            o = dot(raised.astype(jnp.bfloat16), values[s])
            mixed[rows, :] = (o + own_raised * vnew[pl.ds(s, 1), :]) / total
        return carry

    lax.fori_loop(0, blocks, block, 0)
    parts = []
    for c in range(4):
        pair = []
        for h in (2 * c, 2 * c + 1):
            o = mixed[pl.ds(h, SEQS, stride=HEADS_HERE), :]
            pair.append(pltpu.roll(o, 64, 1) if h % 2 != h // 4 else o)
        parts.append(jnp.where(left, pair[0], pair[1]).astype(jnp.bfloat16))
    copies[6].wait()
    out_ref[...] = dot(jnp.concatenate(parts, axis=1), wo[...]).astype(jnp.bfloat16)


def attention(tokens, lengths, key_cache, value_cache, gate_cache, gain, wq, wk, wv, wf, wo, blocks=8):
    width = tokens.shape[1]
    f32, bf16 = jnp.float32, jnp.bfloat16
    any_space = pl.BlockSpec(memory_space=pl.ANY)
    return pl.pallas_call(
        attention_kernel,
        out_shape=jax.ShapeDtypeStruct((SEQS, width), bf16),
        in_specs=[pl.BlockSpec(memory_space=pltpu.SMEM)] + [any_space] * 10,
        out_specs=pl.BlockSpec(memory_space=pltpu.VMEM),
        scratch_shapes=[
            pltpu.VMEM((SEQS, width), bf16),
            pltpu.VMEM((1, width), f32),
            pltpu.VMEM(wq.shape, bf16),
            pltpu.VMEM(wk.shape, bf16),
            pltpu.VMEM(wv.shape, bf16),
            pltpu.VMEM(wf.shape, bf16),
            pltpu.VMEM(wo.shape, bf16),
            pltpu.VMEM(key_cache.shape, bf16),
            pltpu.VMEM(value_cache.shape, bf16),
            pltpu.VMEM(gate_cache.shape, f32),
            pltpu.VMEM((SEQS * HEADS_HERE, LANES), f32),
            pltpu.VMEM((SEQS * HEADS_HERE, LANES), f32),
            pltpu.VMEM((SEQS * HEADS_HERE, LANES), f32),
            pltpu.VMEM((SEQS, LANES), f32),
            pltpu.VMEM((SEQS * HEADS_HERE, LANES), f32),
            pltpu.SemaphoreType.DMA((7,)),
            pltpu.SemaphoreType.DMA((3, blocks)),
        ],
        compiler_params=pltpu.CompilerParams(vmem_limit_bytes=40 * 1024 * 1024),
        cost_estimate=pl.CostEstimate(flops=500_000_000, bytes_accessed=24_000_000, transcendentals=300_000),
        name="attention",
    )(lengths, tokens, key_cache, value_cache, gate_cache, gain.reshape(1, width), wq, wk, wv, wf, wo)


HD = 64
EXPERTS = 8
CAP = 12


eps = 1e-06


def sent_to_all(x, axis):
    copies = jnp.broadcast_to(x, (lax.axis_size(axis), *x.shape))
    return lax.all_to_all(copies, axis, split_axis=0, concat_axis=0, tiled=True)


def of_everyone(x, axis):
    return sent_to_all(x, axis).astype(jnp.float32).sum(axis=0)


def cut_along(x, dim, size):
    before, after = (x.shape[:dim], x.shape[dim + 1 :])
    return jnp.moveaxis(x.reshape(*before, size, -1, *after), dim, 0)


def sent_and_summed(x, axis, dim):
    size = lax.axis_size(axis)
    tiles = lax.all_to_all(cut_along(x, dim, size), axis, 0, 0, tiled=True)
    return jnp.sum(tiles.astype(jnp.float32), axis=0)


def in_order(tiles, dim):
    dims = list(tiles.shape[1:])
    dims[dim] *= tiles.shape[0]
    return jnp.moveaxis(tiles, 0, dim).reshape(dims)


def collect(x, axis, dim):
    tiles = sent_to_all(x, axis)
    return in_order(tiles, dim)


def normed(values, gain):
    floats = values.astype(jnp.float32)
    return floats * lax.rsqrt(jnp.mean(floats * floats, axis=-1, keepdims=True) + eps) * gain


def expert_work(rows_in, expert_gate, expert_up, expert_down):
    leading = rows_in.shape[:-1]
    flat_rows = rows_in.reshape(-1, rows_in.shape[-1])
    gate_out = jnp.dot(flat_rows, expert_gate, preferred_element_type=jnp.float32)
    up_out = jnp.dot(flat_rows, expert_up, preferred_element_type=jnp.float32)
    hidden = (jax.nn.silu(gate_out) * up_out).astype(jnp.bfloat16)
    return jnp.dot(hidden, expert_down, preferred_element_type=jnp.float32).reshape(
        leading + (expert_down.shape[1],)
    )


def combine(returned, target, route_weights):
    capacity = returned.shape[1]
    columns = returned.shape[2]
    blocks = jnp.sum(
        returned.reshape(EXPERTS, -1, capacity, columns).astype(jnp.float32), axis=1
    ).reshape(EXPERTS * capacity, columns)
    picked = jnp.take(blocks, target, axis=0).reshape(route_weights.shape + (columns,))
    return jnp.sum(picked * route_weights[..., None], axis=1)


def on_device(
    tokens,
    lengths,
    key_cache,
    value_cache,
    gate_cache,
    mix_gain,
    query_weight,
    key_weight,
    value_weight,
    forget_weight,
    out_weight,
    expert_gain,
    routes,
    route_weights,
    expert_gate,
    expert_up,
    expert_down,
):
    width = tokens.shape[1]
    partial_out = attention(
        tokens, lengths, key_cache, value_cache, gate_cache, mix_gain,
        query_weight, key_weight, value_weight, forget_weight, out_weight,
    )
    residual = (
        tokens.astype(jnp.float32) + of_everyone(partial_out, "tp").astype(jnp.float32)
    ).astype(jnp.bfloat16)
    expert_in = normed(residual, expert_gain).astype(jnp.bfloat16)
    top_count = routes.shape[1]
    flat_routes = routes.reshape(-1)
    one_hot = (flat_routes[:, None] == jnp.arange(EXPERTS, dtype=jnp.int32)[None, :]).astype(
        jnp.int32
    )
    slot_index = jnp.sum((jnp.cumsum(one_hot, axis=0) - 1) * one_hot, axis=1)
    target = flat_routes * CAP + slot_index
    dispatch = (jnp.arange(EXPERTS * CAP, dtype=jnp.int32)[:, None] == target[None, :]).astype(
        jnp.bfloat16
    )
    repeated = jnp.repeat(expert_in, top_count, axis=0)
    outgoing = jnp.dot(dispatch, repeated, preferred_element_type=jnp.float32).astype(jnp.bfloat16)
    pieces = lax.axis_size("ep") // EXPERTS
    outgoing = jnp.broadcast_to(
        outgoing.reshape(EXPERTS, 1, CAP, width), (EXPERTS, pieces, CAP, width)
    ).reshape(EXPERTS * pieces, CAP, width)
    half_width = width // lax.axis_size("tp")
    start = lax.axis_index("tp") * half_width
    outgoing_half = lax.dynamic_slice_in_dim(outgoing, start, half_width, 2)
    full_rows = lax.all_gather(
        lax.all_to_all(outgoing_half, "ep", split_axis=0, concat_axis=0, tiled=True),
        "tp",
        axis=2,
        tiled=True,
    )
    partial_rows = expert_work(full_rows, expert_gate, expert_up, expert_down).astype(jnp.bfloat16)
    share = sent_and_summed(partial_rows, "tp", 2).astype(jnp.bfloat16)
    returned = lax.all_to_all(share, "ep", split_axis=0, concat_axis=0, tiled=True)
    mixture = combine(returned, target, route_weights)
    own_half = lax.dynamic_slice_in_dim(residual, start, half_width, 1).astype(jnp.float32)
    return collect((own_half + mixture).astype(jnp.bfloat16), "tp", 1)


def solution(mesh):
    return jax.shard_map(
        on_device,
        mesh=mesh,
        in_specs=(
            P("ep", None),
            P("ep"),
            P("ep", None, "tp"),
            P("ep", None, "tp"),
            P("ep", "tp", None),
            P(),
            P(None, "tp"),
            P(None, "tp"),
            P(None, "tp"),
            P(None, "tp"),
            P("tp", None),
            P(),
            P("ep", None),
            P("ep", None),
            P(None, ("ep", "tp")),
            P(None, ("ep", "tp")),
            P(("ep", "tp"), None),
        ),
        out_specs=P("ep", None),
        check_vma=False,
    )
```

```python
import functools
import jax
import jax.numpy as jnp
from jax import lax
from jax.experimental import pallas as pl
from jax.experimental.pallas import tpu as pltpu
from jax.sharding import PartitionSpec as P

SEQS = 32
POS = 1024
LANES = 128
HEADS_HERE = 8


def rms(values, gain):
    return values * lax.rsqrt(jnp.mean(values * values, axis=-1, keepdims=True) + 1e-06) * gain


def attention_kernel(
    len_ref, tok_hbm, key_hbm, value_hbm, gate_hbm, gain_hbm, wq_hbm, wk_hbm, wv_hbm, wf_hbm, wo_hbm,
    out_ref,
    tok, gain, wq, wk, wv, wf, wo, keys, values, gates, qs, owns, lgs, vnew, mixed, sems, kv_sems,
):
    blocks, per = kv_sems.shape[1], SEQS // kv_sems.shape[1]
    small = [(tok_hbm, tok), (gain_hbm, gain), (wq_hbm, wq), (wk_hbm, wk), (wv_hbm, wv), (wf_hbm, wf), (wo_hbm, wo)]
    copies = [pltpu.make_async_copy(a, b, sems.at[i]) for i, (a, b) in enumerate(small)]

    def block_copies(b):
        rows = pl.ds(b * per, per)
        return [
            pltpu.make_async_copy(src.at[rows], dst.at[rows], kv_sems.at[i, b])
            for i, (src, dst) in enumerate(((key_hbm, keys), (gate_hbm, gates), (value_hbm, values)))
        ]

    for c in copies[:6]:
        c.start()
    for b in range(blocks):
        for c in block_copies(b):
            c.start()
    copies[6].start()

    copies[0].wait()
    copies[1].wait()
    ni = rms(tok[...].astype(jnp.float32), gain[...]).astype(jnp.bfloat16)
    lane = lax.broadcasted_iota(jnp.int32, (SEQS, LANES), 1)
    left = lane < 64
    for c in copies[2:6]:
        c.wait()
    dot = functools.partial(jnp.dot, preferred_element_type=jnp.float32)
    q = dot(ni, wq[...]).astype(jnp.bfloat16).astype(jnp.float32) * 0.125
    kn = dot(ni, wk[...]).astype(jnp.bfloat16).astype(jnp.float32)
    vnew[...] = dot(ni, wv[...]).astype(jnp.bfloat16).astype(jnp.float32)
    f = dot(ni, wf[...])
    lg = jnp.minimum(f, 0.0) - jnp.log1p(jnp.exp(-jnp.abs(f)))
    for h in range(HEADS_HERE):
        column = q[:, 128 * (h // 2) : 128 * (h // 2) + 128]
        if h % 2 != h // 4:
            column = pltpu.roll(column, 64, 1)
        column = jnp.where(left if h < 4 else ~left, column, 0.0)
        rows = pl.ds(h, SEQS, stride=HEADS_HERE)
        qs[rows, :] = column
        owns[rows, :] = jnp.broadcast_to(jnp.sum(column * kn, axis=1, keepdims=True), (SEQS, LANES))
        lgs[rows, :] = jnp.broadcast_to(lg[:, h : h + 1], (SEQS, LANES))

    position = lax.broadcasted_iota(jnp.int32, (HEADS_HERE, POS), 1)

    def block(b, carry):
        for c in block_copies(b):
            c.wait()
        for j in range(per):
            s = b * per + j
            rows = pl.ds(s * HEADS_HERE, HEADS_HERE)
            length = len_ref[s]
            g = gates[s]
            score = lax.dot_general(
                qs[rows, :].astype(jnp.bfloat16), keys[s], (((1,), (1,)), ((), ())),
                preferred_element_type=jnp.float32,
            )
            latest = jnp.sum(jnp.where(position == length - 1, g, 0.0), axis=1, keepdims=True)
            own = owns[rows, 0:1]
            score = jnp.where(position < length, score + (latest + lgs[rows, 0:1]) - g, -jnp.inf)
            top = jnp.maximum(jnp.max(score, axis=1, keepdims=True), own)
            raised = jnp.exp(score - top)
            own_raised = jnp.exp(own - top)
            total = jnp.sum(raised, axis=1, keepdims=True) + own_raised
            o = dot(raised.astype(jnp.bfloat16), values[s])
            mixed[rows, :] = (o + own_raised * vnew[pl.ds(s, 1), :]) / total
        return carry

    lax.fori_loop(0, blocks, block, 0)
    parts = []
    for c in range(4):
        pair = []
        for h in (2 * c, 2 * c + 1):
            o = mixed[pl.ds(h, SEQS, stride=HEADS_HERE), :]
            pair.append(pltpu.roll(o, 64, 1) if h % 2 != h // 4 else o)
        parts.append(jnp.where(left, pair[0], pair[1]).astype(jnp.bfloat16))
    copies[6].wait()
    out_ref[...] = dot(jnp.concatenate(parts, axis=1), wo[...]).astype(jnp.bfloat16)


def attention(tokens, lengths, key_cache, value_cache, gate_cache, gain, wq, wk, wv, wf, wo, blocks=8):
    width = tokens.shape[1]
    f32, bf16 = jnp.float32, jnp.bfloat16
    any_space = pl.BlockSpec(memory_space=pl.ANY)
    return pl.pallas_call(
        attention_kernel,
        out_shape=jax.ShapeDtypeStruct((SEQS, width), bf16),
        in_specs=[pl.BlockSpec(memory_space=pltpu.SMEM)] + [any_space] * 10,
        out_specs=pl.BlockSpec(memory_space=pltpu.VMEM),
        scratch_shapes=[
            pltpu.VMEM((SEQS, width), bf16),
            pltpu.VMEM((1, width), f32),
            pltpu.VMEM(wq.shape, bf16),
            pltpu.VMEM(wk.shape, bf16),
            pltpu.VMEM(wv.shape, bf16),
            pltpu.VMEM(wf.shape, bf16),
            pltpu.VMEM(wo.shape, bf16),
            pltpu.VMEM(key_cache.shape, bf16),
            pltpu.VMEM(value_cache.shape, bf16),
            pltpu.VMEM(gate_cache.shape, f32),
            pltpu.VMEM((SEQS * HEADS_HERE, LANES), f32),
            pltpu.VMEM((SEQS * HEADS_HERE, LANES), f32),
            pltpu.VMEM((SEQS * HEADS_HERE, LANES), f32),
            pltpu.VMEM((SEQS, LANES), f32),
            pltpu.VMEM((SEQS * HEADS_HERE, LANES), f32),
            pltpu.SemaphoreType.DMA((7,)),
            pltpu.SemaphoreType.DMA((3, blocks)),
        ],
        compiler_params=pltpu.CompilerParams(vmem_limit_bytes=60 * 1024 * 1024),
        cost_estimate=pl.CostEstimate(flops=500_000_000, bytes_accessed=24_000_000, transcendentals=300_000),
        name="attention",
    )(lengths, tokens, key_cache, value_cache, gate_cache, gain.reshape(1, width), wq, wk, wv, wf, wo)


MESH = pl.DeviceIdType.MESH
CAP = 12
HALF = 1024
BLOCK = 48
CHUNK = 4 * BLOCK


def moe_kernel(
    part_ref, tok_ref, gain_ref, routes_ref, rw_ref, wg_hbm, wu_hbm, wd_hbm,
    out_ref,
    wg, wu, wd, other_part, res, xe, wts, wtg, xg, cross_out, xf,
    pm, po, pi, ys, ry, zs_out, rxo, rxc, c_out, rc, cf_out, rr, rb, u_out, ur, fo,
    wsem, ss, rs,
):
    f32, bf16 = jnp.float32, jnp.bfloat16
    dot = functools.partial(jnp.dot, preferred_element_type=f32)
    e, t = lax.axis_index("ep"), lax.axis_index("tp")
    z, y, x = e // 16, lax.rem(e // 4, 4), lax.rem(e, 4)
    g = y // 2

    def chip(zz, yy, xx):
        return (zz * 16 + yy * 4 + xx, t)

    partner = (e, 1 - t)
    z_peer = {k: chip(jnp.bitwise_xor(z, k), y, x) for k in (1, 2, 3)}
    x_peer = {k: chip(z, y, jnp.bitwise_xor(x, k)) for k in (1, 2, 3)}
    y_peer = chip(z, jnp.bitwise_xor(y, 1), x)
    y_cross = chip(z, 3 - y, x)
    near = (1, 3, 2)

    loads = [
        pltpu.make_async_copy(wg_hbm, wg, wsem.at[0]),
        pltpu.make_async_copy(wu_hbm, wu, wsem.at[1]),
        pltpu.make_async_copy(wd_hbm.at[:, pl.ds(0, HALF)], wd.at[0], wsem.at[2]),
        pltpu.make_async_copy(wd_hbm.at[:, pl.ds(HALF, HALF)], wd.at[1], wsem.at[3]),
    ]
    for c in loads:
        c.start()

    count = [0]
    started = []

    def send(src, dst, device):
        i = count[0]
        count[0] += 1
        c = pltpu.make_async_remote_copy(
            src_ref=src, dst_ref=dst, send_sem=ss.at[i], recv_sem=rs.at[i], device_id=device, device_id_type=MESH
        )
        c.start()
        started.append(c)
        return c

    barrier = pltpu.get_barrier_semaphore()
    peers = [partner, y_peer, y_cross, *z_peer.values(), *x_peer.values()]
    for p in peers:
        pl.semaphore_signal(barrier, inc=1, device_id=p, device_id_type=MESH)

    rows = tok_ref.shape[0]
    lane = lax.broadcasted_iota(jnp.int32, (rows, LANES), 1)
    upper = lane >= 64
    sub = jnp.where(upper, lane - 64, lane)
    owner = lax.shift_right_logical(sub * 43, 9)
    slot = sub - CAP * owner
    mine = (sub < 4 * CAP) & (owner == z)
    which = jnp.where(upper, 1 - g, g)
    r0, r1 = routes_ref[:, 0:1], routes_ref[:, 1:2]
    w0, w1 = rw_ref[:, 0:1], rw_ref[:, 1:2]
    before = (
        lax.broadcasted_iota(jnp.int32, (rows, rows), 1) < lax.broadcasted_iota(jnp.int32, (rows, rows), 0)
    ).astype(f32).astype(bf16)
    for k in range(4):
        expert = 2 * jnp.bitwise_xor(z, k) + which
        named = jnp.where((r0 == expert) | (r1 == expert), 1.0, 0.0).astype(bf16)
        earlier = dot(before, named)
        here = mine & (named.astype(f32) > 0.5) & (earlier == slot.astype(f32))
        wts[k] = jnp.where(here, jnp.where(r0 == expert, w0, w1), 0.0)
    wtg[0] = wts[0]

    pl.semaphore_wait(barrier, len(peers))
    c_part = send(part_ref, other_part, partner)
    c_wt = {k: send(wts.at[k], wtg.at[k], z_peer[k]) for k in near}

    c_part.wait_recv()
    total = tok_ref[...].astype(f32) + (part_ref[...].astype(f32) + other_part[...].astype(f32))
    res_b = total.astype(bf16)
    res[0] = res_b[:, :HALF]
    res[1] = res_b[:, HALF:]
    expert_in = rms(res_b.astype(f32), gain_ref[...]).astype(bf16)
    xe[0] = expert_in[:, :HALF]
    xe[1] = expert_in[:, HALF:]
    xg[0] = xe[t]
    c_x = {k: send(xg.at[0], xg.at[k], z_peer[k]) for k in near}
    for k in near:
        c_wt[k].wait_recv()
    for k in near:
        c_x[k].wait_recv()

    weights = wtg[...].reshape(4 * rows, LANES)
    picks = jnp.where(weights > 0.0, 1.0, 0.0).astype(bf16)
    packed = lax.dot_general(
        picks, xg[...].reshape(4 * rows, HALF), (((0,), (0,)), ((), ())), preferred_element_type=f32
    ).astype(bf16)
    xf[t, 0, 0] = packed[0:BLOCK]
    cross_out[...] = packed[64 : 64 + BLOCK]

    mine_at = lambda d, q: xf.at[t, d, q]
    fwd = {}

    def forward(d, q):
        fwd[d, q] = send(mine_at(d, q), mine_at(d, q), partner)

    c_cross = send(cross_out, mine_at(0, 2), y_cross)
    c_ax = {d: send(mine_at(0, 0), mine_at(d, 0), x_peer[d]) for d in near}
    c_ay = {0: send(mine_at(0, 0), mine_at(0, 1), y_peer)}
    forward(0, 0)
    c_cross.wait_recv()
    c_by = send(mine_at(0, 2), mine_at(0, 3), y_peer)
    c_bx = {(d, 2): send(mine_at(0, 2), mine_at(d, 2), x_peer[d]) for d in near}
    forward(0, 2)
    for d in (1, 3):
        c_ax[d].wait_recv()
        c_ay[d] = send(mine_at(d, 0), mine_at(d, 1), y_peer)
        forward(d, 0)
    c_ay[0].wait_recv()
    forward(0, 1)
    c_by.wait_recv()
    for d in near:
        c_bx[d, 3] = send(mine_at(0, 3), mine_at(d, 3), x_peer[d])
    forward(0, 3)
    c_ax[2].wait_recv()
    c_ay[2] = send(mine_at(2, 0), mine_at(2, 1), y_peer)
    forward(2, 0)

    for c in loads:
        c.wait()
    c_pi = {}

    def compute(d):
        for q in range(4):
            fwd[d, q].wait_recv()
        x0, x1 = xf[0, d].reshape(CHUNK, HALF), xf[1, d].reshape(CHUNK, HALF)
        gate = dot(x0, wg[0:HALF]) + dot(x1, wg[HALF : 2 * HALF])
        up = dot(x0, wu[0:HALF]) + dot(x1, wu[HALF : 2 * HALF])
        hidden = (gate / (1.0 + jnp.exp(-gate)) * up).astype(bf16)
        po[d] = dot(hidden, wd[1 - t]).astype(bf16)
        c_pi[d] = send(po.at[d], pi.at[d], partner)
        pm[d] = dot(hidden, wd[t])

    c_ry, c_xc, c_xo = {}, {}, {}

    def arrive(d):
        c_bx[d, 2].wait_recv()
        forward(d, 2)
        c_ay[d].wait_recv()
        forward(d, 1)
        c_bx[d, 3].wait_recv()
        forward(d, 3)

    def finish(d):
        c_pi[d].wait_recv()
        ys[d] = (pm[d] + pi[d].astype(f32)).astype(bf16).reshape(4, BLOCK, HALF)
        if d:
            c_xc[d] = send(ys.at[d, pl.ds(2, 2)], rxc.at[d], x_peer[d])
        c_ry[d] = send(ys.at[d, 1], ry.at[d], y_peer)

    def second(d):
        c_ry[d].wait_recv()
        zs_out[d] = (ys[d, 0].astype(f32) + ry[d].astype(f32)).astype(bf16)
        if d:
            c_xo[d] = send(zs_out.at[d], rxo.at[d], x_peer[d])

    compute(0)
    arrive(1)
    compute(1)
    finish(0)
    arrive(3)
    compute(3)
    finish(1)
    second(0)
    arrive(2)
    compute(2)
    finish(3)
    second(1)
    finish(2)
    second(3)
    second(2)

    for d in near:
        c_xc[d].wait_recv()
    crossed = ys[0, 2:4].astype(f32) + rxc[1].astype(f32) + rxc[3].astype(f32) + rxc[2].astype(f32)
    c_out[...] = crossed[1].astype(bf16)
    c_rc = send(c_out, rc, y_peer)
    for d in near:
        c_xo[d].wait_recv()
    own = zs_out[0].astype(f32) + rxo[1].astype(f32) + rxo[3].astype(f32) + rxo[2].astype(f32)
    rb[...] = jnp.zeros(rb.shape, bf16)
    rb[0:BLOCK] = own.astype(bf16)
    c_rc.wait_recv()
    cf_out[...] = (crossed[0] + rc[...].astype(f32)).astype(bf16)
    c_rr = send(cf_out, rr, y_cross)
    high = weights.astype(bf16)
    low = (weights - high.astype(f32)).astype(bf16)
    c_rr.wait_recv()
    rb[64 : 64 + BLOCK] = rr[...]
    back = dot(high, rb[...]) + dot(low, rb[...])
    u_out[...] = back.astype(bf16).reshape(4, rows, HALF)
    c_u = {k: send(u_out.at[k], ur.at[k], z_peer[k]) for k in near}
    mixture = res[t].astype(f32) + back[0:rows]
    for k in near:
        c_u[k].wait_recv()
    mixture = mixture + ur[1].astype(f32) + ur[2].astype(f32) + ur[3].astype(f32)
    fo[t] = mixture.astype(bf16)
    c_fo = send(fo.at[t], fo.at[t], partner)
    c_fo.wait_recv()
    out_ref[:, 0:HALF] = fo[0]
    out_ref[:, HALF : 2 * HALF] = fo[1]
    for c in started:
        c.wait_send()


def moe(partial_out, tokens, gain, routes, route_weights, wg, wu, wd):
    rows, width = tokens.shape
    f32, bf16 = jnp.float32, jnp.bfloat16
    any_space = pl.BlockSpec(memory_space=pl.ANY)
    vmem = pl.BlockSpec(memory_space=pltpu.VMEM)
    blocks = lambda *s: pltpu.VMEM((*s, BLOCK, HALF), bf16)
    return pl.pallas_call(
        moe_kernel,
        out_shape=jax.ShapeDtypeStruct((rows, width), bf16),
        in_specs=[vmem] * 5 + [any_space] * 3,
        out_specs=vmem,
        scratch_shapes=[
            pltpu.VMEM(wg.shape, bf16),
            pltpu.VMEM(wu.shape, bf16),
            pltpu.VMEM((2, wd.shape[0], HALF), bf16),
            pltpu.VMEM((rows, width), bf16),
            pltpu.VMEM((2, rows, HALF), bf16),
            pltpu.VMEM((2, rows, HALF), bf16),
            pltpu.VMEM((4, rows, LANES), f32),
            pltpu.VMEM((4, rows, LANES), f32),
            pltpu.VMEM((4, rows, HALF), bf16),
            blocks(),
            blocks(2, 4, 4),
            pltpu.VMEM((4, CHUNK, HALF), f32),
            pltpu.VMEM((4, CHUNK, HALF), bf16),
            pltpu.VMEM((4, CHUNK, HALF), bf16),
            blocks(4, 4),
            blocks(4),
            blocks(4),
            blocks(4),
            blocks(4, 2),
            blocks(),
            blocks(),
            blocks(),
            blocks(),
            pltpu.VMEM((LANES, HALF), bf16),
            pltpu.VMEM((4, rows, HALF), bf16),
            pltpu.VMEM((4, rows, HALF), bf16),
            pltpu.VMEM((2, rows, HALF), bf16),
            pltpu.SemaphoreType.DMA((4,)),
            pltpu.SemaphoreType.DMA((64,)),
            pltpu.SemaphoreType.DMA((64,)),
        ],
        compiler_params=pltpu.CompilerParams(
            collective_id=0, has_side_effects=True, vmem_limit_bytes=56 * 1024 * 1024
        ),
        cost_estimate=pl.CostEstimate(flops=5_000_000_000, bytes_accessed=8_000_000, transcendentals=400_000),
        name="routed_experts",
    )(partial_out, tokens, gain.reshape(1, width), routes, route_weights, wg, wu, wd)


def on_device(
    tokens, lengths, key_cache, value_cache, gate_cache, mix_gain, query_weight, key_weight, value_weight,
    forget_weight, out_weight, expert_gain, routes, route_weights, expert_gate, expert_up, expert_down,
):
    partial_out = attention(
        tokens, lengths, key_cache, value_cache, gate_cache, mix_gain,
        query_weight, key_weight, value_weight, forget_weight, out_weight,
    )
    return moe(partial_out, tokens, expert_gain, routes, route_weights, expert_gate, expert_up, expert_down)


def solution(mesh):
    return jax.shard_map(
        on_device,
        mesh=mesh,
        in_specs=(
            P("ep", None),
            P("ep"),
            P("ep", None, "tp"),
            P("ep", None, "tp"),
            P("ep", "tp", None),
            P(),
            P(None, "tp"),
            P(None, "tp"),
            P(None, "tp"),
            P(None, "tp"),
            P("tp", None),
            P(),
            P("ep", None),
            P("ep", None),
            P(None, ("ep", "tp")),
            P(None, ("ep", "tp")),
            P(("ep", "tp"), None),
        ),
        out_specs=P("ep", None),
        check_vma=False,
    )
```

```python
import functools
import jax
import jax.numpy as jnp
from jax import lax
from jax.experimental import pallas as pl
from jax.experimental.pallas import tpu as pltpu
from jax.sharding import PartitionSpec as P

SEQS = 32
POS = 1024
LANES = 128
HEADS_HERE = 8


def rms(values, gain):
    return values * lax.rsqrt(jnp.mean(values * values, axis=-1, keepdims=True) + 1e-06) * gain


def attention_kernel(
    len_ref, tok_hbm, key_hbm, value_hbm, gate_hbm, gain_hbm, wq_hbm, wk_hbm, wv_hbm, wf_hbm, wo_hbm,
    out_ref,
    tok, gain, wq, wk, wv, wf, wo, keys, values, gates, qs, owns, lgs, vnew, mixed, sems, kv_sems,
):
    blocks, per = kv_sems.shape[1], SEQS // kv_sems.shape[1]
    small = [(tok_hbm, tok), (gain_hbm, gain), (wq_hbm, wq), (wk_hbm, wk), (wv_hbm, wv), (wf_hbm, wf), (wo_hbm, wo)]
    copies = [pltpu.make_async_copy(a, b, sems.at[i]) for i, (a, b) in enumerate(small)]

    def block_copies(b):
        rows = pl.ds(b * per, per)
        return [
            pltpu.make_async_copy(src.at[rows], dst.at[rows], kv_sems.at[i, b])
            for i, (src, dst) in enumerate(((key_hbm, keys), (gate_hbm, gates), (value_hbm, values)))
        ]

    for c in copies[:6]:
        c.start()
    with jax.named_scope("wait_tok"):
        copies[0].wait()
        copies[1].wait()
    for b in range(2):
        for c in block_copies(b):
            c.start()
    ni = rms(tok[...].astype(jnp.float32), gain[...]).astype(jnp.bfloat16)
    lane = lax.broadcasted_iota(jnp.int32, (SEQS, LANES), 1)
    left = lane < 64
    with jax.named_scope("wait_w"):
        for c in copies[2:6]:
            c.wait()
    for b in range(2, blocks):
        for c in block_copies(b):
            c.start()
    copies[6].start()
    dot = functools.partial(jnp.dot, preferred_element_type=jnp.float32)
    q = dot(ni, wq[...]).astype(jnp.bfloat16).astype(jnp.float32) * 0.125
    kn = dot(ni, wk[...]).astype(jnp.bfloat16).astype(jnp.float32)
    vnew[...] = dot(ni, wv[...]).astype(jnp.bfloat16).astype(jnp.float32)
    f = lax.dot_general(ni, wf[...], (((1,), (1,)), ((), ())), preferred_element_type=jnp.float32)
    lg = jnp.minimum(f, 0.0) - jnp.log1p(jnp.exp(-jnp.abs(f)))
    for h in range(HEADS_HERE):
        column = q[:, 128 * (h // 2) : 128 * (h // 2) + 128]
        if h % 2 != h // 4:
            column = pltpu.roll(column, 64, 1)
        column = jnp.where(left if h < 4 else ~left, column, 0.0)
        rows = pl.ds(h, SEQS, stride=HEADS_HERE)
        qs[rows, :] = column
        owns[rows, :] = jnp.broadcast_to(jnp.sum(column * kn, axis=1, keepdims=True), (SEQS, LANES))
        lgs[rows, :] = jnp.broadcast_to(lg[:, h : h + 1], (SEQS, LANES))

    position = lax.broadcasted_iota(jnp.int32, (HEADS_HERE, POS), 1)

    def block(b, carry):
        with jax.named_scope("wait_kv"):
            for c in block_copies(b):
                c.wait()
        for j in range(per):
            s = b * per + j
            rows = pl.ds(s * HEADS_HERE, HEADS_HERE)
            length = len_ref[s]
            g = gates[s]
            score = lax.dot_general(
                qs[rows, :].astype(jnp.bfloat16), keys[s], (((1,), (1,)), ((), ())),
                preferred_element_type=jnp.float32,
            )
            latest = jnp.sum(jnp.where(position == length - 1, g, 0.0), axis=1, keepdims=True)
            own = owns[rows, 0:1]
            score = jnp.where(position < length, score + (latest + lgs[rows, 0:1]) - g, -jnp.inf)
            top = jnp.maximum(jnp.max(score, axis=1, keepdims=True), own)
            raised = jnp.exp(score - top)
            own_raised = jnp.exp(own - top)
            total = jnp.sum(raised, axis=1, keepdims=True) + own_raised
            o = dot(raised.astype(jnp.bfloat16), values[s])
            mixed[rows, :] = (o + own_raised * vnew[pl.ds(s, 1), :]) / total
        return carry

    with jax.named_scope("loop"):
        lax.fori_loop(0, blocks, block, 0)
    parts = []
    for c in range(4):
        pair = []
        for h in (2 * c, 2 * c + 1):
            o = mixed[pl.ds(h, SEQS, stride=HEADS_HERE), :]
            pair.append(pltpu.roll(o, 64, 1) if h % 2 != h // 4 else o)
        parts.append(jnp.where(left, pair[0], pair[1]).astype(jnp.bfloat16))
    with jax.named_scope("wait_wo"):
        copies[6].wait()
    out_ref[...] = dot(jnp.concatenate(parts, axis=1), wo[...]).astype(jnp.bfloat16)


def attention(tokens, lengths, key_cache, value_cache, gate_cache, gain, wq, wk, wv, wf, wo, blocks=8):
    wf = wf.T
    width = tokens.shape[1]
    f32, bf16 = jnp.float32, jnp.bfloat16
    any_space = pl.BlockSpec(memory_space=pl.ANY)
    return pl.pallas_call(
        attention_kernel,
        out_shape=jax.ShapeDtypeStruct((SEQS, width), bf16),
        in_specs=[pl.BlockSpec(memory_space=pltpu.SMEM)] + [any_space] * 10,
        out_specs=pl.BlockSpec(memory_space=pltpu.VMEM),
        scratch_shapes=[
            pltpu.VMEM((SEQS, width), bf16),
            pltpu.VMEM((1, width), f32),
            pltpu.VMEM(wq.shape, bf16),
            pltpu.VMEM(wk.shape, bf16),
            pltpu.VMEM(wv.shape, bf16),
            pltpu.VMEM(wf.shape, bf16),
            pltpu.VMEM(wo.shape, bf16),
            pltpu.VMEM(key_cache.shape, bf16),
            pltpu.VMEM(value_cache.shape, bf16),
            pltpu.VMEM(gate_cache.shape, f32),
            pltpu.VMEM((SEQS * HEADS_HERE, LANES), f32),
            pltpu.VMEM((SEQS * HEADS_HERE, LANES), f32),
            pltpu.VMEM((SEQS * HEADS_HERE, LANES), f32),
            pltpu.VMEM((SEQS, LANES), f32),
            pltpu.VMEM((SEQS * HEADS_HERE, LANES), f32),
            pltpu.SemaphoreType.DMA((7,)),
            pltpu.SemaphoreType.DMA((3, blocks)),
        ],
        compiler_params=pltpu.CompilerParams(vmem_limit_bytes=60 * 1024 * 1024),
        cost_estimate=pl.CostEstimate(flops=500_000_000, bytes_accessed=24_000_000, transcendentals=300_000),
        name="attention",
    )(lengths, tokens, key_cache, value_cache, gate_cache, gain.reshape(1, width), wq, wk, wv, wf, wo)


MESH = pl.DeviceIdType.MESH
CAP = 12
HALF = 1024
BLOCK = 48
CHUNK = 4 * BLOCK
AX_ORDER = (1, 3, 2)


def moe_kernel(
    part_ref, tok_ref, gain_ref, routes_ref, rw_ref, wg_hbm, wu_hbm, wd_hbm,
    out_ref,
    wg, wu, wd, other_part, res, xe, picks, w_high, w_low, pk, sb, xf,
    pm, po, pi, ys, ry, zs_out, rxo, rxc, c_out, rc, er, rb, fo,
    wsem, ss, rs,
):
    f32, bf16 = jnp.float32, jnp.bfloat16
    dot = functools.partial(jnp.dot, preferred_element_type=f32)
    e, t = lax.axis_index("ep"), lax.axis_index("tp")
    z, y, x = e // 16, lax.rem(e // 4, 4), lax.rem(e, 4)
    g = y // 2

    def chip(zz, yy, xx):
        return (zz * 16 + yy * 4 + xx, t)

    partner = (e, 1 - t)
    z_peer = {k: chip(jnp.bitwise_xor(z, k), y, x) for k in (1, 2, 3)}
    x_peer = {k: chip(z, y, jnp.bitwise_xor(x, k)) for k in (1, 2, 3)}
    y_peer = chip(z, jnp.bitwise_xor(y, 1), x)
    z_cross = {k: chip(jnp.bitwise_xor(z, k), 3 - y, x) for k in range(4)}
    near = (1, 3, 2)

    loads = [
        pltpu.make_async_copy(wg_hbm, wg, wsem.at[0]),
        pltpu.make_async_copy(wu_hbm, wu, wsem.at[1]),
        pltpu.make_async_copy(wd_hbm.at[:, pl.ds(0, HALF)], wd.at[0], wsem.at[2]),
        pltpu.make_async_copy(wd_hbm.at[:, pl.ds(HALF, HALF)], wd.at[1], wsem.at[3]),
    ]
    for c in loads:
        c.start()

    count = [0]
    started = []

    def send(src, dst, device):
        i = count[0]
        count[0] += 1
        c = pltpu.make_async_remote_copy(
            src_ref=src, dst_ref=dst, send_sem=ss.at[i], recv_sem=rs.at[i], device_id=device, device_id_type=MESH
        )
        c.start()
        started.append(c)
        return c

    barrier = pltpu.get_barrier_semaphore()
    peers = [partner, y_peer, *z_peer.values(), *z_cross.values(), *x_peer.values()]
    for p in peers:
        pl.semaphore_signal(barrier, inc=1, device_id=p, device_id_type=MESH)

    rows = tok_ref.shape[0]
    lane = lax.broadcasted_iota(jnp.int32, (rows, LANES), 1)
    place = jnp.bitwise_and(lane, 15)
    plane = jnp.bitwise_xor(z, jnp.bitwise_and(lax.shift_right_logical(lane, 4), 3))
    expert = (2 * plane + jnp.where(lane < 64, g, 1 - g)).astype(f32)
    ahead = lax.broadcasted_iota(jnp.int32, (rows, rows), 1)
    behind = lax.broadcasted_iota(jnp.int32, (rows, rows), 0)
    before = (ahead < behind).astype(f32).astype(bf16)
    unit = (ahead == behind).astype(f32)
    upright = lambda v: lax.dot_general(
        unit, v, (((1,), (1,)), ((), ())), precision=lax.Precision.HIGHEST, preferred_element_type=f32
    )
    named_here, weight_here = upright(routes_ref[...].astype(f32)), upright(rw_ref[...])
    first, second_one = named_here[:, 0:1] == expert, named_here[:, 1:2] == expert
    named = first | second_one
    earlier = dot(before, jnp.where(named, 1.0, 0.0).astype(bf16))
    here = named & (place < CAP) & (earlier == place.astype(f32))
    picks[...] = jnp.where(here, 1.0, 0.0).astype(bf16)
    weights = jnp.where(here, jnp.where(first, weight_here[:, 0:1], weight_here[:, 1:2]), 0.0)
    high = weights.astype(bf16)
    w_high[...] = high
    w_low[...] = (weights - high.astype(f32)).astype(bf16)

    pl.semaphore_wait(barrier, len(peers))
    c_part = send(part_ref, other_part, partner)

    c_part.wait_recv()
    total = tok_ref[...].astype(f32) + (part_ref[...].astype(f32) + other_part[...].astype(f32))
    res_b = total.astype(bf16)
    res[0] = res_b[:, :HALF]
    res[1] = res_b[:, HALF:]
    expert_in = rms(res_b.astype(f32), gain_ref[...]).astype(bf16)
    xe[0] = expert_in[:, :HALF]
    xe[1] = expert_in[:, HALF:]
    pk[...] = lax.dot_general(
        picks[...], xe[t], (((0,), (0,)), ((), ())), preferred_element_type=f32
    ).astype(bf16).reshape(8, 16, HALF)
    sb[0, 0] = pk[0]
    c_s0 = {k: send(pk.at[k], sb.at[0, k], z_peer[k]) for k in near}
    c_s1 = {k: send(pk.at[4 + k], sb.at[1, k], z_cross[k]) for k in (0, 1, 3, 2)}
    r_i = lax.broadcasted_iota(jnp.int32, (BLOCK, 64), 0)
    c_i = lax.broadcasted_iota(jnp.int32, (BLOCK, 64), 1)
    r_k = lax.shift_right_logical(r_i * 43, 9)
    tight = (c_i == 16 * r_k + (r_i - CAP * r_k)).astype(f32).astype(bf16)

    mine_at = lambda d, q: xf.at[t, d, q]
    fwd = {}

    def forward(d, q):
        fwd[d, q] = send(mine_at(d, q), mine_at(d, q), partner)

    for k in near:
        c_s0[k].wait_recv()
    xf[t, 0, 0] = dot(tight, sb[0].reshape(64, HALF)).astype(bf16)
    c_ax = {d: send(mine_at(0, 0), mine_at(d, 0), x_peer[d]) for d in AX_ORDER}
    c_ay = {0: send(mine_at(0, 0), mine_at(0, 1), y_peer)}
    forward(0, 0)
    for k in (0, 1, 3, 2):
        c_s1[k].wait_recv()
    xf[t, 0, 2] = dot(tight, sb[1].reshape(64, HALF)).astype(bf16)
    c_by = send(mine_at(0, 2), mine_at(0, 3), y_peer)
    c_bx = {(d, 2): send(mine_at(0, 2), mine_at(d, 2), x_peer[d]) for d in AX_ORDER}
    forward(0, 2)
    for d in AX_ORDER[:2]:
        c_ax[d].wait_recv()
        c_ay[d] = send(mine_at(d, 0), mine_at(d, 1), y_peer)
        forward(d, 0)
    c_ay[0].wait_recv()
    forward(0, 1)
    c_by.wait_recv()
    for d in AX_ORDER:
        c_bx[d, 3] = send(mine_at(0, 3), mine_at(d, 3), x_peer[d])
    forward(0, 3)
    d = AX_ORDER[2]
    c_ax[d].wait_recv()
    c_ay[d] = send(mine_at(d, 0), mine_at(d, 1), y_peer)
    forward(d, 0)

    for c in loads:
        c.wait()
    c_pi = {}

    def compute(d):
        for q in range(4):
            fwd[d, q].wait_recv()
        x0, x1 = xf[0, d].reshape(CHUNK, HALF), xf[1, d].reshape(CHUNK, HALF)
        gate = dot(x0, wg[0:HALF]) + dot(x1, wg[HALF : 2 * HALF])
        up = dot(x0, wu[0:HALF]) + dot(x1, wu[HALF : 2 * HALF])
        hidden = (gate / (1.0 + jnp.exp(-gate)) * up).astype(bf16)
        po[d] = dot(hidden, wd[1 - t]).astype(bf16)
        c_pi[d] = send(po.at[d], pi.at[d], partner)
        pm[d] = dot(hidden, wd[t])

    c_ry, c_xc, c_xo = {}, {}, {}

    def arrive(d):
        c_bx[d, 2].wait_recv()
        forward(d, 2)
        c_ay[d].wait_recv()
        forward(d, 1)
        c_bx[d, 3].wait_recv()
        forward(d, 3)

    def finish(d):
        c_pi[d].wait_recv()
        ys[d] = (pm[d] + pi[d].astype(f32)).astype(bf16).reshape(4, BLOCK, HALF)
        if d:
            c_xc[d] = send(ys.at[d, pl.ds(2, 2)], rxc.at[d], x_peer[d])
        c_ry[d] = send(ys.at[d, 1], ry.at[d], y_peer)

    def second(d):
        c_ry[d].wait_recv()
        zs_out[d] = (ys[d, 0].astype(f32) + ry[d].astype(f32)).astype(bf16)
        if d:
            c_xo[d] = send(zs_out.at[d], rxo.at[d], x_peer[d])

    compute(0)
    arrive(1)
    compute(1)
    finish(0)
    arrive(3)
    compute(3)
    finish(1)
    second(0)
    arrive(2)
    compute(2)
    finish(3)
    second(1)
    finish(2)
    second(3)
    second(2)

    for d in near:
        c_xc[d].wait_recv()
    crossed = ys[0, 2:4].astype(f32) + rxc[1].astype(f32) + rxc[3].astype(f32) + rxc[2].astype(f32)
    c_out[...] = crossed[1].astype(bf16)
    c_rc = send(c_out, rc, y_peer)
    spread = lambda v: lax.dot_general(
        tight, v.astype(bf16), (((0,), (0,)), ((), ())), preferred_element_type=f32
    ).astype(bf16).reshape(4, 16, HALF)
    for d in near:
        c_xo[d].wait_recv()
    own = zs_out[0].astype(f32) + rxo[1].astype(f32) + rxo[3].astype(f32) + rxo[2].astype(f32)
    er[0] = spread(own)
    rb[0, 0] = er[0, 0]
    c_r0 = {k: send(er.at[0, k], rb.at[0, k], z_peer[k]) for k in near}
    c_rc.wait_recv()
    er[1] = spread(crossed[0] + rc[...].astype(f32))
    c_r1 = {k: send(er.at[1, k], rb.at[1, k], z_cross[k]) for k in (2, 1, 3, 0)}
    for k in near:
        c_r0[k].wait_recv()
    for k in (2, 1, 3, 0):
        c_r1[k].wait_recv()
    returned = rb[...].reshape(LANES, HALF)
    mixture = res[t].astype(f32) + dot(w_high[...], returned) + dot(w_low[...], returned)
    fo[t] = mixture.astype(bf16)
    c_fo = send(fo.at[t], fo.at[t], partner)
    c_fo.wait_recv()
    out_ref[:, 0:HALF] = fo[0]
    out_ref[:, HALF : 2 * HALF] = fo[1]
    for c in started:
        c.wait_send()


def moe(partial_out, tokens, gain, routes, route_weights, wg, wu, wd):
    rows, width = tokens.shape
    f32, bf16 = jnp.float32, jnp.bfloat16
    any_space = pl.BlockSpec(memory_space=pl.ANY)
    vmem = pl.BlockSpec(memory_space=pltpu.VMEM)
    blocks = lambda *s: pltpu.VMEM((*s, BLOCK, HALF), bf16)
    return pl.pallas_call(
        moe_kernel,
        out_shape=jax.ShapeDtypeStruct((rows, width), bf16),
        in_specs=[vmem] * 5 + [any_space] * 3,
        out_specs=vmem,
        scratch_shapes=[
            pltpu.VMEM(wg.shape, bf16),
            pltpu.VMEM(wu.shape, bf16),
            pltpu.VMEM((2, wd.shape[0], HALF), bf16),
            pltpu.VMEM((rows, width), bf16),
            pltpu.VMEM((2, rows, HALF), bf16),
            pltpu.VMEM((2, rows, HALF), bf16),
            pltpu.VMEM((rows, LANES), bf16),
            pltpu.VMEM((rows, LANES), bf16),
            pltpu.VMEM((rows, LANES), bf16),
            pltpu.VMEM((8, 16, HALF), bf16),
            pltpu.VMEM((2, 4, 16, HALF), bf16),
            blocks(2, 4, 4),
            pltpu.VMEM((4, CHUNK, HALF), f32),
            pltpu.VMEM((4, CHUNK, HALF), bf16),
            pltpu.VMEM((4, CHUNK, HALF), bf16),
            blocks(4, 4),
            blocks(4),
            blocks(4),
            blocks(4),
            blocks(4, 2),
            blocks(),
            blocks(),
            pltpu.VMEM((2, 4, 16, HALF), bf16),
            pltpu.VMEM((2, 4, 16, HALF), bf16),
            pltpu.VMEM((2, rows, HALF), bf16),
            pltpu.SemaphoreType.DMA((4,)),
            pltpu.SemaphoreType.DMA((64,)),
            pltpu.SemaphoreType.DMA((64,)),
        ],
        compiler_params=pltpu.CompilerParams(
            collective_id=0, has_side_effects=True, vmem_limit_bytes=56 * 1024 * 1024
        ),
        cost_estimate=pl.CostEstimate(flops=5_000_000_000, bytes_accessed=8_000_000, transcendentals=400_000),
        name="routed_experts",
    )(partial_out, tokens, gain.reshape(1, width), routes.T, route_weights.T, wg, wu, wd)


def on_device(
    tokens, lengths, key_cache, value_cache, gate_cache, mix_gain, query_weight, key_weight, value_weight,
    forget_weight, out_weight, expert_gain, routes, route_weights, expert_gate, expert_up, expert_down,
):
    partial_out = attention(
        tokens, lengths, key_cache, value_cache, gate_cache, mix_gain,
        query_weight, key_weight, value_weight, forget_weight, out_weight,
    )
    return moe(partial_out, tokens, expert_gain, routes, route_weights, expert_gate, expert_up, expert_down)


def solution(mesh):
    return jax.shard_map(
        on_device,
        mesh=mesh,
        in_specs=(
            P("ep", None),
            P("ep"),
            P("ep", None, "tp"),
            P("ep", None, "tp"),
            P("ep", "tp", None),
            P(),
            P(None, "tp"),
            P(None, "tp"),
            P(None, "tp"),
            P(None, "tp"),
            P("tp", None),
            P(),
            P("ep", None),
            P("ep", None),
            P(None, ("ep", "tp")),
            P(None, ("ep", "tp")),
            P(("ep", "tp"), None),
        ),
        out_specs=P("ep", None),
        check_vma=False,
    )
```

```python
import functools
import jax
import jax.numpy as jnp
from jax import lax
from jax.experimental import pallas as pl
from jax.experimental.pallas import tpu as pltpu
from jax.sharding import PartitionSpec as P

SEQS = 32
POS = 1024
LANES = 128
HEADS_HERE = 8


def rms(values, gain):
    return values * lax.rsqrt(jnp.mean(values * values, axis=-1, keepdims=True) + 1e-06) * gain


def attention_kernel(
    len_ref, tok_hbm, key_hbm, value_hbm, gate_hbm, gain_hbm, wq_hbm, wk_hbm, wv_hbm, wf_hbm, wo_hbm,
    out_ref,
    tok, gain, wq, wk, wv, wf, wo, keys, values, gates, qs, owns, lgs, vnew, mixed, sems, kv_sems,
):
    blocks, per = kv_sems.shape[1], SEQS // kv_sems.shape[1]
    small = [(tok_hbm, tok), (gain_hbm, gain), (wq_hbm, wq), (wk_hbm, wk), (wv_hbm, wv), (wf_hbm, wf), (wo_hbm, wo)]
    copies = [pltpu.make_async_copy(a, b, sems.at[i]) for i, (a, b) in enumerate(small)]

    def block_copies(b):
        rows = pl.ds(b * per, per)
        return [
            pltpu.make_async_copy(src.at[rows], dst.at[rows], kv_sems.at[i, b])
            for i, (src, dst) in enumerate(((key_hbm, keys), (gate_hbm, gates), (value_hbm, values)))
        ]

    for c in copies[:6]:
        c.start()
    with jax.named_scope("wait_tok"):
        copies[0].wait()
        copies[1].wait()
    for b in range(2):
        for c in block_copies(b):
            c.start()
    ni = rms(tok[...].astype(jnp.float32), gain[...]).astype(jnp.bfloat16)
    lane = lax.broadcasted_iota(jnp.int32, (SEQS, LANES), 1)
    left = lane < 64
    with jax.named_scope("wait_w"):
        for c in copies[2:6]:
            c.wait()
    for b in range(2, blocks):
        for c in block_copies(b):
            c.start()
    copies[6].start()
    dot = functools.partial(jnp.dot, preferred_element_type=jnp.float32)
    q = dot(ni, wq[...]).astype(jnp.bfloat16).astype(jnp.float32) * 0.125
    kn = dot(ni, wk[...]).astype(jnp.bfloat16).astype(jnp.float32)
    vnew[...] = dot(ni, wv[...]).astype(jnp.bfloat16).astype(jnp.float32)
    f = lax.dot_general(ni, wf[...], (((1,), (1,)), ((), ())), preferred_element_type=jnp.float32)
    lg = jnp.minimum(f, 0.0) - jnp.log1p(jnp.exp(-jnp.abs(f)))
    for h in range(HEADS_HERE):
        column = q[:, 128 * (h // 2) : 128 * (h // 2) + 128]
        if h % 2 != h // 4:
            column = pltpu.roll(column, 64, 1)
        column = jnp.where(left if h < 4 else ~left, column, 0.0)
        rows = pl.ds(h, SEQS, stride=HEADS_HERE)
        qs[rows, :] = column
        owns[rows, :] = jnp.broadcast_to(jnp.sum(column * kn, axis=1, keepdims=True), (SEQS, LANES))
        lgs[rows, :] = jnp.broadcast_to(lg[:, h : h + 1], (SEQS, LANES))

    position = lax.broadcasted_iota(jnp.int32, (HEADS_HERE, POS), 1)

    def block(b, carry):
        with jax.named_scope("wait_kv"):
            for c in block_copies(b):
                c.wait()
        seqs = [b * per + j for j in range(per)]
        rows = [pl.ds(s * HEADS_HERE, HEADS_HERE) for s in seqs]
        scores = [
            lax.dot_general(
                qs[r, :].astype(jnp.bfloat16), keys[s], (((1,), (1,)), ((), ())),
                preferred_element_type=jnp.float32,
            )
            for s, r in zip(seqs, rows)
        ]
        raised, scale, own_part = [], [], []
        for s, r, score in zip(seqs, rows, scores):
            length = len_ref[s]
            g = gates[s]
            latest = jnp.sum(jnp.where(position == length - 1, g, 0.0), axis=1, keepdims=True)
            own = owns[r, 0:1]
            score = jnp.where(position < length, score + (latest + lgs[r, 0:1]) - g, -jnp.inf)
            top = jnp.maximum(jnp.max(score, axis=1, keepdims=True), own)
            lifted = jnp.exp(score - top)
            own_raised = jnp.exp(own - top)
            raised.append(lifted.astype(jnp.bfloat16))
            scale.append(1.0 / (jnp.sum(lifted, axis=1, keepdims=True) + own_raised))
            own_part.append(own_raised * vnew[pl.ds(s, 1), :])
        sums = [dot(p, values[s]) for p, s in zip(raised, seqs)]
        for r, o, c, w in zip(rows, sums, scale, own_part):
            mixed[r, :] = (o + w) * c
        return carry

    with jax.named_scope("loop"):
        lax.fori_loop(0, blocks, block, 0)
    parts = []
    for c in range(4):
        pair = []
        for h in (2 * c, 2 * c + 1):
            o = mixed[pl.ds(h, SEQS, stride=HEADS_HERE), :]
            pair.append(pltpu.roll(o, 64, 1) if h % 2 != h // 4 else o)
        parts.append(jnp.where(left, pair[0], pair[1]).astype(jnp.bfloat16))
    with jax.named_scope("wait_wo"):
        copies[6].wait()
    out_ref[...] = dot(jnp.concatenate(parts, axis=1), wo[...]).astype(jnp.bfloat16)


def attention(tokens, lengths, key_cache, value_cache, gate_cache, gain, wq, wk, wv, wf, wo, blocks=4):
    wf = wf.T
    width = tokens.shape[1]
    f32, bf16 = jnp.float32, jnp.bfloat16
    any_space = pl.BlockSpec(memory_space=pl.ANY)
    return pl.pallas_call(
        attention_kernel,
        out_shape=jax.ShapeDtypeStruct((SEQS, width), bf16),
        in_specs=[pl.BlockSpec(memory_space=pltpu.SMEM)] + [any_space] * 10,
        out_specs=pl.BlockSpec(memory_space=pltpu.VMEM),
        scratch_shapes=[
            pltpu.VMEM((SEQS, width), bf16),
            pltpu.VMEM((1, width), f32),
            pltpu.VMEM(wq.shape, bf16),
            pltpu.VMEM(wk.shape, bf16),
            pltpu.VMEM(wv.shape, bf16),
            pltpu.VMEM(wf.shape, bf16),
            pltpu.VMEM(wo.shape, bf16),
            pltpu.VMEM(key_cache.shape, bf16),
            pltpu.VMEM(value_cache.shape, bf16),
            pltpu.VMEM(gate_cache.shape, f32),
            pltpu.VMEM((SEQS * HEADS_HERE, LANES), f32),
            pltpu.VMEM((SEQS * HEADS_HERE, LANES), f32),
            pltpu.VMEM((SEQS * HEADS_HERE, LANES), f32),
            pltpu.VMEM((SEQS, LANES), f32),
            pltpu.VMEM((SEQS * HEADS_HERE, LANES), f32),
            pltpu.SemaphoreType.DMA((7,)),
            pltpu.SemaphoreType.DMA((3, blocks)),
        ],
        compiler_params=pltpu.CompilerParams(vmem_limit_bytes=60 * 1024 * 1024),
        cost_estimate=pl.CostEstimate(flops=500_000_000, bytes_accessed=24_000_000, transcendentals=300_000),
        name="attention",
    )(lengths, tokens, key_cache, value_cache, gate_cache, gain.reshape(1, width), wq, wk, wv, wf, wo)


MESH = pl.DeviceIdType.MESH
CAP = 12
HALF = 1024
BLOCK = 48
CHUNK = 4 * BLOCK
AX_ORDER = (2, 1, 3)


def moe_kernel(
    part_ref, tok_ref, gain_ref, routes_ref, rw_ref, wg_hbm, wu_hbm, wd_hbm,
    out_ref,
    wg, wu, wd, other_part, res, xe, picks, w_high, w_low, pk, sb, xf,
    pm, po, pi, ys, ry, zs_out, rxo, rxc, c_out, rc, er, rb, fo,
    wsem, ss, rs,
):
    f32, bf16 = jnp.float32, jnp.bfloat16
    dot = functools.partial(jnp.dot, preferred_element_type=f32)
    e, t = lax.axis_index("ep"), lax.axis_index("tp")
    z, y, x = e // 16, lax.rem(e // 4, 4), lax.rem(e, 4)
    g = y // 2

    def chip(zz, yy, xx):
        return (zz * 16 + yy * 4 + xx, t)

    partner = (e, 1 - t)
    z_peer = {k: chip(jnp.bitwise_xor(z, k), y, x) for k in (1, 2, 3)}
    x_peer = {k: chip(z, y, jnp.bitwise_xor(x, k)) for k in (1, 2, 3)}
    y_peer = chip(z, jnp.bitwise_xor(y, 1), x)
    z_cross = {k: chip(jnp.bitwise_xor(z, k), 3 - y, x) for k in range(4)}
    near = (1, 3, 2)

    loads = [
        pltpu.make_async_copy(wg_hbm, wg, wsem.at[0]),
        pltpu.make_async_copy(wu_hbm, wu, wsem.at[1]),
        pltpu.make_async_copy(wd_hbm.at[:, pl.ds(0, HALF)], wd.at[0], wsem.at[2]),
        pltpu.make_async_copy(wd_hbm.at[:, pl.ds(HALF, HALF)], wd.at[1], wsem.at[3]),
    ]
    for c in loads:
        c.start()

    count = [0]
    started = []

    def send(src, dst, device):
        i = count[0]
        count[0] += 1
        c = pltpu.make_async_remote_copy(
            src_ref=src, dst_ref=dst, send_sem=ss.at[i], recv_sem=rs.at[i], device_id=device, device_id_type=MESH
        )
        c.start()
        started.append(c)
        return c

    barrier = pltpu.get_barrier_semaphore()
    peers = [partner, y_peer, *z_peer.values(), *z_cross.values(), *x_peer.values()]
    for p in peers:
        pl.semaphore_signal(barrier, inc=1, device_id=p, device_id_type=MESH)

    rows = tok_ref.shape[0]
    lane = lax.broadcasted_iota(jnp.int32, (rows, LANES), 1)
    place = jnp.bitwise_and(lane, 15)
    plane = jnp.bitwise_xor(z, jnp.bitwise_and(lax.shift_right_logical(lane, 4), 3))
    expert = (2 * plane + jnp.where(lane < 64, g, 1 - g)).astype(f32)
    ahead = lax.broadcasted_iota(jnp.int32, (rows, rows), 1)
    behind = lax.broadcasted_iota(jnp.int32, (rows, rows), 0)
    before = (ahead < behind).astype(f32).astype(bf16)
    unit = (ahead == behind).astype(f32)
    upright = lambda v: lax.dot_general(
        unit, v, (((1,), (1,)), ((), ())), precision=lax.Precision.HIGHEST, preferred_element_type=f32
    )
    named_here, weight_here = upright(routes_ref[...].astype(f32)), upright(rw_ref[...])
    first, second_one = named_here[:, 0:1] == expert, named_here[:, 1:2] == expert
    named = first | second_one
    earlier = dot(before, jnp.where(named, 1.0, 0.0).astype(bf16))
    here = named & (place < CAP) & (earlier == place.astype(f32))
    picks[...] = jnp.where(here, 1.0, 0.0).astype(bf16)
    weights = jnp.where(here, jnp.where(first, weight_here[:, 0:1], weight_here[:, 1:2]), 0.0)
    high = weights.astype(bf16)
    w_high[...] = high
    w_low[...] = (weights - high.astype(f32)).astype(bf16)

    pl.semaphore_wait(barrier, len(peers))
    c_part = send(part_ref, other_part, partner)

    c_part.wait_recv()
    total = tok_ref[...].astype(f32) + (part_ref[...].astype(f32) + other_part[...].astype(f32))
    res_b = total.astype(bf16)
    res[0] = res_b[:, :HALF]
    res[1] = res_b[:, HALF:]
    expert_in = rms(res_b.astype(f32), gain_ref[...]).astype(bf16)
    xe[0] = expert_in[:, :HALF]
    xe[1] = expert_in[:, HALF:]
    pk[...] = lax.dot_general(
        picks[...], xe[t], (((0,), (0,)), ((), ())), preferred_element_type=f32
    ).astype(bf16).reshape(8, 16, HALF)
    sb[0, 0] = pk[0]
    c_s0 = {k: send(pk.at[k], sb.at[0, k], z_peer[k]) for k in near}
    c_s1 = {k: send(pk.at[4 + k], sb.at[1, k], z_cross[k]) for k in (0, 1, 3, 2)}
    r_i = lax.broadcasted_iota(jnp.int32, (BLOCK, 64), 0)
    c_i = lax.broadcasted_iota(jnp.int32, (BLOCK, 64), 1)
    r_k = lax.shift_right_logical(r_i * 43, 9)
    tight = (c_i == 16 * r_k + (r_i - CAP * r_k)).astype(f32).astype(bf16)

    mine_at = lambda d, q: xf.at[t, d, q]
    fwd = {}

    def forward(d, q):
        fwd[d, q] = send(mine_at(d, q), mine_at(d, q), partner)

    for k in near:
        c_s0[k].wait_recv()
    xf[t, 0, 0] = dot(tight, sb[0].reshape(64, HALF)).astype(bf16)
    c_ax = {d: send(mine_at(0, 0), mine_at(d, 0), x_peer[d]) for d in AX_ORDER}
    c_ay = {0: send(mine_at(0, 0), mine_at(0, 1), y_peer)}
    forward(0, 0)
    for k in (0, 1, 3, 2):
        c_s1[k].wait_recv()
    xf[t, 0, 2] = dot(tight, sb[1].reshape(64, HALF)).astype(bf16)
    c_by = send(mine_at(0, 2), mine_at(0, 3), y_peer)
    c_bx = {(d, 2): send(mine_at(0, 2), mine_at(d, 2), x_peer[d]) for d in AX_ORDER}
    forward(0, 2)
    for d in AX_ORDER[:2]:
        c_ax[d].wait_recv()
        c_ay[d] = send(mine_at(d, 0), mine_at(d, 1), y_peer)
        forward(d, 0)
    c_ay[0].wait_recv()
    forward(0, 1)
    c_by.wait_recv()
    for d in AX_ORDER:
        c_bx[d, 3] = send(mine_at(0, 3), mine_at(d, 3), x_peer[d])
    forward(0, 3)
    d = AX_ORDER[2]
    c_ax[d].wait_recv()
    c_ay[d] = send(mine_at(d, 0), mine_at(d, 1), y_peer)
    forward(d, 0)

    for c in loads:
        c.wait()
    c_pi = {}

    def compute(d):
        for q in range(4):
            fwd[d, q].wait_recv()
        x0, x1 = xf[0, d].reshape(CHUNK, HALF), xf[1, d].reshape(CHUNK, HALF)
        gate = dot(x0, wg[0:HALF]) + dot(x1, wg[HALF : 2 * HALF])
        up = dot(x0, wu[0:HALF]) + dot(x1, wu[HALF : 2 * HALF])
        hidden = (gate / (1.0 + jnp.exp(-gate)) * up).astype(bf16)
        po[d] = dot(hidden, wd[1 - t]).astype(bf16)
        c_pi[d] = send(po.at[d], pi.at[d], partner)
        pm[d] = dot(hidden, wd[t])

    c_ry, c_xc, c_xo = {}, {}, {}

    def arrive(d):
        c_bx[d, 2].wait_recv()
        forward(d, 2)
        c_ay[d].wait_recv()
        forward(d, 1)
        c_bx[d, 3].wait_recv()
        forward(d, 3)

    def finish(d):
        c_pi[d].wait_recv()
        ys[d] = (pm[d] + pi[d].astype(f32)).astype(bf16).reshape(4, BLOCK, HALF)
        if d:
            c_xc[d] = send(ys.at[d, pl.ds(2, 2)], rxc.at[d], x_peer[d])
        c_ry[d] = send(ys.at[d, 1], ry.at[d], y_peer)

    def second(d):
        c_ry[d].wait_recv()
        zs_out[d] = (ys[d, 0].astype(f32) + ry[d].astype(f32)).astype(bf16)
        if d:
            c_xo[d] = send(zs_out.at[d], rxo.at[d], x_peer[d])

    compute(0)
    arrive(2)
    arrive(1)
    compute(2)
    finish(0)
    arrive(3)
    compute(1)
    finish(2)
    compute(3)
    second(2)
    finish(1)
    finish(3)
    second(1)
    second(3)
    second(0)

    for d in near:
        c_xc[d].wait_recv()
    crossed = ys[0, 2:4].astype(f32) + rxc[1].astype(f32) + rxc[3].astype(f32) + rxc[2].astype(f32)
    c_out[...] = crossed[1].astype(bf16)
    c_rc = send(c_out, rc, y_peer)
    spread = lambda v: lax.dot_general(
        tight, v.astype(bf16), (((0,), (0,)), ((), ())), preferred_element_type=f32
    ).astype(bf16).reshape(4, 16, HALF)
    for d in near:
        c_xo[d].wait_recv()
    own = zs_out[0].astype(f32) + rxo[1].astype(f32) + rxo[3].astype(f32) + rxo[2].astype(f32)
    er[0] = spread(own)
    rb[0, 0] = er[0, 0]
    c_r0 = {k: send(er.at[0, k], rb.at[0, k], z_peer[k]) for k in near}
    c_rc.wait_recv()
    er[1] = spread(crossed[0] + rc[...].astype(f32))
    c_r1 = {k: send(er.at[1, k], rb.at[1, k], z_cross[k]) for k in (2, 1, 3, 0)}
    for k in near:
        c_r0[k].wait_recv()
    for k in (2, 1, 3, 0):
        c_r1[k].wait_recv()
    returned = rb[...].reshape(LANES, HALF)
    mixture = res[t].astype(f32) + dot(w_high[...], returned) + dot(w_low[...], returned)
    fo[t] = mixture.astype(bf16)
    c_fo = send(fo.at[t], fo.at[t], partner)
    c_fo.wait_recv()
    out_ref[:, 0:HALF] = fo[0]
    out_ref[:, HALF : 2 * HALF] = fo[1]
    for c in started:
        c.wait_send()


def moe(partial_out, tokens, gain, routes, route_weights, wg, wu, wd):
    rows, width = tokens.shape
    f32, bf16 = jnp.float32, jnp.bfloat16
    any_space = pl.BlockSpec(memory_space=pl.ANY)
    vmem = pl.BlockSpec(memory_space=pltpu.VMEM)
    blocks = lambda *s: pltpu.VMEM((*s, BLOCK, HALF), bf16)
    return pl.pallas_call(
        moe_kernel,
        out_shape=jax.ShapeDtypeStruct((rows, width), bf16),
        in_specs=[vmem] * 5 + [any_space] * 3,
        out_specs=vmem,
        scratch_shapes=[
            pltpu.VMEM(wg.shape, bf16),
            pltpu.VMEM(wu.shape, bf16),
            pltpu.VMEM((2, wd.shape[0], HALF), bf16),
            pltpu.VMEM((rows, width), bf16),
            pltpu.VMEM((2, rows, HALF), bf16),
            pltpu.VMEM((2, rows, HALF), bf16),
            pltpu.VMEM((rows, LANES), bf16),
            pltpu.VMEM((rows, LANES), bf16),
            pltpu.VMEM((rows, LANES), bf16),
            pltpu.VMEM((8, 16, HALF), bf16),
            pltpu.VMEM((2, 4, 16, HALF), bf16),
            blocks(2, 4, 4),
            pltpu.VMEM((4, CHUNK, HALF), f32),
            pltpu.VMEM((4, CHUNK, HALF), bf16),
            pltpu.VMEM((4, CHUNK, HALF), bf16),
            blocks(4, 4),
            blocks(4),
            blocks(4),
            blocks(4),
            blocks(4, 2),
            blocks(),
            blocks(),
            pltpu.VMEM((2, 4, 16, HALF), bf16),
            pltpu.VMEM((2, 4, 16, HALF), bf16),
            pltpu.VMEM((2, rows, HALF), bf16),
            pltpu.SemaphoreType.DMA((4,)),
            pltpu.SemaphoreType.DMA((64,)),
            pltpu.SemaphoreType.DMA((64,)),
        ],
        compiler_params=pltpu.CompilerParams(
            collective_id=0, has_side_effects=True, vmem_limit_bytes=56 * 1024 * 1024
        ),
        cost_estimate=pl.CostEstimate(flops=5_000_000_000, bytes_accessed=8_000_000, transcendentals=400_000),
        name="routed_experts",
    )(partial_out, tokens, gain.reshape(1, width), routes.T, route_weights.T, wg, wu, wd)


def on_device(
    tokens, lengths, key_cache, value_cache, gate_cache, mix_gain, query_weight, key_weight, value_weight,
    forget_weight, out_weight, expert_gain, routes, route_weights, expert_gate, expert_up, expert_down,
):
    partial_out = attention(
        tokens, lengths, key_cache, value_cache, gate_cache, mix_gain,
        query_weight, key_weight, value_weight, forget_weight, out_weight,
    )
    return moe(partial_out, tokens, expert_gain, routes, route_weights, expert_gate, expert_up, expert_down)


def solution(mesh):
    return jax.shard_map(
        on_device,
        mesh=mesh,
        in_specs=(
            P("ep", None),
            P("ep"),
            P("ep", None, "tp"),
            P("ep", None, "tp"),
            P("ep", "tp", None),
            P(),
            P(None, "tp"),
            P(None, "tp"),
            P(None, "tp"),
            P(None, "tp"),
            P("tp", None),
            P(),
            P("ep", None),
            P("ep", None),
            P(None, ("ep", "tp")),
            P(None, ("ep", "tp")),
            P(("ep", "tp"), None),
        ),
        out_specs=P("ep", None),
        check_vma=False,
    )
```

```python
import functools
import jax
import jax.numpy as jnp
from jax import lax
from jax.experimental import pallas as pl
from jax.experimental.pallas import tpu as pltpu
from jax.sharding import PartitionSpec as P

SEQS = 32
POS = 1024
LANES = 128
HEADS_HERE = 8
KV_BLOCKS = 4


def rms(values, gain):
    return values * lax.rsqrt(jnp.mean(values * values, axis=-1, keepdims=True) + 1e-06) * gain


def attend(
    then, meanwhile, len_ref, tok_hbm, key_hbm, value_hbm, gate_hbm, gain_hbm, wq_hbm, wk_hbm, wv_hbm, wf_hbm, wo_hbm,
    out_ref,
    tok, gain, wq, wk, wv, wf, wo, keys, values, gates, qs, owns, lgs, vnew, mixed, sems, kv_sems,
):
    blocks, per = kv_sems.shape[1], SEQS // kv_sems.shape[1]
    small = [(tok_hbm, tok), (gain_hbm, gain), (wq_hbm, wq), (wk_hbm, wk), (wv_hbm, wv), (wf_hbm, wf), (wo_hbm, wo)]
    copies = [pltpu.make_async_copy(a, b, sems.at[i]) for i, (a, b) in enumerate(small)]

    def block_copies(b):
        rows = pl.ds(b * per, per)
        return [
            pltpu.make_async_copy(src.at[rows], dst.at[rows], kv_sems.at[i, b])
            for i, (src, dst) in enumerate(((key_hbm, keys), (gate_hbm, gates), (value_hbm, values)))
        ]

    for c in copies[:6]:
        c.start()
    meanwhile()
    with jax.named_scope("wait_tok"):
        copies[0].wait()
        copies[1].wait()
    for b in range(2):
        for c in block_copies(b):
            c.start()
    ni = rms(tok[...].astype(jnp.float32), gain[...]).astype(jnp.bfloat16)
    lane = lax.broadcasted_iota(jnp.int32, (SEQS, LANES), 1)
    left = lane < 64
    with jax.named_scope("wait_w"):
        for c in copies[2:6]:
            c.wait()
    for b in range(2, blocks):
        for c in block_copies(b):
            c.start()
    copies[6].start()
    then()
    dot = functools.partial(jnp.dot, preferred_element_type=jnp.float32)
    q = dot(ni, wq[...]).astype(jnp.bfloat16).astype(jnp.float32) * 0.125
    kn = dot(ni, wk[...]).astype(jnp.bfloat16).astype(jnp.float32)
    vnew[...] = dot(ni, wv[...]).astype(jnp.bfloat16).astype(jnp.float32)
    f = lax.dot_general(ni, wf[...], (((1,), (1,)), ((), ())), preferred_element_type=jnp.float32)
    lg = jnp.minimum(f, 0.0) - jnp.log1p(jnp.exp(-jnp.abs(f)))
    for h in range(HEADS_HERE):
        column = q[:, 128 * (h // 2) : 128 * (h // 2) + 128]
        if h % 2 != h // 4:
            column = pltpu.roll(column, 64, 1)
        column = jnp.where(left if h < 4 else ~left, column, 0.0)
        rows = pl.ds(h, SEQS, stride=HEADS_HERE)
        qs[rows, :] = column
        owns[rows, :] = jnp.broadcast_to(jnp.sum(column * kn, axis=1, keepdims=True), (SEQS, LANES))
        lgs[rows, :] = jnp.broadcast_to(lg[:, h : h + 1], (SEQS, LANES))

    position = lax.broadcasted_iota(jnp.int32, (HEADS_HERE, POS), 1)

    def block(b, carry):
        with jax.named_scope("wait_kv"):
            for c in block_copies(b):
                c.wait()
        seqs = [b * per + j for j in range(per)]
        rows = [pl.ds(s * HEADS_HERE, HEADS_HERE) for s in seqs]
        scores = [
            lax.dot_general(
                qs[r, :].astype(jnp.bfloat16), keys[s], (((1,), (1,)), ((), ())),
                preferred_element_type=jnp.float32,
            )
            for s, r in zip(seqs, rows)
        ]
        raised, scale, own_part = [], [], []
        for s, r, score in zip(seqs, rows, scores):
            length = len_ref[s]
            g = gates[s]
            latest = jnp.sum(jnp.where(position == length - 1, g, 0.0), axis=1, keepdims=True)
            own = owns[r, 0:1]
            score = jnp.where(position < length, score + (latest + lgs[r, 0:1]) - g, -jnp.inf)
            top = jnp.maximum(jnp.max(score, axis=1, keepdims=True), own)
            lifted = jnp.exp(score - top)
            own_raised = jnp.exp(own - top)
            raised.append(lifted.astype(jnp.bfloat16))
            scale.append(1.0 / (jnp.sum(lifted, axis=1, keepdims=True) + own_raised))
            own_part.append(own_raised * vnew[pl.ds(s, 1), :])
        sums = [dot(p, values[s]) for p, s in zip(raised, seqs)]
        for r, o, c, w in zip(rows, sums, scale, own_part):
            mixed[r, :] = (o + w) * c
        return carry

    with jax.named_scope("loop"):
        lax.fori_loop(0, blocks, block, 0)
    parts = []
    for c in range(4):
        pair = []
        for h in (2 * c, 2 * c + 1):
            o = mixed[pl.ds(h, SEQS, stride=HEADS_HERE), :]
            pair.append(pltpu.roll(o, 64, 1) if h % 2 != h // 4 else o)
        parts.append(jnp.where(left, pair[0], pair[1]).astype(jnp.bfloat16))
    with jax.named_scope("wait_wo"):
        copies[6].wait()
    out_ref[...] = dot(jnp.concatenate(parts, axis=1), wo[...]).astype(jnp.bfloat16)


MESH = pl.DeviceIdType.MESH
CAP = 12
HALF = 1024
BLOCK = 48
CHUNK = 4 * BLOCK


ATTEND_SCRATCH = 17


def layer_kernel(
    len_ref, tok_hbm, key_hbm, value_hbm, gate_hbm, mix_hbm, wq_hbm, wk_hbm, wv_hbm, wf_hbm, wo_hbm,
    gain_hbm, routes_ref, rw_ref, wg_hbm, wu_hbm, wd_hbm,
    out_ref,
    part_ref, *scratch,
):
    (
        gain, wg, wu, wd, other_part, res, xe, picks, w_high, w_low, pk, sb, xf,
        pm, po, pi, ys, ry, zs_out, rxo, rxc, c_out, rc, er, rb, fo, hid, hop_c, hop_o,
        wsem, ss, rs,
    ) = scratch[ATTEND_SCRATCH:]
    tok_ref = scratch[0]
    f32, bf16 = jnp.float32, jnp.bfloat16
    dot = functools.partial(jnp.dot, preferred_element_type=f32)
    e, t = lax.axis_index("ep"), lax.axis_index("tp")
    z, y, x = e // 16, lax.rem(e // 4, 4), lax.rem(e, 4)
    g = y // 2

    def chip(zz, yy, xx):
        return (zz * 16 + yy * 4 + xx, t)

    partner = (e, 1 - t)
    z_peer = {k: chip(jnp.bitwise_xor(z, k), y, x) for k in (1, 2, 3)}
    x_peer = {k: chip(z, y, jnp.bitwise_xor(x, k)) for k in (1, 2, 3)}
    y_peer = chip(z, jnp.bitwise_xor(y, 1), x)
    z_cross = {k: chip(jnp.bitwise_xor(z, k), 3 - y, x) for k in range(4)}
    near = (1, 3, 2)

    loads = [
        pltpu.make_async_copy(wg_hbm, wg, wsem.at[0]),
        pltpu.make_async_copy(wu_hbm, wu, wsem.at[1]),
        pltpu.make_async_copy(wd_hbm.at[:, pl.ds(0, HALF)], wd.at[0], wsem.at[2]),
        pltpu.make_async_copy(wd_hbm.at[:, pl.ds(HALF, HALF)], wd.at[1], wsem.at[3]),
        pltpu.make_async_copy(gain_hbm, gain, wsem.at[4]),
    ]

    count = [0]
    started = []

    def send(src, dst, device):
        i = count[0]
        count[0] += 1
        c = pltpu.make_async_remote_copy(
            src_ref=src, dst_ref=dst, send_sem=ss.at[i], recv_sem=rs.at[i], device_id=device, device_id_type=MESH
        )
        c.start()
        started.append(c)
        return c

    barrier = pltpu.get_barrier_semaphore()
    peers = [partner, y_peer, *z_peer.values(), *z_cross.values(), *x_peer.values()]
    for p in peers:
        pl.semaphore_signal(barrier, inc=1, device_id=p, device_id_type=MESH)

    rows = tok_ref.shape[0]

    def choose():
        lane = lax.broadcasted_iota(jnp.int32, (rows, LANES), 1)
        place = jnp.bitwise_and(lane, 15)
        plane = jnp.bitwise_xor(z, jnp.bitwise_and(lax.shift_right_logical(lane, 4), 3))
        expert = (2 * plane + jnp.where(lane < 64, g, 1 - g)).astype(f32)
        ahead = lax.broadcasted_iota(jnp.int32, (rows, rows), 1)
        behind = lax.broadcasted_iota(jnp.int32, (rows, rows), 0)
        before = (ahead < behind).astype(f32).astype(bf16)
        unit = (ahead == behind).astype(f32)
        upright = lambda v: lax.dot_general(
            unit, v, (((1,), (1,)), ((), ())), precision=lax.Precision.HIGHEST, preferred_element_type=f32
        )
        named_here, weight_here = upright(routes_ref[...].astype(f32)), upright(rw_ref[...])
        first, second_one = named_here[:, 0:1] == expert, named_here[:, 1:2] == expert
        named = first | second_one
        earlier = dot(before, jnp.where(named, 1.0, 0.0).astype(bf16))
        here = named & (place < CAP) & (earlier == place.astype(f32))
        picks[...] = jnp.where(here, 1.0, 0.0).astype(bf16)
        weights = jnp.where(here, jnp.where(first, weight_here[:, 0:1], weight_here[:, 1:2]), 0.0)
        high = weights.astype(bf16)
        w_high[...] = high
        w_low[...] = (weights - high.astype(f32)).astype(bf16)

    def load():
        for c in loads:
            c.start()

    attend(
        load, choose, len_ref, tok_hbm, key_hbm, value_hbm, gate_hbm, mix_hbm, wq_hbm, wk_hbm, wv_hbm, wf_hbm, wo_hbm,
        part_ref, *scratch[:ATTEND_SCRATCH],
    )
    loads[4].wait()
    pl.semaphore_wait(barrier, len(peers))
    c_part = send(part_ref, other_part, partner)

    c_part.wait_recv()
    total = tok_ref[...].astype(f32) + (part_ref[...].astype(f32) + other_part[...].astype(f32))
    res_b = total.astype(bf16)
    res[0] = res_b[:, :HALF]
    res[1] = res_b[:, HALF:]
    expert_in = rms(res_b.astype(f32), gain[...]).astype(bf16)
    xe[0] = expert_in[:, :HALF]
    xe[1] = expert_in[:, HALF:]
    pk[...] = lax.dot_general(
        picks[...], xe[t], (((0,), (0,)), ((), ())), preferred_element_type=f32
    ).astype(bf16).reshape(8, 16, HALF)
    sb[0, 0] = pk[0]
    c_s0 = {k: send(pk.at[k], sb.at[0, k], z_peer[k]) for k in near}
    c_s1 = {k: send(pk.at[4 + k], sb.at[1, k], z_cross[k]) for k in (0, 1, 3, 2)}
    r_i = lax.broadcasted_iota(jnp.int32, (BLOCK, 64), 0)
    c_i = lax.broadcasted_iota(jnp.int32, (BLOCK, 64), 1)
    r_k = lax.shift_right_logical(r_i * 43, 9)
    tight = (c_i == 16 * r_k + (r_i - CAP * r_k)).astype(f32).astype(bf16)

    mine_at = lambda d, q: xf.at[t, d, q]
    fwd = {}

    def forward(d, q):
        fwd[d, q] = send(mine_at(d, q), mine_at(d, q), partner)

    for k in near:
        c_s0[k].wait_recv()
    xf[t, 0, 0] = dot(tight, sb[0].reshape(64, HALF)).astype(bf16)
    c_ax, c_ay, c_bx = {}, {}, {}

    def ax(d):
        c_ax[d] = send(mine_at(0, 0), mine_at(d, 0), x_peer[d])

    def bx(d, q):
        c_bx[d, q] = send(mine_at(0, q), mine_at(d, q), x_peer[d])

    def ay(d):
        if d:
            c_ax[d].wait_recv()
        c_ay[d] = send(mine_at(d, 0), mine_at(d, 1), y_peer)
        forward(d, 0)

    ax(2)
    ay(0)
    for k in (0, 1, 3, 2):
        c_s1[k].wait_recv()
    xf[t, 0, 2] = dot(tight, sb[1].reshape(64, HALF)).astype(bf16)
    c_by = send(mine_at(0, 2), mine_at(0, 3), y_peer)
    bx(2, 2)
    ax(1)
    ax(3)
    forward(0, 2)
    ay(2)
    c_ay[0].wait_recv()
    forward(0, 1)
    c_by.wait_recv()
    bx(2, 3)
    forward(0, 3)
    bx(1, 2)
    bx(3, 2)
    bx(1, 3)
    bx(3, 3)
    ay(1)
    ay(3)
    for c in loads[:4]:
        c.wait()
    c_pi = {}

    def hide(d):
        for q in range(4):
            fwd[d, q].wait_recv()
        x0, x1 = xf[0, d].reshape(CHUNK, HALF), xf[1, d].reshape(CHUNK, HALF)
        gate = dot(x0, wg[0:HALF]) + dot(x1, wg[HALF : 2 * HALF])
        up = dot(x0, wu[0:HALF]) + dot(x1, wu[HALF : 2 * HALF])
        hid[d] = (gate / (1.0 + jnp.exp(-gate)) * up).astype(bf16)

    def down(d):
        po[d] = dot(hid[d], wd[1 - t]).astype(bf16)
        c_pi[d] = send(po.at[d], pi.at[d], partner)
        pm[d] = dot(hid[d], wd[t])

    def compute(d):
        hide(d)
        down(d)

    c_ry, c_xc, c_xo = {}, {}, {}

    def arrive(d):
        c_bx[d, 2].wait_recv()
        forward(d, 2)
        c_ay[d].wait_recv()
        forward(d, 1)
        c_bx[d, 3].wait_recv()
        forward(d, 3)

    side = {1: pl.ds(HALF // 2, HALF // 2), 3: pl.ds(0, HALF // 2)}

    def finish(d):
        c_pi[d].wait_recv()
        ys[d] = (pm[d] + pi[d].astype(f32)).astype(bf16).reshape(4, BLOCK, HALF)
        c_ry[d] = send(ys.at[d, 1], ry.at[d], y_peer)
        if d == 2:
            for n in (1, 3):
                c_xc[2, n] = send(ys.at[2, pl.ds(2, 2), :, side[4 - n]], hop_c.at[n], x_peer[n])

    def across(d):
        c_xc[2, 4 - d].wait_recv()
        ys[d, 2:4, :, side[d]] = (ys[d, 2:4, :, side[d]].astype(f32) + hop_c[4 - d].astype(f32)).astype(bf16)
        c_xc[d] = send(ys.at[d, pl.ds(2, 2)], rxc.at[d], x_peer[d])

    def second(d):
        c_ry[d].wait_recv()
        zs_out[d] = (ys[d, 0].astype(f32) + ry[d].astype(f32)).astype(bf16)
        if d == 2:
            for n in (1, 3):
                c_xo[2, n] = send(zs_out.at[2, :, side[4 - n]], hop_o.at[n], x_peer[n])
        elif d:
            c_xo[2, 4 - d].wait_recv()
            zs_out[d, :, side[d]] = (zs_out[d, :, side[d]].astype(f32) + hop_o[4 - d].astype(f32)).astype(bf16)
            c_xo[d] = send(zs_out.at[d], rxo.at[d], x_peer[d])

    compute(0)
    arrive(2)
    compute(2)
    finish(0)
    arrive(1)
    hide(1)
    finish(2)
    down(1)
    arrive(3)
    compute(3)
    second(2)
    finish(1)
    across(1)
    finish(3)
    across(3)
    second(1)
    second(3)
    second(0)


    for d in (1, 3):
        c_xc[d].wait_recv()
    crossed = ys[0, 2:4].astype(f32) + rxc[1].astype(f32) + rxc[3].astype(f32)
    c_out[...] = crossed[1].astype(bf16)
    c_rc = send(c_out, rc, y_peer)
    spread = lambda v: lax.dot_general(
        tight, v.astype(bf16), (((0,), (0,)), ((), ())), preferred_element_type=f32
    ).astype(bf16).reshape(4, 16, HALF)
    for d in (1, 3):
        c_xo[d].wait_recv()
    own = zs_out[0].astype(f32) + rxo[1].astype(f32) + rxo[3].astype(f32)
    er[0] = spread(own)
    rb[0, 0] = er[0, 0]
    c_r0 = {k: send(er.at[0, k], rb.at[0, k], z_peer[k]) for k in near}
    c_rc.wait_recv()
    er[1] = spread(crossed[0] + rc[...].astype(f32))
    c_r1 = {k: send(er.at[1, k], rb.at[1, k], z_cross[k]) for k in (2, 1, 3, 0)}
    for k in near:
        c_r0[k].wait_recv()
    for k in (2, 1, 3, 0):
        c_r1[k].wait_recv()
    returned = rb[...].reshape(LANES, HALF)
    mixture = res[t].astype(f32) + dot(w_high[...], returned) + dot(w_low[...], returned)
    fo[t] = mixture.astype(bf16)
    c_fo = send(fo.at[t], fo.at[t], partner)
    c_fo.wait_recv()
    out_ref[:, 0:HALF] = fo[0]
    out_ref[:, HALF : 2 * HALF] = fo[1]
    for c in started:
        c.wait_send()


def on_device(
    tokens, lengths, key_cache, value_cache, gate_cache, mix_gain, query_weight, key_weight, value_weight,
    forget_weight, out_weight, expert_gain, routes, route_weights, expert_gate, expert_up, expert_down,
):
    rows, width = tokens.shape
    f32, bf16 = jnp.float32, jnp.bfloat16
    any_space = pl.BlockSpec(memory_space=pl.ANY)
    vmem = pl.BlockSpec(memory_space=pltpu.VMEM)
    smem = pl.BlockSpec(memory_space=pltpu.SMEM)
    blocks = lambda *s: pltpu.VMEM((*s, BLOCK, HALF), bf16)
    heads = pltpu.VMEM((SEQS * HEADS_HERE, LANES), f32)
    forget = forget_weight.T
    return pl.pallas_call(
        layer_kernel,
        out_shape=jax.ShapeDtypeStruct((rows, width), bf16),
        in_specs=[smem] + [any_space] * 11 + [vmem] * 2 + [any_space] * 3,
        out_specs=vmem,
        scratch_shapes=[
            pltpu.VMEM((rows, width), bf16),
            pltpu.VMEM((rows, width), bf16),
            pltpu.VMEM((1, width), f32),
            pltpu.VMEM(query_weight.shape, bf16),
            pltpu.VMEM(key_weight.shape, bf16),
            pltpu.VMEM(value_weight.shape, bf16),
            pltpu.VMEM(forget.shape, bf16),
            pltpu.VMEM(out_weight.shape, bf16),
            pltpu.VMEM(key_cache.shape, bf16),
            pltpu.VMEM(value_cache.shape, bf16),
            pltpu.VMEM(gate_cache.shape, f32),
            heads,
            heads,
            heads,
            pltpu.VMEM((SEQS, LANES), f32),
            heads,
            pltpu.SemaphoreType.DMA((7,)),
            pltpu.SemaphoreType.DMA((3, KV_BLOCKS)),
            pltpu.VMEM((1, width), f32),
            pltpu.VMEM(expert_gate.shape, bf16),
            pltpu.VMEM(expert_up.shape, bf16),
            pltpu.VMEM((2, expert_down.shape[0], HALF), bf16),
            pltpu.VMEM((rows, width), bf16),
            pltpu.VMEM((2, rows, HALF), bf16),
            pltpu.VMEM((2, rows, HALF), bf16),
            pltpu.VMEM((rows, LANES), bf16),
            pltpu.VMEM((rows, LANES), bf16),
            pltpu.VMEM((rows, LANES), bf16),
            pltpu.VMEM((8, 16, HALF), bf16),
            pltpu.VMEM((2, 4, 16, HALF), bf16),
            blocks(2, 4, 4),
            pltpu.VMEM((4, CHUNK, HALF), f32),
            pltpu.VMEM((4, CHUNK, HALF), bf16),
            pltpu.VMEM((4, CHUNK, HALF), bf16),
            blocks(4, 4),
            blocks(4),
            blocks(4),
            blocks(4),
            blocks(4, 2),
            blocks(),
            blocks(),
            pltpu.VMEM((2, 4, 16, HALF), bf16),
            pltpu.VMEM((2, 4, 16, HALF), bf16),
            pltpu.VMEM((2, rows, HALF), bf16),
            pltpu.VMEM((4, CHUNK, expert_gate.shape[1]), bf16),
            pltpu.VMEM((4, 2, BLOCK, HALF // 2), bf16),
            pltpu.VMEM((4, BLOCK, HALF // 2), bf16),
            pltpu.SemaphoreType.DMA((5,)),
            pltpu.SemaphoreType.DMA((72,)),
            pltpu.SemaphoreType.DMA((72,)),
        ],
        compiler_params=pltpu.CompilerParams(
            collective_id=0, has_side_effects=True, vmem_limit_bytes=60 * 1024 * 1024
        ),
        cost_estimate=pl.CostEstimate(flops=5_500_000_000, bytes_accessed=30_000_000, transcendentals=700_000),
        name="decode_layer",
    )(
        lengths, tokens, key_cache, value_cache, gate_cache, mix_gain.reshape(1, width), query_weight, key_weight,
        value_weight, forget, out_weight, expert_gain.reshape(1, width), routes.T, route_weights.T,
        expert_gate, expert_up, expert_down,
    )


def solution(mesh):
    return jax.shard_map(
        on_device,
        mesh=mesh,
        in_specs=(
            P("ep", None),
            P("ep"),
            P("ep", None, "tp"),
            P("ep", None, "tp"),
            P("ep", "tp", None),
            P(),
            P(None, "tp"),
            P(None, "tp"),
            P(None, "tp"),
            P(None, "tp"),
            P("tp", None),
            P(),
            P("ep", None),
            P("ep", None),
            P(None, ("ep", "tp")),
            P(None, ("ep", "tp")),
            P(("ep", "tp"), None),
        ),
        out_specs=P("ep", None),
        check_vma=False,
    )
```

```python
import functools
import jax
import jax.numpy as jnp
from jax import lax
from jax.experimental import pallas as pl
from jax.experimental.pallas import tpu as pltpu
from jax.sharding import PartitionSpec as P

SEQS = 32
POS = 1024
LANES = 128
HEADS_HERE = 8
KV_BLOCKS = 4


def rms(values, gain):
    return values * lax.rsqrt(jnp.mean(values * values, axis=-1, keepdims=True) + 1e-06) * gain


def attend(
    first, then, meanwhile, len_ref, tok_hbm, key_hbm, value_hbm, gate_hbm, gain_hbm, wq_hbm, wk_hbm, wv_hbm, wf_hbm, wo_hbm,
    out_ref,
    tok, gain, wq, wk, wv, wf, wo, keys, values, gates, qs, owns, lgs, vnew, mixed, sems, kv_sems,
):
    blocks, per = kv_sems.shape[1], SEQS // kv_sems.shape[1]
    small = [(tok_hbm, tok), (gain_hbm, gain), (wq_hbm, wq), (wk_hbm, wk), (wv_hbm, wv), (wf_hbm, wf), (wo_hbm, wo)]
    copies = [pltpu.make_async_copy(a, b, sems.at[i]) for i, (a, b) in enumerate(small)]

    def block_copies(b):
        rows = pl.ds(b * per, per)
        return [
            pltpu.make_async_copy(src.at[rows], dst.at[rows], kv_sems.at[i, b])
            for i, (src, dst) in enumerate(((key_hbm, keys), (gate_hbm, gates), (value_hbm, values)))
        ]

    copies[0].start()
    copies[1].start()
    first()
    for c in copies[2:6]:
        c.start()
    meanwhile()
    with jax.named_scope("wait_tok"):
        copies[0].wait()
        copies[1].wait()
    for b in range(2):
        for c in block_copies(b):
            c.start()
    ni = rms(tok[...].astype(jnp.float32), gain[...]).astype(jnp.bfloat16)
    lane = lax.broadcasted_iota(jnp.int32, (SEQS, LANES), 1)
    left = lane < 64
    with jax.named_scope("wait_w"):
        for c in copies[2:6]:
            c.wait()
    for b in range(2, blocks):
        for c in block_copies(b):
            c.start()
    copies[6].start()
    dot = functools.partial(jnp.dot, preferred_element_type=jnp.float32)
    q = dot(ni, wq[...]).astype(jnp.bfloat16).astype(jnp.float32) * 0.125
    kn = dot(ni, wk[...]).astype(jnp.bfloat16).astype(jnp.float32)
    vnew[...] = dot(ni, wv[...]).astype(jnp.bfloat16).astype(jnp.float32)
    f = lax.dot_general(ni, wf[...], (((1,), (1,)), ((), ())), preferred_element_type=jnp.float32)
    lg = jnp.minimum(f, 0.0) - jnp.log1p(jnp.exp(-jnp.abs(f)))
    for h in range(HEADS_HERE):
        column = q[:, 128 * (h // 2) : 128 * (h // 2) + 128]
        if h % 2 != h // 4:
            column = pltpu.roll(column, 64, 1)
        column = jnp.where(left if h < 4 else ~left, column, 0.0)
        rows = pl.ds(h, SEQS, stride=HEADS_HERE)
        qs[rows, :] = column
        owns[rows, :] = jnp.broadcast_to(jnp.sum(column * kn, axis=1, keepdims=True), (SEQS, LANES))
        lgs[rows, :] = jnp.broadcast_to(lg[:, h : h + 1], (SEQS, LANES))

    position = lax.broadcasted_iota(jnp.int32, (HEADS_HERE, POS), 1)

    def block(b, carry):
        with jax.named_scope("wait_kv"):
            for c in block_copies(b):
                c.wait()
        seqs = [b * per + j for j in range(per)]
        rows = [pl.ds(s * HEADS_HERE, HEADS_HERE) for s in seqs]
        scores = [
            lax.dot_general(
                qs[r, :].astype(jnp.bfloat16), keys[s], (((1,), (1,)), ((), ())),
                preferred_element_type=jnp.float32,
            )
            for s, r in zip(seqs, rows)
        ]
        raised, scale, own_part = [], [], []
        for s, r, score in zip(seqs, rows, scores):
            length = len_ref[s]
            g = gates[s]
            latest = jnp.sum(jnp.where(position == length - 1, g, 0.0), axis=1, keepdims=True)
            own = owns[r, 0:1]
            score = jnp.where(position < length, score + (latest + lgs[r, 0:1]) - g, -jnp.inf)
            top = jnp.maximum(jnp.max(score, axis=1, keepdims=True), own)
            lifted = jnp.exp(score - top)
            own_raised = jnp.exp(own - top)
            raised.append(lifted.astype(jnp.bfloat16))
            scale.append(1.0 / (jnp.sum(lifted, axis=1, keepdims=True) + own_raised))
            own_part.append(own_raised * vnew[pl.ds(s, 1), :])
        sums = [dot(p, values[s]) for p, s in zip(raised, seqs)]
        for r, o, c, w in zip(rows, sums, scale, own_part):
            mixed[r, :] = (o + w) * c
        return carry

    with jax.named_scope("loop"):
        lax.fori_loop(0, blocks, block, 0)
    then()
    parts = []
    for c in range(4):
        pair = []
        for h in (2 * c, 2 * c + 1):
            o = mixed[pl.ds(h, SEQS, stride=HEADS_HERE), :]
            pair.append(pltpu.roll(o, 64, 1) if h % 2 != h // 4 else o)
        parts.append(jnp.where(left, pair[0], pair[1]).astype(jnp.bfloat16))
    with jax.named_scope("wait_wo"):
        copies[6].wait()
    out_ref[...] = dot(jnp.concatenate(parts, axis=1), wo[...]).astype(jnp.bfloat16)


MESH = pl.DeviceIdType.MESH
CAP = 12
HALF = 1024
BLOCK = 48
CHUNK = 4 * BLOCK


ATTEND_SCRATCH = 17


def layer_kernel(
    len_hbm, tok_hbm, key_hbm, value_hbm, gate_hbm, mix_hbm, wq_hbm, wk_hbm, wv_hbm, wf_hbm, wo_hbm,
    gain_hbm, routes_hbm, rw_hbm, wg_hbm, wu_hbm, wd_hbm,
    out_ref,
    part_ref, *scratch,
):
    (
        len_ref, routes_ref, rw_ref, gain, wg, wu, wd, other_part, res, xe, picks, w_high, w_low, pk, sb, xf,
        pm, po, pi, ys, ry, zs_out, rxo, rxc, er, rb, fo, hid, hop_c, hop_o,
        wsem, ss, rs,
    ) = scratch[ATTEND_SCRATCH:]
    tok_ref = scratch[0]
    f32, bf16 = jnp.float32, jnp.bfloat16
    dot = functools.partial(jnp.dot, preferred_element_type=f32)
    e, t = lax.axis_index("ep"), lax.axis_index("tp")
    z, y, x = e // 16, lax.rem(e // 4, 4), lax.rem(e, 4)
    g = y // 2

    def chip(zz, yy, xx):
        return (zz * 16 + yy * 4 + xx, t)

    partner = (e, 1 - t)
    z_peer = {k: chip(jnp.bitwise_xor(z, k), y, x) for k in (1, 2, 3)}
    x_peer = {k: chip(z, y, jnp.bitwise_xor(x, k)) for k in (1, 2, 3)}
    y_peer = chip(z, jnp.bitwise_xor(y, 1), x)
    z_cross = {k: chip(jnp.bitwise_xor(z, k), 3 - y, x) for k in range(4)}
    z_far = {k: chip(jnp.bitwise_xor(z, k), jnp.bitwise_xor(y, 2), x) for k in range(4)}
    near = (1, 3, 2)

    loads = [
        pltpu.make_async_copy(wg_hbm, wg, wsem.at[0]),
        pltpu.make_async_copy(wu_hbm, wu, wsem.at[1]),
        pltpu.make_async_copy(wd_hbm.at[:, pl.ds(0, HALF)], wd.at[0], wsem.at[2]),
        pltpu.make_async_copy(wd_hbm.at[:, pl.ds(HALF, HALF)], wd.at[1], wsem.at[3]),
        pltpu.make_async_copy(gain_hbm, gain, wsem.at[4]),
    ]
    tables = [
        pltpu.make_async_copy(routes_hbm, routes_ref, wsem.at[5]),
        pltpu.make_async_copy(rw_hbm, rw_ref, wsem.at[6]),
        pltpu.make_async_copy(len_hbm, len_ref, wsem.at[7]),
    ]

    def first_loads():
        for c in (*tables, loads[4]):
            c.start()

    count = [0]
    started = []

    def send(src, dst, device):
        i = count[0]
        count[0] += 1
        c = pltpu.make_async_remote_copy(
            src_ref=src, dst_ref=dst, send_sem=ss.at[i], recv_sem=rs.at[i], device_id=device, device_id_type=MESH
        )
        c.start()
        started.append(c)
        return c

    barrier = pltpu.get_barrier_semaphore()
    peers = [partner, y_peer, *z_peer.values(), *z_cross.values(), *z_far.values(), *x_peer.values()]
    for p in peers:
        pl.semaphore_signal(barrier, inc=1, device_id=p, device_id_type=MESH)

    rows = tok_ref.shape[0]

    def choose():
        for c in tables:
            c.wait()
        lane = lax.broadcasted_iota(jnp.int32, (rows, LANES), 1)
        place = jnp.bitwise_and(lane, 15)
        plane = jnp.bitwise_xor(z, jnp.bitwise_and(lax.shift_right_logical(lane, 4), 3))
        expert = (2 * plane + jnp.where(lane < 64, g, 1 - g)).astype(f32)
        ahead = lax.broadcasted_iota(jnp.int32, (rows, rows), 1)
        behind = lax.broadcasted_iota(jnp.int32, (rows, rows), 0)
        before = (ahead < behind).astype(f32).astype(bf16)
        unit = (ahead == behind).astype(f32)
        upright = lambda v: lax.dot_general(
            unit, v, (((1,), (1,)), ((), ())), precision=lax.Precision.HIGHEST, preferred_element_type=f32
        )
        named_here, weight_here = upright(routes_ref[...].astype(f32)), upright(rw_ref[...])
        first, second_one = named_here[:, 0:1] == expert, named_here[:, 1:2] == expert
        named = first | second_one
        earlier = dot(before, jnp.where(named, 1.0, 0.0).astype(bf16))
        here = named & (place < CAP) & (earlier == place.astype(f32))
        picks[...] = jnp.where(here, 1.0, 0.0).astype(bf16)
        weights = jnp.where(here, jnp.where(first, weight_here[:, 0:1], weight_here[:, 1:2]), 0.0)
        high = weights.astype(bf16)
        w_high[...] = high
        w_low[...] = (weights - high.astype(f32)).astype(bf16)

    def load():
        for c in loads[:4]:
            c.start()

    attend(
        first_loads, load, choose, len_ref, tok_hbm, key_hbm, value_hbm, gate_hbm, mix_hbm, wq_hbm, wk_hbm, wv_hbm, wf_hbm, wo_hbm,
        part_ref, *scratch[:ATTEND_SCRATCH],
    )
    loads[4].wait()
    pl.semaphore_wait(barrier, len(peers))
    c_part = send(part_ref, other_part, partner)

    c_part.wait_recv()
    total = tok_ref[...].astype(f32) + (part_ref[...].astype(f32) + other_part[...].astype(f32))
    res_b = total.astype(bf16)
    res[0] = res_b[:, :HALF]
    res[1] = res_b[:, HALF:]
    expert_in = rms(res_b.astype(f32), gain[...]).astype(bf16)
    xe[0] = expert_in[:, :HALF]
    xe[1] = expert_in[:, HALF:]
    pk[...] = lax.dot_general(
        picks[...], xe[t], (((0,), (0,)), ((), ())), preferred_element_type=f32
    ).astype(bf16).reshape(8, 16, HALF)
    sb[0, 0] = pk[0]
    c_s0 = {k: send(pk.at[k], sb.at[0, k], z_peer[k]) for k in near}
    c_s1 = {k: send(pk.at[4 + k], sb.at[1, k], z_cross[k]) for k in (0, 1, 3, 2)}
    r_i = lax.broadcasted_iota(jnp.int32, (BLOCK, 64), 0)
    c_i = lax.broadcasted_iota(jnp.int32, (BLOCK, 64), 1)
    r_k = lax.shift_right_logical(r_i * 43, 9)
    tight = (c_i == 16 * r_k + (r_i - CAP * r_k)).astype(f32).astype(bf16)

    mine_at = lambda d, q: xf.at[t, d, q]
    fwd = {}

    def forward(d, q):
        fwd[d, q] = send(mine_at(d, q), mine_at(d, q), partner)

    for k in near:
        c_s0[k].wait_recv()
    xf[t, 0, 0] = dot(tight, sb[0].reshape(64, HALF)).astype(bf16)
    c_ax, c_ay, c_bx = {}, {}, {}

    def ax(d):
        c_ax[d] = send(mine_at(0, 0), mine_at(d, 0), x_peer[d])

    def bx(d, q):
        c_bx[d, q] = send(mine_at(0, q), mine_at(d, q), x_peer[d])

    def ay(d):
        if d:
            c_ax[d].wait_recv()
        c_ay[d] = send(mine_at(d, 0), mine_at(d, 1), y_peer)
        forward(d, 0)

    ax(2)
    ay(0)
    for k in (0, 1, 3, 2):
        c_s1[k].wait_recv()
    xf[t, 0, 2] = dot(tight, sb[1].reshape(64, HALF)).astype(bf16)
    c_by = send(mine_at(0, 2), mine_at(0, 3), y_peer)
    bx(2, 2)
    ax(1)
    ax(3)
    forward(0, 2)
    ay(2)
    c_ay[0].wait_recv()
    forward(0, 1)
    c_by.wait_recv()
    bx(2, 3)
    forward(0, 3)
    bx(1, 2)
    bx(3, 2)
    bx(1, 3)
    bx(3, 3)
    ay(1)
    ay(3)
    for c in loads[:4]:
        c.wait()
    c_pi = {}

    def hide(d):
        for q in range(4):
            fwd[d, q].wait_recv()
        x0, x1 = xf[0, d].reshape(CHUNK, HALF), xf[1, d].reshape(CHUNK, HALF)
        gate = dot(x0, wg[0:HALF]) + dot(x1, wg[HALF : 2 * HALF])
        up = dot(x0, wu[0:HALF]) + dot(x1, wu[HALF : 2 * HALF])
        hid[d] = (gate / (1.0 + jnp.exp(-gate)) * up).astype(bf16)

    def down(d):
        po[d] = dot(hid[d], wd[1 - t]).astype(bf16)
        c_pi[d] = send(po.at[d], pi.at[d], partner)
        pm[d] = dot(hid[d], wd[t])

    def compute(d):
        hide(d)
        down(d)

    c_ry, c_xc, c_xo = {}, {}, {}

    def arrive(d):
        c_bx[d, 2].wait_recv()
        forward(d, 2)
        c_ay[d].wait_recv()
        forward(d, 1)
        c_bx[d, 3].wait_recv()
        forward(d, 3)

    side = {1: pl.ds(HALF // 2, HALF // 2), 3: pl.ds(0, HALF // 2)}

    def finish(d):
        c_pi[d].wait_recv()
        ys[d] = (pm[d] + pi[d].astype(f32)).astype(bf16).reshape(4, BLOCK, HALF)
        c_ry[d] = send(ys.at[d, 1], ry.at[d], y_peer)
        if d == 2:
            for n in (1, 3):
                c_xc[2, n] = send(ys.at[2, pl.ds(2, 2), :, side[4 - n]], hop_c.at[n], x_peer[n])

    def across(d):
        c_xc[2, 4 - d].wait_recv()
        ys[d, 2:4, :, side[d]] = (ys[d, 2:4, :, side[d]].astype(f32) + hop_c[4 - d].astype(f32)).astype(bf16)
        c_xc[d] = send(ys.at[d, pl.ds(2, 2)], rxc.at[d], x_peer[d])

    def second(d):
        c_ry[d].wait_recv()
        zs_out[d] = (ys[d, 0].astype(f32) + ry[d].astype(f32)).astype(bf16)
        if d == 2:
            for n in (1, 3):
                c_xo[2, n] = send(zs_out.at[2, :, side[4 - n]], hop_o.at[n], x_peer[n])
        elif d:
            c_xo[2, 4 - d].wait_recv()
            zs_out[d, :, side[d]] = (zs_out[d, :, side[d]].astype(f32) + hop_o[4 - d].astype(f32)).astype(bf16)
            c_xo[d] = send(zs_out.at[d], rxo.at[d], x_peer[d])

    compute(0)
    arrive(2)
    compute(2)
    finish(0)
    arrive(1)
    hide(1)
    finish(2)
    down(1)
    arrive(3)
    compute(3)
    second(2)
    finish(1)
    across(1)
    finish(3)
    across(3)
    second(1)
    second(3)
    second(0)


    for d in (1, 3):
        c_xc[d].wait_recv()
    crossed = ys[0, 2:4].astype(f32) + rxc[1].astype(f32) + rxc[3].astype(f32)
    spread = lambda v: lax.dot_general(
        tight, v.astype(bf16), (((0,), (0,)), ((), ())), preferred_element_type=f32
    ).astype(bf16).reshape(4, 16, HALF)
    er[1] = spread(crossed[0])
    er[2] = spread(crossed[1])
    order = (2, 1, 3, 0)
    c_r = [send(er.at[1, k], rb.at[1, k], z_cross[k]) for k in order]
    c_r += [send(er.at[2, k], rb.at[2, k], z_far[k]) for k in order]
    for d in (1, 3):
        c_xo[d].wait_recv()
    own = zs_out[0].astype(f32) + rxo[1].astype(f32) + rxo[3].astype(f32)
    er[0] = spread(own)
    rb[0, 0] = er[0, 0]
    c_r += [send(er.at[0, k], rb.at[0, k], z_peer[k]) for k in order[:3]]
    mixture = res[t].astype(f32)
    for c in c_r[:8]:
        c.wait_recv()
    weigh = lambda a, v: dot(w_high[:, a : a + 64], v) + dot(w_low[:, a : a + 64], v)
    for i in (1, 2):
        mixture = mixture + weigh(64, rb[i].reshape(64, HALF))
    for c in c_r[8:]:
        c.wait_recv()
    mixture = mixture + weigh(0, rb[0].reshape(64, HALF))
    fo[t] = mixture.astype(bf16)
    c_fo = send(fo.at[t], fo.at[t], partner)
    c_fo.wait_recv()
    out_ref[:, 0:HALF] = fo[0]
    out_ref[:, HALF : 2 * HALF] = fo[1]
    for c in started:
        c.wait_send()


def on_device(
    tokens, lengths, key_cache, value_cache, gate_cache, mix_gain, query_weight, key_weight, value_weight,
    forget_weight, out_weight, expert_gain, routes, route_weights, expert_gate, expert_up, expert_down,
):
    rows, width = tokens.shape
    f32, bf16 = jnp.float32, jnp.bfloat16
    any_space = pl.BlockSpec(memory_space=pl.ANY)
    vmem = pl.BlockSpec(memory_space=pltpu.VMEM)
    blocks = lambda *s: pltpu.VMEM((*s, BLOCK, HALF), bf16)
    heads = pltpu.VMEM((SEQS * HEADS_HERE, LANES), f32)
    forget = forget_weight.T
    return pl.pallas_call(
        layer_kernel,
        out_shape=pltpu.VMEM((rows, width), bf16),
        in_specs=[any_space] * 17,
        out_specs=vmem,
        scratch_shapes=[
            pltpu.VMEM((rows, width), bf16),
            pltpu.VMEM((rows, width), bf16),
            pltpu.VMEM((1, width), f32),
            pltpu.VMEM(query_weight.shape, bf16),
            pltpu.VMEM(key_weight.shape, bf16),
            pltpu.VMEM(value_weight.shape, bf16),
            pltpu.VMEM(forget.shape, bf16),
            pltpu.VMEM(out_weight.shape, bf16),
            pltpu.VMEM(key_cache.shape, bf16),
            pltpu.VMEM(value_cache.shape, bf16),
            pltpu.VMEM(gate_cache.shape, f32),
            heads,
            heads,
            heads,
            pltpu.VMEM((SEQS, LANES), f32),
            heads,
            pltpu.SemaphoreType.DMA((7,)),
            pltpu.SemaphoreType.DMA((3, KV_BLOCKS)),
            pltpu.SMEM((rows,), jnp.int32),
            pltpu.VMEM((2, rows), jnp.int32),
            pltpu.VMEM((2, rows), f32),
            pltpu.VMEM((1, width), f32),
            pltpu.VMEM(expert_gate.shape, bf16),
            pltpu.VMEM(expert_up.shape, bf16),
            pltpu.VMEM((2, expert_down.shape[0], HALF), bf16),
            pltpu.VMEM((rows, width), bf16),
            pltpu.VMEM((2, rows, HALF), bf16),
            pltpu.VMEM((2, rows, HALF), bf16),
            pltpu.VMEM((rows, LANES), bf16),
            pltpu.VMEM((rows, LANES), bf16),
            pltpu.VMEM((rows, LANES), bf16),
            pltpu.VMEM((8, 16, HALF), bf16),
            pltpu.VMEM((2, 4, 16, HALF), bf16),
            blocks(2, 4, 4),
            pltpu.VMEM((4, CHUNK, HALF), f32),
            pltpu.VMEM((4, CHUNK, HALF), bf16),
            pltpu.VMEM((4, CHUNK, HALF), bf16),
            blocks(4, 4),
            blocks(4),
            blocks(4),
            blocks(4),
            blocks(4, 2),
            pltpu.VMEM((3, 4, 16, HALF), bf16),
            pltpu.VMEM((3, 4, 16, HALF), bf16),
            pltpu.VMEM((2, rows, HALF), bf16),
            pltpu.VMEM((4, CHUNK, expert_gate.shape[1]), bf16),
            pltpu.VMEM((4, 2, BLOCK, HALF // 2), bf16),
            pltpu.VMEM((4, BLOCK, HALF // 2), bf16),
            pltpu.SemaphoreType.DMA((8,)),
            pltpu.SemaphoreType.DMA((80,)),
            pltpu.SemaphoreType.DMA((80,)),
        ],
        compiler_params=pltpu.CompilerParams(
            collective_id=0, has_side_effects=True, vmem_limit_bytes=60 * 1024 * 1024
        ),
        cost_estimate=pl.CostEstimate(flops=5_500_000_000, bytes_accessed=30_000_000, transcendentals=700_000),
        name="decode_layer",
    )(
        lengths, tokens, key_cache, value_cache, gate_cache, mix_gain.reshape(1, width), query_weight, key_weight,
        value_weight, forget, out_weight, expert_gain.reshape(1, width), routes.T, route_weights.T,
        expert_gate, expert_up, expert_down,
    )


def solution(mesh):
    return jax.shard_map(
        on_device,
        mesh=mesh,
        in_specs=(
            P("ep", None),
            P("ep"),
            P("ep", None, "tp"),
            P("ep", None, "tp"),
            P("ep", "tp", None),
            P(),
            P(None, "tp"),
            P(None, "tp"),
            P(None, "tp"),
            P(None, "tp"),
            P("tp", None),
            P(),
            P("ep", None),
            P("ep", None),
            P(None, ("ep", "tp")),
            P(None, ("ep", "tp")),
            P(("ep", "tp"), None),
        ),
        out_specs=P("ep", None),
        check_vma=False,
    )
```

```python
import functools
import jax
import jax.numpy as jnp
from jax import lax
from jax.experimental import pallas as pl
from jax.experimental.pallas import tpu as pltpu
from jax.sharding import PartitionSpec as P

SEQS = 32
POS = 1024
LANES = 128
HEADS_HERE = 8
KV_BLOCKS = 4


def rms(values, gain):
    return values * lax.rsqrt(jnp.mean(values * values, axis=-1, keepdims=True) + 1e-06) * gain


def attend(
    first, then, meanwhile, len_ref, tok_hbm, key_hbm, value_hbm, gate_hbm, gain_hbm, wq_hbm, wk_hbm, wv_hbm, wf_hbm, wo_hbm,
    out_ref,
    tok, gain, wq, wk, wv, wf, wo, keys, values, gates, qs, owns, lgs, vnew, mixed, sems, kv_sems,
):
    blocks, per = kv_sems.shape[1], SEQS // kv_sems.shape[1]
    small = [(tok_hbm, tok), (gain_hbm, gain), (wq_hbm, wq), (wk_hbm, wk), (wv_hbm, wv), (wf_hbm, wf), (wo_hbm, wo)]
    copies = [pltpu.make_async_copy(a, b, sems.at[i]) for i, (a, b) in enumerate(small)]

    def block_copies(b):
        rows = pl.ds(b * per, per)
        return [
            pltpu.make_async_copy(src.at[rows], dst.at[rows], kv_sems.at[i, b])
            for i, (src, dst) in enumerate(((key_hbm, keys), (gate_hbm, gates), (value_hbm, values)))
        ]

    copies[0].start()
    copies[1].start()
    first()
    for c in copies[2:6]:
        c.start()
    meanwhile()
    with jax.named_scope("wait_tok"):
        copies[0].wait()
        copies[1].wait()
    for b in range(2):
        for c in block_copies(b):
            c.start()
    ni = rms(tok[...].astype(jnp.float32), gain[...]).astype(jnp.bfloat16)
    lane = lax.broadcasted_iota(jnp.int32, (SEQS, LANES), 1)
    left = lane < 64
    with jax.named_scope("wait_w"):
        for c in copies[2:6]:
            c.wait()
    for b in range(2, blocks):
        for c in block_copies(b):
            c.start()
    copies[6].start()
    dot = functools.partial(jnp.dot, preferred_element_type=jnp.float32)
    q = dot(ni, wq[...]).astype(jnp.bfloat16).astype(jnp.float32) * 0.125
    kn = dot(ni, wk[...]).astype(jnp.bfloat16).astype(jnp.float32)
    vnew[...] = dot(ni, wv[...]).astype(jnp.bfloat16).astype(jnp.float32)
    f = lax.dot_general(ni, wf[...], (((1,), (1,)), ((), ())), preferred_element_type=jnp.float32)
    lg = jnp.minimum(f, 0.0) - jnp.log1p(jnp.exp(-jnp.abs(f)))
    for h in range(HEADS_HERE):
        column = q[:, 128 * (h // 2) : 128 * (h // 2) + 128]
        if h % 2 != h // 4:
            column = pltpu.roll(column, 64, 1)
        column = jnp.where(left if h < 4 else ~left, column, 0.0)
        rows = pl.ds(h, SEQS, stride=HEADS_HERE)
        qs[rows, :] = column
        owns[rows, :] = jnp.broadcast_to(jnp.sum(column * kn, axis=1, keepdims=True), (SEQS, LANES))
        lgs[rows, :] = jnp.broadcast_to(lg[:, h : h + 1], (SEQS, LANES))

    position = lax.broadcasted_iota(jnp.int32, (HEADS_HERE, POS), 1)

    def block(b, carry):
        with jax.named_scope("wait_kv"):
            for c in block_copies(b):
                c.wait()
        seqs = [b * per + j for j in range(per)]
        rows = [pl.ds(s * HEADS_HERE, HEADS_HERE) for s in seqs]
        scores = [
            lax.dot_general(
                qs[r, :].astype(jnp.bfloat16), keys[s], (((1,), (1,)), ((), ())),
                preferred_element_type=jnp.float32,
            )
            for s, r in zip(seqs, rows)
        ]
        raised, scale, own_part = [], [], []
        for s, r, score in zip(seqs, rows, scores):
            length = len_ref[s]
            g = gates[s]
            latest = jnp.sum(jnp.where(position == length - 1, g, 0.0), axis=1, keepdims=True)
            own = owns[r, 0:1]
            score = jnp.where(position < length, score + (latest + lgs[r, 0:1]) - g, -jnp.inf)
            top = jnp.maximum(jnp.max(score, axis=1, keepdims=True), own)
            lifted = jnp.exp(score - top)
            own_raised = jnp.exp(own - top)
            raised.append(lifted.astype(jnp.bfloat16))
            scale.append(1.0 / (jnp.sum(lifted, axis=1, keepdims=True) + own_raised))
            own_part.append(own_raised * vnew[pl.ds(s, 1), :])
        sums = [dot(p, values[s]) for p, s in zip(raised, seqs)]
        for r, o, c, w in zip(rows, sums, scale, own_part):
            mixed[r, :] = (o + w) * c
        return carry

    with jax.named_scope("loop"):
        lax.fori_loop(0, blocks, block, 0)
    then()
    parts = []
    for c in range(4):
        pair = []
        for h in (2 * c, 2 * c + 1):
            o = mixed[pl.ds(h, SEQS, stride=HEADS_HERE), :]
            pair.append(pltpu.roll(o, 64, 1) if h % 2 != h // 4 else o)
        parts.append(jnp.where(left, pair[0], pair[1]).astype(jnp.bfloat16))
    with jax.named_scope("wait_wo"):
        copies[6].wait()
    out_ref[...] = dot(jnp.concatenate(parts, axis=1), wo[...]).astype(jnp.bfloat16)


MESH = pl.DeviceIdType.MESH
CAP = 12
HALF = 1024
BLOCK = 48
CHUNK = 4 * BLOCK
SEND_SLOTS = 34
COPIES = 66


ATTEND_SCRATCH = 17


def layer_kernel(
    len_hbm, tok_hbm, key_hbm, value_hbm, gate_hbm, mix_hbm, wq_hbm, wk_hbm, wv_hbm, wf_hbm, wo_hbm,
    gain_hbm, routes_hbm, rw_hbm, wg_hbm, wu_hbm, wd_hbm,
    out_ref,
    part_ref, *scratch,
):
    (
        len_ref, routes_ref, rw_ref, gain, wg, wu, wd, other_part, res, xe, picks, w_high, w_low, pk, sb, xf,
        pm, po, pi, ys, ry, zs_out, rxo, rxc, er, rb, fo, hid, hop_c, hop_o,
        wsem, ss, rs,
    ) = scratch[ATTEND_SCRATCH:]
    tok_ref = scratch[0]
    f32, bf16 = jnp.float32, jnp.bfloat16
    dot = functools.partial(jnp.dot, preferred_element_type=f32)
    e, t = lax.axis_index("ep"), lax.axis_index("tp")
    z, y, x = e // 16, lax.rem(e // 4, 4), lax.rem(e, 4)
    g = y // 2

    def chip(zz, yy, xx):
        return (zz * 16 + yy * 4 + xx, t)

    partner = (e, 1 - t)
    z_peer = {k: chip(jnp.bitwise_xor(z, k), y, x) for k in (1, 2, 3)}
    x_peer = {k: chip(z, y, jnp.bitwise_xor(x, k)) for k in (1, 2, 3)}
    y_peer = chip(z, jnp.bitwise_xor(y, 1), x)
    z_cross = {k: chip(jnp.bitwise_xor(z, k), 3 - y, x) for k in range(4)}
    z_far = {k: chip(jnp.bitwise_xor(z, k), jnp.bitwise_xor(y, 2), x) for k in range(4)}
    near = (1, 3, 2)

    loads = [
        pltpu.make_async_copy(wg_hbm, wg, wsem.at[0]),
        pltpu.make_async_copy(wu_hbm, wu, wsem.at[1]),
        pltpu.make_async_copy(wd_hbm.at[:, pl.ds(0, HALF)], wd.at[0], wsem.at[2]),
        pltpu.make_async_copy(wd_hbm.at[:, pl.ds(HALF, HALF)], wd.at[1], wsem.at[3]),
        pltpu.make_async_copy(gain_hbm, gain, wsem.at[4]),
    ]
    tables = [
        pltpu.make_async_copy(routes_hbm, routes_ref, wsem.at[5]),
        pltpu.make_async_copy(rw_hbm, rw_ref, wsem.at[6]),
        pltpu.make_async_copy(len_hbm, len_ref, wsem.at[7]),
    ]

    def first_loads():
        for c in (*tables, loads[4]):
            c.start()

    count = [0]
    started = []

    def send(src, dst, device):
        i = count[0]
        count[0] += 1
        if i >= SEND_SLOTS:
            started[i - SEND_SLOTS].wait_send()
        c = pltpu.make_async_remote_copy(
            src_ref=src, dst_ref=dst, send_sem=ss.at[i % SEND_SLOTS], recv_sem=rs.at[i], device_id=device, device_id_type=MESH
        )
        c.start()
        started.append(c)
        return c

    barrier = pltpu.get_barrier_semaphore()
    peers = [partner, y_peer, *z_peer.values(), *z_cross.values(), *z_far.values(), *x_peer.values()]
    for p in peers:
        pl.semaphore_signal(barrier, inc=1, device_id=p, device_id_type=MESH)

    rows = tok_ref.shape[0]

    def choose():
        for c in tables:
            c.wait()
        lane = lax.broadcasted_iota(jnp.int32, (rows, LANES), 1)
        place = jnp.bitwise_and(lane, 15)
        plane = jnp.bitwise_xor(z, jnp.bitwise_and(lax.shift_right_logical(lane, 4), 3))
        expert = (2 * plane + jnp.where(lane < 64, g, 1 - g)).astype(f32)
        ahead = lax.broadcasted_iota(jnp.int32, (rows, rows), 1)
        behind = lax.broadcasted_iota(jnp.int32, (rows, rows), 0)
        before = (ahead < behind).astype(f32).astype(bf16)
        unit = (ahead == behind).astype(f32)
        upright = lambda v: lax.dot_general(
            unit, v, (((1,), (1,)), ((), ())), precision=lax.Precision.HIGHEST, preferred_element_type=f32
        )
        named_here, weight_here = upright(routes_ref[...].astype(f32)), upright(rw_ref[...])
        first, second_one = named_here[:, 0:1] == expert, named_here[:, 1:2] == expert
        named = first | second_one
        earlier = dot(before, jnp.where(named, 1.0, 0.0).astype(bf16))
        here = named & (place < CAP) & (earlier == place.astype(f32))
        picks[...] = jnp.where(here, 1.0, 0.0).astype(bf16)
        weights = jnp.where(here, jnp.where(first, weight_here[:, 0:1], weight_here[:, 1:2]), 0.0)
        high = weights.astype(bf16)
        w_high[...] = high
        w_low[...] = (weights - high.astype(f32)).astype(bf16)

    def load():
        for c in loads[:4]:
            c.start()

    attend(
        first_loads, load, choose, len_ref, tok_hbm, key_hbm, value_hbm, gate_hbm, mix_hbm, wq_hbm, wk_hbm, wv_hbm, wf_hbm, wo_hbm,
        part_ref, *scratch[:ATTEND_SCRATCH],
    )
    loads[4].wait()
    pl.semaphore_wait(barrier, len(peers))
    c_part = send(part_ref, other_part, partner)

    c_part.wait_recv()
    total = tok_ref[...].astype(f32) + (part_ref[...].astype(f32) + other_part[...].astype(f32))
    res_b = total.astype(bf16)
    res[0] = res_b[:, :HALF]
    res[1] = res_b[:, HALF:]
    expert_in = rms(res_b.astype(f32), gain[...]).astype(bf16)
    xe[0] = expert_in[:, :HALF]
    xe[1] = expert_in[:, HALF:]
    pk[...] = lax.dot_general(
        picks[...], xe[t], (((0,), (0,)), ((), ())), preferred_element_type=f32
    ).astype(bf16).reshape(8, 16, HALF)
    sb[0, 0] = pk[0]
    c_s0 = {k: send(pk.at[k], sb.at[0, k], z_peer[k]) for k in near}
    c_s1 = {k: send(pk.at[4 + k], sb.at[1, k], z_cross[k]) for k in (0, 1, 3, 2)}
    r_i = lax.broadcasted_iota(jnp.int32, (BLOCK, 64), 0)
    c_i = lax.broadcasted_iota(jnp.int32, (BLOCK, 64), 1)
    r_k = lax.shift_right_logical(r_i * 43, 9)
    tight = (c_i == 16 * r_k + (r_i - CAP * r_k)).astype(f32).astype(bf16)

    mine_at = lambda d, q: xf.at[t, d, q]
    fwd = {}

    def forward(d, q):
        fwd[d, q] = send(mine_at(d, q), mine_at(d, q), partner)

    for k in near:
        c_s0[k].wait_recv()
    xf[t, 0, 0] = dot(tight, sb[0].reshape(64, HALF)).astype(bf16)
    c_ax, c_ay, c_bx = {}, {}, {}

    def ax(d):
        c_ax[d] = send(mine_at(0, 0), mine_at(d, 0), x_peer[d])

    def bx(d, q):
        c_bx[d, q] = send(mine_at(0, q), mine_at(d, q), x_peer[d])

    def ay(d):
        if d:
            c_ax[d].wait_recv()
        c_ay[d] = send(mine_at(d, 0), mine_at(d, 1), y_peer)
        forward(d, 0)

    ax(2)
    ay(0)
    for k in (0, 1, 3, 2):
        c_s1[k].wait_recv()
    xf[t, 0, 2] = dot(tight, sb[1].reshape(64, HALF)).astype(bf16)
    c_by = send(mine_at(0, 2), mine_at(0, 3), y_peer)
    bx(2, 2)
    ax(1)
    ax(3)
    forward(0, 2)
    ay(2)
    c_ay[0].wait_recv()
    forward(0, 1)
    c_by.wait_recv()
    bx(2, 3)
    forward(0, 3)
    bx(1, 2)
    bx(3, 2)
    bx(1, 3)
    bx(3, 3)
    ay(1)
    ay(3)
    for c in loads[:4]:
        c.wait()
    c_pi = {}

    def hide(d):
        for q in range(4):
            fwd[d, q].wait_recv()
        x0, x1 = xf[0, d].reshape(CHUNK, HALF), xf[1, d].reshape(CHUNK, HALF)
        gate = dot(x0, wg[0:HALF]) + dot(x1, wg[HALF : 2 * HALF])
        up = dot(x0, wu[0:HALF]) + dot(x1, wu[HALF : 2 * HALF])
        hid[d] = (gate / (1.0 + jnp.exp(-gate)) * up).astype(bf16)

    def down(d):
        po[d] = dot(hid[d], wd[1 - t]).astype(bf16)
        c_pi[d] = send(po.at[d], pi.at[d], partner)
        pm[d] = dot(hid[d], wd[t])

    def compute(d):
        hide(d)
        down(d)

    c_ry, c_xc, c_xo = {}, {}, {}

    def arrive(d):
        c_bx[d, 2].wait_recv()
        forward(d, 2)
        c_ay[d].wait_recv()
        forward(d, 1)
        c_bx[d, 3].wait_recv()
        forward(d, 3)

    side = {1: pl.ds(HALF // 2, HALF // 2), 3: pl.ds(0, HALF // 2)}

    def finish(d):
        c_pi[d].wait_recv()
        ys[d] = (pm[d] + pi[d].astype(f32)).astype(bf16).reshape(4, BLOCK, HALF)
        c_ry[d] = send(ys.at[d, 1], ry.at[d], y_peer)
        if d == 2:
            for n in (1, 3):
                c_xc[2, n] = send(ys.at[2, pl.ds(2, 2), :, side[4 - n]], hop_c.at[n], x_peer[n])

    def across(d):
        c_xc[2, 4 - d].wait_recv()
        ys[d, 2:4, :, side[d]] = (ys[d, 2:4, :, side[d]].astype(f32) + hop_c[4 - d].astype(f32)).astype(bf16)
        c_xc[d] = send(ys.at[d, pl.ds(2, 2)], rxc.at[d], x_peer[d])

    def second(d):
        c_ry[d].wait_recv()
        zs_out[d] = (ys[d, 0].astype(f32) + ry[d].astype(f32)).astype(bf16)
        if d == 2:
            for n in (1, 3):
                c_xo[2, n] = send(zs_out.at[2, :, side[4 - n]], hop_o.at[n], x_peer[n])
        elif d:
            c_xo[2, 4 - d].wait_recv()
            zs_out[d, :, side[d]] = (zs_out[d, :, side[d]].astype(f32) + hop_o[4 - d].astype(f32)).astype(bf16)
            c_xo[d] = send(zs_out.at[d], rxo.at[d], x_peer[d])

    compute(0)
    arrive(2)
    hide(2)
    arrive(1)
    down(2)
    finish(0)
    hide(1)
    finish(2)
    arrive(3)
    down(1)
    hide(3)
    finish(1)
    down(3)
    across(1)
    second(2)
    finish(3)
    across(3)
    second(1)
    second(3)
    second(0)


    for d in (1, 3):
        c_xc[d].wait_recv()
    crossed = ys[0, 2:4].astype(f32) + rxc[1].astype(f32) + rxc[3].astype(f32)
    spread = lambda v: lax.dot_general(
        tight, v.astype(bf16), (((0,), (0,)), ((), ())), preferred_element_type=f32
    ).astype(bf16).reshape(4, 16, HALF)
    er[1] = spread(crossed[0])
    er[2] = spread(crossed[1])
    order = (2, 1, 3, 0)
    c_r = [send(er.at[1, k], rb.at[1, k], z_cross[k]) for k in order]
    c_r += [send(er.at[2, k], rb.at[2, k], z_far[k]) for k in order]
    for d in (1, 3):
        c_xo[d].wait_recv()
    own = zs_out[0].astype(f32) + rxo[1].astype(f32) + rxo[3].astype(f32)
    er[0] = spread(own)
    rb[0, 0] = er[0, 0]
    c_r += [send(er.at[0, k], rb.at[0, k], z_peer[k]) for k in order[:3]]
    mixture = res[t].astype(f32)
    for c in c_r[:8]:
        c.wait_recv()
    weigh = lambda a, v: dot(w_high[:, a : a + 64], v) + dot(w_low[:, a : a + 64], v)
    for i in (1, 2):
        mixture = mixture + weigh(64, rb[i].reshape(64, HALF))
    for c in c_r[8:]:
        c.wait_recv()
    mixture = mixture + weigh(0, rb[0].reshape(64, HALF))
    fo[t] = mixture.astype(bf16)
    c_fo = send(fo.at[t], fo.at[t], partner)
    c_fo.wait_recv()
    out_ref[:, 0:HALF] = fo[0]
    out_ref[:, HALF : 2 * HALF] = fo[1]
    for c in started[-SEND_SLOTS:]:
        c.wait_send()


def on_device(
    tokens, lengths, key_cache, value_cache, gate_cache, mix_gain, query_weight, key_weight, value_weight,
    forget_weight, out_weight, expert_gain, routes, route_weights, expert_gate, expert_up, expert_down,
):
    rows, width = tokens.shape
    f32, bf16 = jnp.float32, jnp.bfloat16
    any_space = pl.BlockSpec(memory_space=pl.ANY)
    vmem = pl.BlockSpec(memory_space=pltpu.VMEM)
    blocks = lambda *s: pltpu.VMEM((*s, BLOCK, HALF), bf16)
    heads = pltpu.VMEM((SEQS * HEADS_HERE, LANES), f32)
    forget = forget_weight.T
    return pl.pallas_call(
        layer_kernel,
        out_shape=pltpu.VMEM((rows, width), bf16),
        in_specs=[any_space] * 17,
        out_specs=vmem,
        scratch_shapes=[
            pltpu.VMEM((rows, width), bf16),
            pltpu.VMEM((rows, width), bf16),
            pltpu.VMEM((1, width), f32),
            pltpu.VMEM(query_weight.shape, bf16),
            pltpu.VMEM(key_weight.shape, bf16),
            pltpu.VMEM(value_weight.shape, bf16),
            pltpu.VMEM(forget.shape, bf16),
            pltpu.VMEM(out_weight.shape, bf16),
            pltpu.VMEM(key_cache.shape, bf16),
            pltpu.VMEM(value_cache.shape, bf16),
            pltpu.VMEM(gate_cache.shape, f32),
            heads,
            heads,
            heads,
            pltpu.VMEM((SEQS, LANES), f32),
            heads,
            pltpu.SemaphoreType.DMA((7,)),
            pltpu.SemaphoreType.DMA((3, KV_BLOCKS)),
            pltpu.SMEM((rows,), jnp.int32),
            pltpu.VMEM((2, rows), jnp.int32),
            pltpu.VMEM((2, rows), f32),
            pltpu.VMEM((1, width), f32),
            pltpu.VMEM(expert_gate.shape, bf16),
            pltpu.VMEM(expert_up.shape, bf16),
            pltpu.VMEM((2, expert_down.shape[0], HALF), bf16),
            pltpu.VMEM((rows, width), bf16),
            pltpu.VMEM((2, rows, HALF), bf16),
            pltpu.VMEM((2, rows, HALF), bf16),
            pltpu.VMEM((rows, LANES), bf16),
            pltpu.VMEM((rows, LANES), bf16),
            pltpu.VMEM((rows, LANES), bf16),
            pltpu.VMEM((8, 16, HALF), bf16),
            pltpu.VMEM((2, 4, 16, HALF), bf16),
            blocks(2, 4, 4),
            pltpu.VMEM((4, CHUNK, HALF), f32),
            pltpu.VMEM((4, CHUNK, HALF), bf16),
            pltpu.VMEM((4, CHUNK, HALF), bf16),
            blocks(4, 4),
            blocks(4),
            blocks(4),
            blocks(4),
            blocks(4, 2),
            pltpu.VMEM((3, 4, 16, HALF), bf16),
            pltpu.VMEM((3, 4, 16, HALF), bf16),
            pltpu.VMEM((2, rows, HALF), bf16),
            pltpu.VMEM((4, CHUNK, expert_gate.shape[1]), bf16),
            pltpu.VMEM((4, 2, BLOCK, HALF // 2), bf16),
            pltpu.VMEM((4, BLOCK, HALF // 2), bf16),
            pltpu.SemaphoreType.DMA((8,)),
            pltpu.SemaphoreType.DMA((SEND_SLOTS,)),
            pltpu.SemaphoreType.DMA((COPIES,)),
        ],
        compiler_params=pltpu.CompilerParams(
            collective_id=0, has_side_effects=True, vmem_limit_bytes=60 * 1024 * 1024
        ),
        cost_estimate=pl.CostEstimate(flops=5_500_000_000, bytes_accessed=30_000_000, transcendentals=700_000),
        name="decode_layer",
    )(
        lengths, tokens, key_cache, value_cache, gate_cache, mix_gain.reshape(1, width), query_weight, key_weight,
        value_weight, forget, out_weight, expert_gain.reshape(1, width), routes.T, route_weights.T,
        expert_gate, expert_up, expert_down,
    )


def solution(mesh):
    return jax.shard_map(
        on_device,
        mesh=mesh,
        in_specs=(
            P("ep", None),
            P("ep"),
            P("ep", None, "tp"),
            P("ep", None, "tp"),
            P("ep", "tp", None),
            P(),
            P(None, "tp"),
            P(None, "tp"),
            P(None, "tp"),
            P(None, "tp"),
            P("tp", None),
            P(),
            P("ep", None),
            P("ep", None),
            P(None, ("ep", "tp")),
            P(None, ("ep", "tp")),
            P(("ep", "tp"), None),
        ),
        out_specs=P("ep", None),
        check_vma=False,
    )
```

```python
import functools
import jax
import jax.numpy as jnp
from jax import lax
from jax.experimental import pallas as pl
from jax.experimental.pallas import tpu as pltpu
from jax.sharding import PartitionSpec as P

SEQS = 32
POS = 1024
LANES = 128
HEADS_HERE = 8
KV_BLOCKS = 4


def rms(values, gain):
    return values * lax.rsqrt(jnp.mean(values * values, axis=-1, keepdims=True) + 1e-06) * gain


def attend(
    first, then, meanwhile, len_ref, tok_hbm, key_hbm, value_hbm, gate_hbm, gain_hbm, wq_hbm, wk_hbm, wv_hbm, wf_hbm, wo_hbm,
    out_ref,
    tok, gain, wq, wk, wv, wf, wo, keys, values, gates, qs, owns, lgs, vnew, mixed, sems, kv_sems,
):
    blocks, per = kv_sems.shape[1], SEQS // kv_sems.shape[1]
    small = [(tok_hbm, tok), (gain_hbm, gain), (wq_hbm, wq), (wk_hbm, wk), (wv_hbm, wv), (wf_hbm, wf), (wo_hbm, wo)]
    copies = [pltpu.make_async_copy(a, b, sems.at[i]) for i, (a, b) in enumerate(small)]

    def block_copies(b):
        rows = pl.ds(b * per, per)
        return [
            pltpu.make_async_copy(src.at[rows], dst.at[rows], kv_sems.at[i, b])
            for i, (src, dst) in enumerate(((key_hbm, keys), (gate_hbm, gates), (value_hbm, values)))
        ]

    copies[0].start()
    copies[1].start()
    first()
    for c in copies[2:6]:
        c.start()
    meanwhile()
    with jax.named_scope("wait_tok"):
        copies[0].wait()
        copies[1].wait()
    for b in range(2):
        for c in block_copies(b):
            c.start()
    ni = rms(tok[...].astype(jnp.float32), gain[...]).astype(jnp.bfloat16)
    lane = lax.broadcasted_iota(jnp.int32, (SEQS, LANES), 1)
    left = lane < 64
    with jax.named_scope("wait_w"):
        for c in copies[2:6]:
            c.wait()
    for b in range(2, blocks):
        for c in block_copies(b):
            c.start()
    copies[6].start()
    dot = functools.partial(jnp.dot, preferred_element_type=jnp.float32)
    q = dot(ni, wq[...]).astype(jnp.bfloat16).astype(jnp.float32) * 0.125
    kn = dot(ni, wk[...]).astype(jnp.bfloat16).astype(jnp.float32)
    vnew[...] = dot(ni, wv[...]).astype(jnp.bfloat16).astype(jnp.float32)
    f = lax.dot_general(ni, wf[...], (((1,), (1,)), ((), ())), preferred_element_type=jnp.float32)
    lg = jnp.minimum(f, 0.0) - jnp.log1p(jnp.exp(-jnp.abs(f)))
    for h in range(HEADS_HERE):
        column = q[:, 128 * (h // 2) : 128 * (h // 2) + 128]
        if h % 2 != h // 4:
            column = pltpu.roll(column, 64, 1)
        column = jnp.where(left if h < 4 else ~left, column, 0.0)
        rows = pl.ds(h, SEQS, stride=HEADS_HERE)
        qs[rows, :] = column
        owns[rows, :] = jnp.broadcast_to(jnp.sum(column * kn, axis=1, keepdims=True), (SEQS, LANES))
        lgs[rows, :] = jnp.broadcast_to(lg[:, h : h + 1], (SEQS, LANES))

    position = lax.broadcasted_iota(jnp.int32, (HEADS_HERE, POS), 1)

    def block(b, carry):
        with jax.named_scope("wait_kv"):
            for c in block_copies(b):
                c.wait()
        seqs = [b * per + j for j in range(per)]
        rows = [pl.ds(s * HEADS_HERE, HEADS_HERE) for s in seqs]
        scores = [
            lax.dot_general(
                qs[r, :].astype(jnp.bfloat16), keys[s], (((1,), (1,)), ((), ())),
                preferred_element_type=jnp.float32,
            )
            for s, r in zip(seqs, rows)
        ]
        raised, scale, own_part = [], [], []
        for s, r, score in zip(seqs, rows, scores):
            length = len_ref[s]
            g = gates[s]
            latest = jnp.sum(jnp.where(position == length - 1, g, 0.0), axis=1, keepdims=True)
            own = owns[r, 0:1]
            score = jnp.where(position < length, score + (latest + lgs[r, 0:1]) - g, -jnp.inf)
            top = jnp.maximum(jnp.max(score, axis=1, keepdims=True), own)
            lifted = jnp.exp(score - top)
            own_raised = jnp.exp(own - top)
            raised.append(lifted.astype(jnp.bfloat16))
            scale.append(1.0 / (jnp.sum(lifted, axis=1, keepdims=True) + own_raised))
            own_part.append(own_raised * vnew[pl.ds(s, 1), :])
        sums = [dot(p, values[s]) for p, s in zip(raised, seqs)]
        for r, o, c, w in zip(rows, sums, scale, own_part):
            mixed[r, :] = (o + w) * c
        return carry

    with jax.named_scope("loop"):
        lax.fori_loop(0, blocks, block, 0)
    then()
    parts = []
    for c in range(4):
        pair = []
        for h in (2 * c, 2 * c + 1):
            o = mixed[pl.ds(h, SEQS, stride=HEADS_HERE), :]
            pair.append(pltpu.roll(o, 64, 1) if h % 2 != h // 4 else o)
        parts.append(jnp.where(left, pair[0], pair[1]).astype(jnp.bfloat16))
    with jax.named_scope("wait_wo"):
        copies[6].wait()
    out_ref[...] = dot(jnp.concatenate(parts, axis=1), wo[...]).astype(jnp.bfloat16)


MESH = pl.DeviceIdType.MESH
CAP = 12
HALF = 1024
BLOCK = 48
CHUNK = 4 * BLOCK
SEND_SLOTS = 26
COPIES = 66


ATTEND_SCRATCH = 17


def layer_kernel(
    len_hbm, tok_hbm, key_hbm, value_hbm, gate_hbm, mix_hbm, wq_hbm, wk_hbm, wv_hbm, wf_hbm, wo_hbm,
    gain_hbm, routes_hbm, rw_hbm, wg_hbm, wu_hbm, wd_hbm,
    out_ref,
    part_ref, *scratch,
):
    (
        len_ref, routes_ref, rw_ref, gain, wg, wu, wd, other_part, res, xe, picks, w_high, w_low, pk, sb, xf,
        pm, po, pi, ys, ry, zs_out, rxo, rxc, er, rb, fo, hid, hop_c, hop_o,
        wsem, ss, rs,
    ) = scratch[ATTEND_SCRATCH:]
    tok_ref = scratch[0]
    f32, bf16 = jnp.float32, jnp.bfloat16
    dot = functools.partial(jnp.dot, preferred_element_type=f32)
    e, t = lax.axis_index("ep"), lax.axis_index("tp")
    z, y, x = e // 16, lax.rem(e // 4, 4), lax.rem(e, 4)
    g = y // 2

    def chip(zz, yy, xx):
        return (zz * 16 + yy * 4 + xx, t)

    partner = (e, 1 - t)
    z_peer = {k: chip(jnp.bitwise_xor(z, k), y, x) for k in (1, 2, 3)}
    x_peer = {k: chip(z, y, jnp.bitwise_xor(x, k)) for k in (1, 2, 3)}
    y_peer = chip(z, jnp.bitwise_xor(y, 1), x)
    z_cross = {k: chip(jnp.bitwise_xor(z, k), 3 - y, x) for k in range(4)}
    z_far = {k: chip(jnp.bitwise_xor(z, k), jnp.bitwise_xor(y, 2), x) for k in range(4)}
    near = (1, 3, 2)

    loads = [
        pltpu.make_async_copy(wg_hbm, wg, wsem.at[0]),
        pltpu.make_async_copy(wu_hbm, wu, wsem.at[1]),
        pltpu.make_async_copy(wd_hbm.at[:, pl.ds(0, HALF)], wd.at[0], wsem.at[2]),
        pltpu.make_async_copy(wd_hbm.at[:, pl.ds(HALF, HALF)], wd.at[1], wsem.at[3]),
        pltpu.make_async_copy(gain_hbm, gain, wsem.at[4]),
    ]
    tables = [
        pltpu.make_async_copy(routes_hbm, routes_ref, wsem.at[5]),
        pltpu.make_async_copy(rw_hbm, rw_ref, wsem.at[6]),
        pltpu.make_async_copy(len_hbm, len_ref, wsem.at[7]),
    ]

    def first_loads():
        for c in (*tables, loads[4]):
            c.start()

    count = [0]
    started = []

    def send(src, dst, device):
        i = count[0]
        count[0] += 1
        if i >= SEND_SLOTS:
            started[i - SEND_SLOTS].wait_send()
        c = pltpu.make_async_remote_copy(
            src_ref=src, dst_ref=dst, send_sem=ss.at[i % SEND_SLOTS], recv_sem=rs.at[i], device_id=device, device_id_type=MESH
        )
        c.start()
        started.append(c)
        return c

    barrier = pltpu.get_barrier_semaphore()
    peers = [partner, y_peer, *z_peer.values(), *z_cross.values(), *z_far.values(), *x_peer.values()]
    for p in peers:
        pl.semaphore_signal(barrier, inc=1, device_id=p, device_id_type=MESH)

    rows = tok_ref.shape[0]

    def choose():
        for c in tables:
            c.wait()
        lane = lax.broadcasted_iota(jnp.int32, (rows, LANES), 1)
        place = jnp.bitwise_and(lane, 15)
        plane = jnp.bitwise_xor(z, jnp.bitwise_and(lax.shift_right_logical(lane, 4), 3))
        expert = (2 * plane + jnp.where(lane < 64, g, 1 - g)).astype(f32)
        ahead = lax.broadcasted_iota(jnp.int32, (rows, rows), 1)
        behind = lax.broadcasted_iota(jnp.int32, (rows, rows), 0)
        before = (ahead < behind).astype(f32).astype(bf16)
        unit = (ahead == behind).astype(f32)
        upright = lambda v: lax.dot_general(
            unit, v, (((1,), (1,)), ((), ())), precision=lax.Precision.HIGHEST, preferred_element_type=f32
        )
        named_here, weight_here = upright(routes_ref[...].astype(f32)), upright(rw_ref[...])
        first, second_one = named_here[:, 0:1] == expert, named_here[:, 1:2] == expert
        named = first | second_one
        earlier = dot(before, jnp.where(named, 1.0, 0.0).astype(bf16))
        here = named & (place < CAP) & (earlier == place.astype(f32))
        picks[...] = jnp.where(here, 1.0, 0.0).astype(bf16)
        weights = jnp.where(here, jnp.where(first, weight_here[:, 0:1], weight_here[:, 1:2]), 0.0)
        high = weights.astype(bf16)
        w_high[...] = high
        w_low[...] = (weights - high.astype(f32)).astype(bf16)

    def load():
        for c in loads[:4]:
            c.start()

    attend(
        first_loads, load, choose, len_ref, tok_hbm, key_hbm, value_hbm, gate_hbm, mix_hbm, wq_hbm, wk_hbm, wv_hbm, wf_hbm, wo_hbm,
        part_ref, *scratch[:ATTEND_SCRATCH],
    )
    loads[4].wait()
    pl.semaphore_wait(barrier, len(peers))
    c_part = send(part_ref, other_part, partner)

    c_part.wait_recv()
    total = tok_ref[...].astype(f32) + (part_ref[...].astype(f32) + other_part[...].astype(f32))
    res_b = total.astype(bf16)
    res[0] = res_b[:, :HALF]
    res[1] = res_b[:, HALF:]
    expert_in = rms(res_b.astype(f32), gain[...]).astype(bf16)
    xe[0] = expert_in[:, :HALF]
    xe[1] = expert_in[:, HALF:]
    pk[...] = lax.dot_general(
        picks[...], xe[t], (((0,), (0,)), ((), ())), preferred_element_type=f32
    ).astype(bf16).reshape(8, 16, HALF)
    sb[0, 0] = pk[0]
    c_s0 = {k: send(pk.at[k], sb.at[0, k], z_peer[k]) for k in (2, 1, 3)}
    c_s1 = {k: send(pk.at[4 + k], sb.at[1, k], z_cross[k]) for k in (2, 1, 3, 0)}
    r_i = lax.broadcasted_iota(jnp.int32, (BLOCK, 64), 0)
    c_i = lax.broadcasted_iota(jnp.int32, (BLOCK, 64), 1)
    r_k = lax.shift_right_logical(r_i * 43, 9)
    tight = (c_i == 16 * r_k + (r_i - CAP * r_k)).astype(f32).astype(bf16)

    mine_at = lambda d, q: xf.at[t, d, q]
    fwd = {}

    def forward(d, q):
        fwd[d, q] = send(mine_at(d, q), mine_at(d, q), partner)

    for k in near:
        c_s0[k].wait_recv()
    xf[t, 0, 0] = dot(tight, sb[0].reshape(64, HALF)).astype(bf16)
    c_ax, c_ay, c_bx = {}, {}, {}

    def ax(d):
        c_ax[d] = send(mine_at(0, 0), mine_at(d, 0), x_peer[d])

    def bx(d, q):
        c_bx[d, q] = send(mine_at(0, q), mine_at(d, q), x_peer[d])

    def ay(d):
        if d:
            c_ax[d].wait_recv()
        c_ay[d] = send(mine_at(d, 0), mine_at(d, 1), y_peer)
        forward(d, 0)

    ax(2)
    ay(0)
    for k in (0, 1, 3, 2):
        c_s1[k].wait_recv()
    xf[t, 0, 2] = dot(tight, sb[1].reshape(64, HALF)).astype(bf16)
    c_by = send(mine_at(0, 2), mine_at(0, 3), y_peer)
    bx(2, 2)
    ax(1)
    ax(3)
    forward(0, 2)
    ay(2)
    c_ay[0].wait_recv()
    forward(0, 1)
    c_by.wait_recv()
    bx(2, 3)
    forward(0, 3)
    bx(1, 2)
    bx(3, 2)
    bx(1, 3)
    bx(3, 3)
    ay(1)
    ay(3)
    for c in loads[:4]:
        c.wait()
    c_pi = {}

    def hide(d):
        for q in range(4):
            fwd[d, q].wait_recv()
        x0, x1 = xf[0, d].reshape(CHUNK, HALF), xf[1, d].reshape(CHUNK, HALF)
        gate = dot(x0, wg[0:HALF]) + dot(x1, wg[HALF : 2 * HALF])
        up = dot(x0, wu[0:HALF]) + dot(x1, wu[HALF : 2 * HALF])
        hid[d] = (gate / (1.0 + jnp.exp(-gate)) * up).astype(bf16)

    def down(d):
        po[d] = dot(hid[d], wd[1 - t]).astype(bf16)
        c_pi[d] = send(po.at[d], pi.at[d], partner)
        pm[d] = dot(hid[d], wd[t])

    def compute(d):
        hide(d)
        down(d)

    c_ry, c_xc, c_xo = {}, {}, {}

    def arrive(d):
        c_bx[d, 2].wait_recv()
        forward(d, 2)
        c_ay[d].wait_recv()
        forward(d, 1)
        c_bx[d, 3].wait_recv()
        forward(d, 3)

    side = {1: pl.ds(HALF // 2, HALF // 2), 3: pl.ds(0, HALF // 2)}

    def finish(d):
        c_pi[d].wait_recv()
        ys[d] = (pm[d] + pi[d].astype(f32)).astype(bf16).reshape(4, BLOCK, HALF)
        c_ry[d] = send(ys.at[d, 1], ry.at[d], y_peer)
        if d == 2:
            for n in (1, 3):
                c_xc[2, n] = send(ys.at[2, pl.ds(2, 2), :, side[4 - n]], hop_c.at[n], x_peer[n])

    def across(d):
        c_xc[2, 4 - d].wait_recv()
        ys[d, 2:4, :, side[d]] = (ys[d, 2:4, :, side[d]].astype(f32) + hop_c[4 - d].astype(f32)).astype(bf16)
        c_xc[d] = send(ys.at[d, pl.ds(2, 2)], rxc.at[d], x_peer[d])

    def second(d):
        c_ry[d].wait_recv()
        zs_out[d] = (ys[d, 0].astype(f32) + ry[d].astype(f32)).astype(bf16)
        if d == 2:
            for n in (1, 3):
                c_xo[2, n] = send(zs_out.at[2, :, side[4 - n]], hop_o.at[n], x_peer[n])
        elif d:
            c_xo[2, 4 - d].wait_recv()
            zs_out[d, :, side[d]] = (zs_out[d, :, side[d]].astype(f32) + hop_o[4 - d].astype(f32)).astype(bf16)
            c_xo[d] = send(zs_out.at[d], rxo.at[d], x_peer[d])

    compute(0)
    arrive(2)
    hide(2)
    arrive(1)
    down(2)
    finish(0)
    hide(1)
    finish(2)
    arrive(3)
    down(1)
    hide(3)
    finish(1)
    down(3)
    across(1)
    second(2)
    finish(3)
    across(3)
    second(1)
    second(3)
    second(0)


    for d in (1, 3):
        c_xc[d].wait_recv()
    crossed = ys[0, 2:4].astype(f32) + rxc[1].astype(f32) + rxc[3].astype(f32)
    spread = lambda v: lax.dot_general(
        tight, v.astype(bf16), (((0,), (0,)), ((), ())), preferred_element_type=f32
    ).astype(bf16).reshape(4, 16, HALF)
    er[1] = spread(crossed[0])
    er[2] = spread(crossed[1])
    order = (2, 1, 3, 0)
    c_r = []
    for k in order:
        c_r.append(send(er.at[2, k], rb.at[2, k], z_far[k]))
        c_r.append(send(er.at[1, k], rb.at[1, k], z_cross[k]))
    for d in (1, 3):
        c_xo[d].wait_recv()
    own = zs_out[0].astype(f32) + rxo[1].astype(f32) + rxo[3].astype(f32)
    er[0] = spread(own)
    rb[0, 0] = er[0, 0]
    c_r += [send(er.at[0, k], rb.at[0, k], z_peer[k]) for k in order[:3]]
    mixture = res[t].astype(f32)
    for c in c_r[:8]:
        c.wait_recv()
    weigh = lambda a, v: dot(w_high[:, a : a + 64], v) + dot(w_low[:, a : a + 64], v)
    for i in (1, 2):
        mixture = mixture + weigh(64, rb[i].reshape(64, HALF))
    for c in c_r[8:]:
        c.wait_recv()
    mixture = mixture + weigh(0, rb[0].reshape(64, HALF))
    fo[t] = mixture.astype(bf16)
    c_fo = send(fo.at[t], fo.at[t], partner)
    c_fo.wait_recv()
    out_ref[:, 0:HALF] = fo[0]
    out_ref[:, HALF : 2 * HALF] = fo[1]
    for c in started[-SEND_SLOTS:]:
        c.wait_send()


def on_device(
    tokens, lengths, key_cache, value_cache, gate_cache, mix_gain, query_weight, key_weight, value_weight,
    forget_weight, out_weight, expert_gain, routes, route_weights, expert_gate, expert_up, expert_down,
):
    rows, width = tokens.shape
    f32, bf16 = jnp.float32, jnp.bfloat16
    any_space = pl.BlockSpec(memory_space=pl.ANY)
    vmem = pl.BlockSpec(memory_space=pltpu.VMEM)
    blocks = lambda *s: pltpu.VMEM((*s, BLOCK, HALF), bf16)
    heads = pltpu.VMEM((SEQS * HEADS_HERE, LANES), f32)
    forget = forget_weight.T
    return pl.pallas_call(
        layer_kernel,
        out_shape=pltpu.VMEM((rows, width), bf16),
        in_specs=[any_space] * 17,
        out_specs=vmem,
        scratch_shapes=[
            pltpu.VMEM((rows, width), bf16),
            pltpu.VMEM((rows, width), bf16),
            pltpu.VMEM((1, width), f32),
            pltpu.VMEM(query_weight.shape, bf16),
            pltpu.VMEM(key_weight.shape, bf16),
            pltpu.VMEM(value_weight.shape, bf16),
            pltpu.VMEM(forget.shape, bf16),
            pltpu.VMEM(out_weight.shape, bf16),
            pltpu.VMEM(key_cache.shape, bf16),
            pltpu.VMEM(value_cache.shape, bf16),
            pltpu.VMEM(gate_cache.shape, f32),
            heads,
            heads,
            heads,
            pltpu.VMEM((SEQS, LANES), f32),
            heads,
            pltpu.SemaphoreType.DMA((7,)),
            pltpu.SemaphoreType.DMA((3, KV_BLOCKS)),
            pltpu.SMEM((rows,), jnp.int32),
            pltpu.VMEM((2, rows), jnp.int32),
            pltpu.VMEM((2, rows), f32),
            pltpu.VMEM((1, width), f32),
            pltpu.VMEM(expert_gate.shape, bf16),
            pltpu.VMEM(expert_up.shape, bf16),
            pltpu.VMEM((2, expert_down.shape[0], HALF), bf16),
            pltpu.VMEM((rows, width), bf16),
            pltpu.VMEM((2, rows, HALF), bf16),
            pltpu.VMEM((2, rows, HALF), bf16),
            pltpu.VMEM((rows, LANES), bf16),
            pltpu.VMEM((rows, LANES), bf16),
            pltpu.VMEM((rows, LANES), bf16),
            pltpu.VMEM((8, 16, HALF), bf16),
            pltpu.VMEM((2, 4, 16, HALF), bf16),
            blocks(2, 4, 4),
            pltpu.VMEM((4, CHUNK, HALF), f32),
            pltpu.VMEM((4, CHUNK, HALF), bf16),
            pltpu.VMEM((4, CHUNK, HALF), bf16),
            blocks(4, 4),
            blocks(4),
            blocks(4),
            blocks(4),
            blocks(4, 2),
            pltpu.VMEM((3, 4, 16, HALF), bf16),
            pltpu.VMEM((3, 4, 16, HALF), bf16),
            pltpu.VMEM((2, rows, HALF), bf16),
            pltpu.VMEM((4, CHUNK, expert_gate.shape[1]), bf16),
            pltpu.VMEM((4, 2, BLOCK, HALF // 2), bf16),
            pltpu.VMEM((4, BLOCK, HALF // 2), bf16),
            pltpu.SemaphoreType.DMA((8,)),
            pltpu.SemaphoreType.DMA((SEND_SLOTS,)),
            pltpu.SemaphoreType.DMA((COPIES,)),
        ],
        compiler_params=pltpu.CompilerParams(
            collective_id=0, has_side_effects=True, vmem_limit_bytes=60 * 1024 * 1024
        ),
        cost_estimate=pl.CostEstimate(flops=5_500_000_000, bytes_accessed=30_000_000, transcendentals=700_000),
        name="decode_layer",
    )(
        lengths, tokens, key_cache, value_cache, gate_cache, mix_gain.reshape(1, width), query_weight, key_weight,
        value_weight, forget, out_weight, expert_gain.reshape(1, width), routes.T, route_weights.T,
        expert_gate, expert_up, expert_down,
    )


def solution(mesh):
    return jax.shard_map(
        on_device,
        mesh=mesh,
        in_specs=(
            P("ep", None),
            P("ep"),
            P("ep", None, "tp"),
            P("ep", None, "tp"),
            P("ep", "tp", None),
            P(),
            P(None, "tp"),
            P(None, "tp"),
            P(None, "tp"),
            P(None, "tp"),
            P("tp", None),
            P(),
            P("ep", None),
            P("ep", None),
            P(None, ("ep", "tp")),
            P(None, ("ep", "tp")),
            P(("ep", "tp"), None),
        ),
        out_specs=P("ep", None),
        check_vma=False,
    )
```

```python
import functools
import jax
import jax.numpy as jnp
from jax import lax
from jax.experimental import pallas as pl
from jax.experimental.pallas import tpu as pltpu
from jax.sharding import PartitionSpec as P

SEQS = 32
POS = 1024
LANES = 128
HEADS_HERE = 8
KV_BLOCKS = 4


def rms(values, gain):
    return values * lax.rsqrt(jnp.mean(values * values, axis=-1, keepdims=True) + 1e-06) * gain


def attend(
    first, then, meanwhile, len_ref, tok_hbm, key_hbm, value_hbm, gate_hbm, gain_hbm, wq_hbm, wk_hbm, wv_hbm, wf_hbm, wo_hbm,
    out_ref,
    tok, gain, wq, wk, wv, wf, wo, keys, values, gates, qs, owns, lgs, vnew, mixed, sems, kv_sems,
):
    blocks, per = kv_sems.shape[1], SEQS // kv_sems.shape[1]
    small = [(tok_hbm, tok), (gain_hbm, gain), (wq_hbm, wq), (wk_hbm, wk), (wv_hbm, wv), (wf_hbm, wf), (wo_hbm, wo)]
    copies = [pltpu.make_async_copy(a, b, sems.at[i]) for i, (a, b) in enumerate(small)]

    def block_copies(b):
        rows = pl.ds(b * per, per)
        return [
            pltpu.make_async_copy(src.at[rows], dst.at[rows], kv_sems.at[i, b])
            for i, (src, dst) in enumerate(((key_hbm, keys), (gate_hbm, gates), (value_hbm, values)))
        ]

    copies[0].start()
    copies[1].start()
    first()
    for c in copies[2:6]:
        c.start()
    for c in block_copies(0):
        c.start()
    meanwhile()
    with jax.named_scope("wait_tok"):
        copies[0].wait()
        copies[1].wait()
    for c in block_copies(1):
        c.start()
    ni = rms(tok[...].astype(jnp.float32), gain[...]).astype(jnp.bfloat16)
    lane = lax.broadcasted_iota(jnp.int32, (SEQS, LANES), 1)
    left = lane < 64
    with jax.named_scope("wait_w"):
        for c in copies[2:6]:
            c.wait()
    for b in range(2, blocks):
        for c in block_copies(b):
            c.start()
    copies[6].start()
    dot = functools.partial(jnp.dot, preferred_element_type=jnp.float32)
    q = dot(ni, wq[...]).astype(jnp.bfloat16).astype(jnp.float32) * 0.125
    kn = dot(ni, wk[...]).astype(jnp.bfloat16).astype(jnp.float32)
    vnew[...] = dot(ni, wv[...]).astype(jnp.bfloat16).astype(jnp.float32)
    f = lax.dot_general(ni, wf[...], (((1,), (1,)), ((), ())), preferred_element_type=jnp.float32)
    lg = jnp.minimum(f, 0.0) - jnp.log1p(jnp.exp(-jnp.abs(f)))
    for h in range(HEADS_HERE):
        column = q[:, 128 * (h // 2) : 128 * (h // 2) + 128]
        if h % 2 != h // 4:
            column = pltpu.roll(column, 64, 1)
        column = jnp.where(left if h < 4 else ~left, column, 0.0)
        rows = pl.ds(h, SEQS, stride=HEADS_HERE)
        qs[rows, :] = column
        owns[rows, :] = jnp.broadcast_to(jnp.sum(column * kn, axis=1, keepdims=True), (SEQS, LANES))
        lgs[rows, :] = jnp.broadcast_to(lg[:, h : h + 1], (SEQS, LANES))

    position = lax.broadcasted_iota(jnp.int32, (HEADS_HERE, POS), 1)

    def block(b, carry):
        with jax.named_scope("wait_kv"):
            for c in block_copies(b):
                c.wait()
        seqs = [b * per + j for j in range(per)]
        rows = [pl.ds(s * HEADS_HERE, HEADS_HERE) for s in seqs]
        scores = [
            lax.dot_general(
                qs[r, :].astype(jnp.bfloat16), keys[s], (((1,), (1,)), ((), ())),
                preferred_element_type=jnp.float32,
            )
            for s, r in zip(seqs, rows)
        ]
        raised, scale, own_part = [], [], []
        for s, r, score in zip(seqs, rows, scores):
            length = len_ref[s]
            g = gates[s]
            latest = jnp.sum(jnp.where(position == length - 1, g, 0.0), axis=1, keepdims=True)
            own = owns[r, 0:1]
            score = jnp.where(position < length, score + (latest + lgs[r, 0:1]) - g, -jnp.inf)
            top = jnp.maximum(jnp.max(score, axis=1, keepdims=True), own)
            lifted = jnp.exp(score - top)
            own_raised = jnp.exp(own - top)
            raised.append(lifted.astype(jnp.bfloat16))
            scale.append(1.0 / (jnp.sum(lifted, axis=1, keepdims=True) + own_raised))
            own_part.append(own_raised * vnew[pl.ds(s, 1), :])
        sums = [dot(p, values[s]) for p, s in zip(raised, seqs)]
        for r, o, c, w in zip(rows, sums, scale, own_part):
            mixed[r, :] = (o + w) * c
        return carry

    with jax.named_scope("loop"):
        lax.fori_loop(0, blocks, block, 0)
    then()
    parts = []
    for c in range(4):
        pair = []
        for h in (2 * c, 2 * c + 1):
            o = mixed[pl.ds(h, SEQS, stride=HEADS_HERE), :]
            pair.append(pltpu.roll(o, 64, 1) if h % 2 != h // 4 else o)
        parts.append(jnp.where(left, pair[0], pair[1]).astype(jnp.bfloat16))
    with jax.named_scope("wait_wo"):
        copies[6].wait()
    out_ref[...] = dot(jnp.concatenate(parts, axis=1), wo[...]).astype(jnp.bfloat16)


MESH = pl.DeviceIdType.MESH
CAP = 12
HALF = 1024
BLOCK = 48
CHUNK = 4 * BLOCK
SEND_SLOTS = 26
COPIES = 66


ATTEND_SCRATCH = 17


def layer_kernel(
    len_hbm, tok_hbm, key_hbm, value_hbm, gate_hbm, mix_hbm, wq_hbm, wk_hbm, wv_hbm, wf_hbm, wo_hbm,
    gain_hbm, routes_hbm, rw_hbm, wg_hbm, wu_hbm, wd_hbm,
    out_ref,
    part_ref, *scratch,
):
    (
        len_ref, routes_ref, rw_ref, gain, wg, wu, wd, other_part, res, xe, picks, w_high, w_low, pk, sb, xf,
        pm, po, pi, ys, ry, zs_out, rxo, rxc, er, rb, fo, hid, hop_c, hop_o,
        wsem, ss, rs,
    ) = scratch[ATTEND_SCRATCH:]
    tok_ref = scratch[0]
    f32, bf16 = jnp.float32, jnp.bfloat16
    dot = functools.partial(jnp.dot, preferred_element_type=f32)
    e, t = lax.axis_index("ep"), lax.axis_index("tp")
    z, y, x = e // 16, lax.rem(e // 4, 4), lax.rem(e, 4)
    g = y // 2

    def chip(zz, yy, xx):
        return (zz * 16 + yy * 4 + xx, t)

    partner = (e, 1 - t)
    z_peer = {k: chip(jnp.bitwise_xor(z, k), y, x) for k in (1, 2, 3)}
    x_peer = {k: chip(z, y, jnp.bitwise_xor(x, k)) for k in (1, 2, 3)}
    y_peer = chip(z, jnp.bitwise_xor(y, 1), x)
    z_cross = {k: chip(jnp.bitwise_xor(z, k), 3 - y, x) for k in range(4)}
    z_far = {k: chip(jnp.bitwise_xor(z, k), jnp.bitwise_xor(y, 2), x) for k in range(4)}
    near = (1, 3, 2)

    loads = [
        pltpu.make_async_copy(wg_hbm, wg, wsem.at[0]),
        pltpu.make_async_copy(wu_hbm, wu, wsem.at[1]),
        pltpu.make_async_copy(wd_hbm.at[:, pl.ds(0, HALF)], wd.at[0], wsem.at[2]),
        pltpu.make_async_copy(wd_hbm.at[:, pl.ds(HALF, HALF)], wd.at[1], wsem.at[3]),
        pltpu.make_async_copy(gain_hbm, gain, wsem.at[4]),
    ]
    tables = [
        pltpu.make_async_copy(routes_hbm, routes_ref, wsem.at[5]),
        pltpu.make_async_copy(rw_hbm, rw_ref, wsem.at[6]),
        pltpu.make_async_copy(len_hbm, len_ref, wsem.at[7]),
    ]

    def first_loads():
        for c in (*tables, loads[4]):
            c.start()

    count = [0]
    started = []

    def send(src, dst, device):
        i = count[0]
        count[0] += 1
        if i >= SEND_SLOTS:
            started[i - SEND_SLOTS].wait_send()
        c = pltpu.make_async_remote_copy(
            src_ref=src, dst_ref=dst, send_sem=ss.at[i % SEND_SLOTS], recv_sem=rs.at[i], device_id=device, device_id_type=MESH
        )
        c.start()
        started.append(c)
        return c

    barrier = pltpu.get_barrier_semaphore()
    peers = [partner, y_peer, *z_peer.values(), *z_cross.values(), *z_far.values(), *x_peer.values()]
    for p in peers:
        pl.semaphore_signal(barrier, inc=1, device_id=p, device_id_type=MESH)

    rows = tok_ref.shape[0]

    def choose():
        for c in tables:
            c.wait()
        lane = lax.broadcasted_iota(jnp.int32, (rows, LANES), 1)
        place = jnp.bitwise_and(lane, 15)
        plane = jnp.bitwise_xor(z, jnp.bitwise_and(lax.shift_right_logical(lane, 4), 3))
        expert = (2 * plane + jnp.where(lane < 64, g, 1 - g)).astype(f32)
        ahead = lax.broadcasted_iota(jnp.int32, (rows, rows), 1)
        behind = lax.broadcasted_iota(jnp.int32, (rows, rows), 0)
        before = (ahead < behind).astype(f32).astype(bf16)
        unit = (ahead == behind).astype(f32)
        upright = lambda v: lax.dot_general(
            unit, v, (((1,), (1,)), ((), ())), precision=lax.Precision.HIGHEST, preferred_element_type=f32
        )
        named_here, weight_here = upright(routes_ref[...].astype(f32)), upright(rw_ref[...])
        first, second_one = named_here[:, 0:1] == expert, named_here[:, 1:2] == expert
        named = first | second_one
        earlier = dot(before, jnp.where(named, 1.0, 0.0).astype(bf16))
        here = named & (place < CAP) & (earlier == place.astype(f32))
        picks[...] = jnp.where(here, 1.0, 0.0).astype(bf16)
        weights = jnp.where(here, jnp.where(first, weight_here[:, 0:1], weight_here[:, 1:2]), 0.0)
        high = weights.astype(bf16)
        w_high[...] = high
        w_low[...] = (weights - high.astype(f32)).astype(bf16)

    def load():
        for c in loads[:4]:
            c.start()

    attend(
        first_loads, load, choose, len_ref, tok_hbm, key_hbm, value_hbm, gate_hbm, mix_hbm, wq_hbm, wk_hbm, wv_hbm, wf_hbm, wo_hbm,
        part_ref, *scratch[:ATTEND_SCRATCH],
    )
    loads[4].wait()
    pl.semaphore_wait(barrier, len(peers))
    c_part = send(part_ref, other_part, partner)

    c_part.wait_recv()
    total = tok_ref[...].astype(f32) + (part_ref[...].astype(f32) + other_part[...].astype(f32))
    res_b = total.astype(bf16)
    res[0] = res_b[:, :HALF]
    res[1] = res_b[:, HALF:]
    expert_in = rms(res_b.astype(f32), gain[...]).astype(bf16)
    xe[0] = expert_in[:, :HALF]
    xe[1] = expert_in[:, HALF:]
    pk[...] = lax.dot_general(
        picks[...], xe[t], (((0,), (0,)), ((), ())), preferred_element_type=f32
    ).astype(bf16).reshape(8, 16, HALF)
    sb[0, 0] = pk[0]
    c_s0 = {k: send(pk.at[k], sb.at[0, k], z_peer[k]) for k in (2, 1, 3)}
    c_s1 = {k: send(pk.at[4 + k], sb.at[1, k], z_cross[k]) for k in (2, 1, 3, 0)}
    r_i = lax.broadcasted_iota(jnp.int32, (BLOCK, 64), 0)
    c_i = lax.broadcasted_iota(jnp.int32, (BLOCK, 64), 1)
    r_k = lax.shift_right_logical(r_i * 43, 9)
    tight = (c_i == 16 * r_k + (r_i - CAP * r_k)).astype(f32).astype(bf16)

    mine_at = lambda d, q: xf.at[t, d, q]
    fwd = {}

    def forward(d, q):
        fwd[d, q] = send(mine_at(d, q), mine_at(d, q), partner)

    for k in near:
        c_s0[k].wait_recv()
    xf[t, 0, 0] = dot(tight, sb[0].reshape(64, HALF)).astype(bf16)
    c_ax, c_ay, c_bx = {}, {}, {}

    def ax(d):
        c_ax[d] = send(mine_at(0, 0), mine_at(d, 0), x_peer[d])

    def bx(d, q):
        c_bx[d, q] = send(mine_at(0, q), mine_at(d, q), x_peer[d])

    def ay(d):
        if d:
            c_ax[d].wait_recv()
        c_ay[d] = send(mine_at(d, 0), mine_at(d, 1), y_peer)
        forward(d, 0)

    ax(2)
    ay(0)
    for k in (0, 1, 3, 2):
        c_s1[k].wait_recv()
    xf[t, 0, 2] = dot(tight, sb[1].reshape(64, HALF)).astype(bf16)
    c_by = send(mine_at(0, 2), mine_at(0, 3), y_peer)
    bx(2, 2)
    ax(1)
    ax(3)
    forward(0, 2)
    ay(2)
    c_ay[0].wait_recv()
    forward(0, 1)
    c_by.wait_recv()
    bx(2, 3)
    forward(0, 3)
    bx(1, 2)
    bx(3, 2)
    bx(1, 3)
    bx(3, 3)
    ay(1)
    ay(3)
    for c in loads[:4]:
        c.wait()
    c_pi = {}

    def hide(d):
        for q in range(4):
            fwd[d, q].wait_recv()
        x0, x1 = xf[0, d].reshape(CHUNK, HALF), xf[1, d].reshape(CHUNK, HALF)
        gate = dot(x0, wg[0:HALF]) + dot(x1, wg[HALF : 2 * HALF])
        up = dot(x0, wu[0:HALF]) + dot(x1, wu[HALF : 2 * HALF])
        hid[d] = (gate / (1.0 + jnp.exp(-gate)) * up).astype(bf16)

    def down(d):
        po[d] = dot(hid[d], wd[1 - t]).astype(bf16)
        c_pi[d] = send(po.at[d], pi.at[d], partner)
        pm[d] = dot(hid[d], wd[t])

    def compute(d):
        hide(d)
        down(d)

    c_ry, c_xc, c_xo = {}, {}, {}

    def arrive(d):
        c_bx[d, 2].wait_recv()
        forward(d, 2)
        c_ay[d].wait_recv()
        forward(d, 1)
        c_bx[d, 3].wait_recv()
        forward(d, 3)

    side = {1: pl.ds(HALF // 2, HALF // 2), 3: pl.ds(0, HALF // 2)}

    def finish(d):
        c_pi[d].wait_recv()
        ys[d] = (pm[d] + pi[d].astype(f32)).astype(bf16).reshape(4, BLOCK, HALF)
        c_ry[d] = send(ys.at[d, 1], ry.at[d], y_peer)
        if d == 2:
            for n in (1, 3):
                c_xc[2, n] = send(ys.at[2, pl.ds(2, 2), :, side[4 - n]], hop_c.at[n], x_peer[n])

    def across(d):
        c_xc[2, 4 - d].wait_recv()
        ys[d, 2:4, :, side[d]] = (ys[d, 2:4, :, side[d]].astype(f32) + hop_c[4 - d].astype(f32)).astype(bf16)
        c_xc[d] = send(ys.at[d, pl.ds(2, 2)], rxc.at[d], x_peer[d])

    def second(d):
        c_ry[d].wait_recv()
        zs_out[d] = (ys[d, 0].astype(f32) + ry[d].astype(f32)).astype(bf16)
        if d == 2:
            for n in (1, 3):
                c_xo[2, n] = send(zs_out.at[2, :, side[4 - n]], hop_o.at[n], x_peer[n])
        elif d:
            c_xo[2, 4 - d].wait_recv()
            zs_out[d, :, side[d]] = (zs_out[d, :, side[d]].astype(f32) + hop_o[4 - d].astype(f32)).astype(bf16)
            c_xo[d] = send(zs_out.at[d], rxo.at[d], x_peer[d])

    compute(0)
    arrive(2)
    hide(2)
    arrive(1)
    down(2)
    finish(0)
    hide(1)
    finish(2)
    arrive(3)
    down(1)
    hide(3)
    finish(1)
    down(3)
    across(1)
    second(2)
    finish(3)
    across(3)
    second(1)
    second(3)
    second(0)


    for d in (1, 3):
        c_xc[d].wait_recv()
    crossed = ys[0, 2:4].astype(f32) + rxc[1].astype(f32) + rxc[3].astype(f32)
    spread = lambda v: lax.dot_general(
        tight, v.astype(bf16), (((0,), (0,)), ((), ())), preferred_element_type=f32
    ).astype(bf16).reshape(4, 16, HALF)
    er[1] = spread(crossed[0])
    er[2] = spread(crossed[1])
    order = (2, 1, 3, 0)
    c_r = []
    for k in order:
        c_r.append(send(er.at[2, k], rb.at[2, k], z_far[k]))
        c_r.append(send(er.at[1, k], rb.at[1, k], z_cross[k]))
    for d in (1, 3):
        c_xo[d].wait_recv()
    own = zs_out[0].astype(f32) + rxo[1].astype(f32) + rxo[3].astype(f32)
    er[0] = spread(own)
    rb[0, 0] = er[0, 0]
    c_r += [send(er.at[0, k], rb.at[0, k], z_peer[k]) for k in order[:3]]
    mixture = res[t].astype(f32)
    for c in c_r[:8]:
        c.wait_recv()
    weigh = lambda a, v: dot(w_high[:, a : a + 64], v) + dot(w_low[:, a : a + 64], v)
    for i in (1, 2):
        mixture = mixture + weigh(64, rb[i].reshape(64, HALF))
    for c in c_r[8:]:
        c.wait_recv()
    mixture = mixture + weigh(0, rb[0].reshape(64, HALF))
    fo[t] = mixture.astype(bf16)
    c_fo = send(fo.at[t], fo.at[t], partner)
    c_fo.wait_recv()
    out_ref[:, 0:HALF] = fo[0]
    out_ref[:, HALF : 2 * HALF] = fo[1]
    for c in started[-SEND_SLOTS:]:
        c.wait_send()


def on_device(
    tokens, lengths, key_cache, value_cache, gate_cache, mix_gain, query_weight, key_weight, value_weight,
    forget_weight, out_weight, expert_gain, routes, route_weights, expert_gate, expert_up, expert_down,
):
    rows, width = tokens.shape
    f32, bf16 = jnp.float32, jnp.bfloat16
    any_space = pl.BlockSpec(memory_space=pl.ANY)
    vmem = pl.BlockSpec(memory_space=pltpu.VMEM)
    blocks = lambda *s: pltpu.VMEM((*s, BLOCK, HALF), bf16)
    heads = pltpu.VMEM((SEQS * HEADS_HERE, LANES), f32)
    forget = forget_weight.T
    return pl.pallas_call(
        layer_kernel,
        out_shape=pltpu.VMEM((rows, width), bf16),
        in_specs=[any_space] * 17,
        out_specs=vmem,
        scratch_shapes=[
            pltpu.VMEM((rows, width), bf16),
            pltpu.VMEM((rows, width), bf16),
            pltpu.VMEM((1, width), f32),
            pltpu.VMEM(query_weight.shape, bf16),
            pltpu.VMEM(key_weight.shape, bf16),
            pltpu.VMEM(value_weight.shape, bf16),
            pltpu.VMEM(forget.shape, bf16),
            pltpu.VMEM(out_weight.shape, bf16),
            pltpu.VMEM(key_cache.shape, bf16),
            pltpu.VMEM(value_cache.shape, bf16),
            pltpu.VMEM(gate_cache.shape, f32),
            heads,
            heads,
            heads,
            pltpu.VMEM((SEQS, LANES), f32),
            heads,
            pltpu.SemaphoreType.DMA((7,)),
            pltpu.SemaphoreType.DMA((3, KV_BLOCKS)),
            pltpu.SMEM((rows,), jnp.int32),
            pltpu.VMEM((2, rows), jnp.int32),
            pltpu.VMEM((2, rows), f32),
            pltpu.VMEM((1, width), f32),
            pltpu.VMEM(expert_gate.shape, bf16),
            pltpu.VMEM(expert_up.shape, bf16),
            pltpu.VMEM((2, expert_down.shape[0], HALF), bf16),
            pltpu.VMEM((rows, width), bf16),
            pltpu.VMEM((2, rows, HALF), bf16),
            pltpu.VMEM((2, rows, HALF), bf16),
            pltpu.VMEM((rows, LANES), bf16),
            pltpu.VMEM((rows, LANES), bf16),
            pltpu.VMEM((rows, LANES), bf16),
            pltpu.VMEM((8, 16, HALF), bf16),
            pltpu.VMEM((2, 4, 16, HALF), bf16),
            blocks(2, 4, 4),
            pltpu.VMEM((4, CHUNK, HALF), f32),
            pltpu.VMEM((4, CHUNK, HALF), bf16),
            pltpu.VMEM((4, CHUNK, HALF), bf16),
            blocks(4, 4),
            blocks(4),
            blocks(4),
            blocks(4),
            blocks(4, 2),
            pltpu.VMEM((3, 4, 16, HALF), bf16),
            pltpu.VMEM((3, 4, 16, HALF), bf16),
            pltpu.VMEM((2, rows, HALF), bf16),
            pltpu.VMEM((4, CHUNK, expert_gate.shape[1]), bf16),
            pltpu.VMEM((4, 2, BLOCK, HALF // 2), bf16),
            pltpu.VMEM((4, BLOCK, HALF // 2), bf16),
            pltpu.SemaphoreType.DMA((8,)),
            pltpu.SemaphoreType.DMA((SEND_SLOTS,)),
            pltpu.SemaphoreType.DMA((COPIES,)),
        ],
        compiler_params=pltpu.CompilerParams(
            collective_id=0, has_side_effects=True, vmem_limit_bytes=60 * 1024 * 1024
        ),
        cost_estimate=pl.CostEstimate(flops=5_500_000_000, bytes_accessed=30_000_000, transcendentals=700_000),
        name="decode_layer",
    )(
        lengths, tokens, key_cache, value_cache, gate_cache, mix_gain.reshape(1, width), query_weight, key_weight,
        value_weight, forget, out_weight, expert_gain.reshape(1, width), routes.T, route_weights.T,
        expert_gate, expert_up, expert_down,
    )


def solution(mesh):
    return jax.shard_map(
        on_device,
        mesh=mesh,
        in_specs=(
            P("ep", None),
            P("ep"),
            P("ep", None, "tp"),
            P("ep", None, "tp"),
            P("ep", "tp", None),
            P(),
            P(None, "tp"),
            P(None, "tp"),
            P(None, "tp"),
            P(None, "tp"),
            P("tp", None),
            P(),
            P("ep", None),
            P("ep", None),
            P(None, ("ep", "tp")),
            P(None, ("ep", "tp")),
            P(("ep", "tp"), None),
        ),
        out_specs=P("ep", None),
        check_vma=False,
    )
```
